32 devices in a mesh: sp: 8 (over z, y), tp: 4 (over x, core).
Axes of the slice: x: 2, y: 2, z: 4, core: 2. Of those that a mesh axis runs over, the one named last changes fastest.
Arguments:
- query_narrow: bfloat16 [1024, 2048], P('sp', 'tp'), may hold values from -48 to 48
- key_narrow: bfloat16 [1024, 512], P('sp', 'tp'), may hold values from -15 to 15
- value_narrow: bfloat16 [1024, 512], P('sp', 'tp'), may hold values from -6 to 6
- gates_narrow: float32 [1024, 16], P(None, 'tp'), may hold values from -130 to 0, as said below
- query_broad: bfloat16 [1024, 2048], P('sp', 'tp'), may hold values from -48 to 48
- key_broad: bfloat16 [1024, 1024], P('sp', 'tp'), may hold values from -15 to 15
- value_broad: bfloat16 [1024, 1024], P('sp', 'tp'), may hold values from -6 to 6
- gates_broad: float32 [1024, 8], P(None, 'tp'), may hold values from -130 to 0, as said below
- project_narrow: bfloat16 [2048, 4096], P('tp'), may hold values from -0.1875 to 0.1875
- project_broad: bfloat16 [2048, 4096], P('tp'), may hold values from -0.1875 to 0.1875
- residual: bfloat16 [1024, 4096], P('sp'), may hold values from -6 to 6
- norm_gain: float32 [4096], replicated, may hold values from 0.1 to 1.9
- route_ids: int32 [1024, 4], P(('sp', 'tp')), may hold values from 0 to 31, all different within a row; in each aligned block of 32 rows (0 to 31, 32 to 63, ...) at most 8 rows name the same one
- route_weight: float32 [1024, 4], P(('sp', 'tp')), may hold values from 0.2 to 1.2
- expert_gate: bfloat16 [32, 4096, 256], P(('sp', 'tp')), may hold values from -0.09375 to 0.09375
- expert_up: bfloat16 [32, 4096, 256], P(('sp', 'tp')), may hold values from -0.09375 to 0.09375
- expert_down: bfloat16 [32, 256, 4096], P(('sp', 'tp')), may hold values from -0.375 to 0.375
- shared_gate: bfloat16 [4096, 1024], P(None, 'tp'), may hold values from -0.09375 to 0.09375
- shared_up: bfloat16 [4096, 1024], P(None, 'tp'), may hold values from -0.09375 to 0.09375
- shared_down: bfloat16 [1024, 4096], P('tp'), may hold values from -0.1875 to 0.1875
Outputs:
- layer_out: bfloat16 [1024, 4096], P(('sp', 'tp'))
The draws below stay inside these ranges and needn't reach their ends.
Inputs may be any that keep to these rules, and one draw needn't show every extreme that they name: `gates_narrow`: Non-increasing along positions in each head. `gates_broad`: Non-increasing along positions in each head. `route_ids`: each row names 4 different experts; among the rows of one device no expert is named by more than 8 rows, and that number is reached.
All inputs are finite; a program needn't handle non-finite values.
Results may differ from the reference program's by a relative error of at most 0.014.
Values may be sent and summed in bfloat16 or wider, within the bound.
A program may use at most 128 MiB of HBM per device.

```python
import math
import jax
import jax.numpy as jnp
import numpy as np
from jax import lax

D = 4096
NARROW_HEADS = 16
NARROW_SIZE = 128
NARROW_KV = 4
BROAD_HEADS = 8
BROAD_SIZE = 256
BROAD_KV = 4
EXPERT_WIDTH = 256
SHARED_WIDTH = 1024
TOP = 4
TOK_DEV = 128
SEQUENCE_LENGTH = 1024
TOK_SUB = 32
EXPERTS = 32
CAP = 8
ATT_W = 4096
N_SP = 8
N_TP = 4


def plant_pairs(key, head_count, kv_heads, head_size, salt):
    base = jax.random.fold_in(key, salt)
    sequence_lanes = jax.random.split(base, 7)
    key_rows = 2.5 * jnp.clip(jax.random.normal(sequence_lanes[5], (SEQUENCE_LENGTH, kv_heads * head_size), jnp.float32), -6.0, 6.0)
    query_rows = jnp.clip(jax.random.normal(sequence_lanes[6], (SEQUENCE_LENGTH, head_count * head_size), jnp.float32), -6.0, 6.0)
    return (query_rows, key_rows)


def forget_cumulative(key, head_count, salt):
    base = jax.random.fold_in(key, salt)
    sequence_lanes = jax.random.split(base, 5)
    rough = jnp.exp(jax.random.uniform(sequence_lanes[0], (SEQUENCE_LENGTH, head_count), jnp.float32, math.log(0.5), math.log(2.0)))
    block_rate = jnp.exp(jax.random.uniform(sequence_lanes[1], (SEQUENCE_LENGTH // TOK_DEV, head_count), jnp.float32, math.log(0.5), math.log(2.0)))
    block_rate = jnp.repeat(block_rate, TOK_DEV, axis=0)
    order = jax.random.permutation(sequence_lanes[2], head_count)
    quick = order < head_count // 2
    rate = jnp.where(quick, 1.0 / 40.0, 0.4 / SEQUENCE_LENGTH)
    gate_logarithm = -rate[None, :] * rough * block_rate
    segment_start = jax.random.randint(sequence_lanes[3], (2, head_count), 0, SEQUENCE_LENGTH)
    segment_length = jax.random.uniform(sequence_lanes[4], (2, head_count), jnp.float32, math.log(0.5), math.log(0.8))
    place_indices = jnp.arange(SEQUENCE_LENGTH, dtype=jnp.int32)[:, None]
    for round_index in range(2):
        gate_logarithm = gate_logarithm + jnp.where(place_indices == segment_start[round_index][None, :], segment_length[round_index][None, :], 0.0)
    return jnp.cumsum(gate_logarithm, axis=0)


def draw_query_narrow(key, part):
    return plant_pairs(key, NARROW_HEADS, NARROW_KV, NARROW_SIZE, 101)[0].astype(jnp.bfloat16)


def draw_key_narrow(key, part):
    return plant_pairs(key, NARROW_HEADS, NARROW_KV, NARROW_SIZE, 101)[1].astype(jnp.bfloat16)


def draw_query_broad(key, part):
    return plant_pairs(key, BROAD_HEADS, BROAD_KV, BROAD_SIZE, 202)[0].astype(jnp.bfloat16)


def draw_key_broad(key, part):
    return plant_pairs(key, BROAD_HEADS, BROAD_KV, BROAD_SIZE, 202)[1].astype(jnp.bfloat16)


def draw_gates_narrow(key, part):
    return forget_cumulative(key, NARROW_HEADS, 303)


def draw_gates_broad(key, part):
    return forget_cumulative(key, BROAD_HEADS, 404)


def block_scale(own_key, shape, shards, smallest, top_value):
    def one(dim, blocks):
        steps = jax.random.uniform(jax.random.fold_in(jax.random.fold_in(own_key, 6), dim), (blocks,), jnp.float32, smallest / len(shards), top_value / len(shards))
        return jnp.repeat(jnp.exp(steps), shape[dim] // blocks).reshape((-1,) + (1,) * (len(shape) - dim - 1))

    gain = one(*shards[0])
    for cut in shards[1:]:
        gain = gain * one(*cut)
    return gain


def shared_out(stream_key, own, number, rows, count, top, reach, slope):
    ranking = jax.random.permutation(stream_key, count)
    packed, usual = shares(count, rows * top, reach, slope, True), shares(count, rows * top, reach, slope, False)
    places = jnp.arange(count)

    def named(tallies, turn):
        used = int((tallies > 0).sum())
        fixed = max(1, used // 4)
        moved = fixed + (places - fixed + turn * (used - fixed)) % max(1, count - fixed)
        return jnp.zeros((count,), jnp.int32).at[ranking[jnp.where(places < fixed, places, moved)]].set(jnp.asarray(tallies, jnp.int32))

    tallies = jnp.where(number % 4 == 0, named(packed, number // 4), named(usual, number - number // 4 - 1))
    mixed = jax.random.permutation(jax.random.fold_in(own, 3), count)
    donor, sink = mixed[0:count // 2 * 2:2], mixed[1:count // 2 * 2:2]
    slack = jnp.minimum(tallies[donor] - 1, reach - tallies[sink]) // 2
    slack = jnp.where((donor == ranking[0]) | (sink == ranking[0]) | (tallies[sink] == 0), 0, jnp.maximum(slack, 0))
    moved = jax.random.randint(jax.random.fold_in(own, 4), (count // 2,), 0, 1 << 20) % (slack + 1)
    tallies = tallies.at[donor].add(-moved).at[sink].add(moved)
    items = jnp.searchsorted(jnp.cumsum(tallies), jnp.arange(rows * top), side="right").astype(jnp.int32)
    grid = items.reshape(top, rows).T
    grid = grid[jax.random.permutation(jax.random.fold_in(own, 1), rows)]
    turn = jax.random.randint(jax.random.fold_in(own, 2), (rows, 1), 0, top)
    return jnp.take_along_axis(grid, (jnp.arange(top)[None, :] + turn) % top, axis=1)


def shares(amount, total, bound, skew, full):
    portions = [(1 << 20) // math.isqrt(rank ** skew) + 1 for rank in range(1, amount + 1)]
    largest = bound if full else min(bound, max(-(-total // amount), total * portions[0] // sum(portions)))
    least = 1 if total - largest >= amount - 1 else 0
    holding, surplus = [largest] + [least] * (amount - 1), total - largest - least * (amount - 1)
    while surplus > 0:
        movable = [i for i in range(1, amount) if holding[i] < largest] or [i for i in range(1, amount) if holding[i] < bound]
        pool, left = sum([portions[i] for i in movable]), surplus
        for i in movable:
            more = min(bound - holding[i], max(1, left * portions[i] // pool), surplus)
            holding[i] = holding[i] + more
            surplus = surplus - more
    return np.array(holding)


def centred(stream_key, shape, deviation, most, shards=(), held_as=jnp.bfloat16):
    gain = block_scale(stream_key, shape, shards, -0.22, 0.18) if shards else 1.0
    values = jax.random.normal(stream_key, shape, jnp.float32) * deviation * gain
    return jnp.minimum(jnp.maximum(values, -most), most).astype(held_as)


def setup_inputs(seed: int = 0) -> dict:
    key_list = jax.random.split(jax.random.key(seed), 21)
    query_narrow = draw_query_narrow(jax.random.fold_in(key_list[20], 71), 0)
    key_narrow = draw_key_narrow(jax.random.fold_in(key_list[20], 71), 0)
    value_narrow = centred(key_list[2], (SEQUENCE_LENGTH, NARROW_KV * NARROW_SIZE), 1.0, 6.0, ((0, 8), (1, 4)))
    gates_narrow = draw_gates_narrow(jax.random.fold_in(key_list[20], 71), 0)
    query_broad = draw_query_broad(jax.random.fold_in(key_list[20], 71), 0)
    key_broad = draw_key_broad(jax.random.fold_in(key_list[20], 71), 0)
    value_broad = centred(key_list[6], (SEQUENCE_LENGTH, BROAD_KV * BROAD_SIZE), 1.0, 6.0, ((0, 8), (1, 4)))
    gates_broad = draw_gates_broad(jax.random.fold_in(key_list[20], 71), 0)
    project_narrow = centred(key_list[8], (NARROW_HEADS * NARROW_SIZE, D), (ATT_W // 4) ** -0.5, 0.1875, ((0, 4),))
    project_broad = centred(key_list[9], (BROAD_HEADS * BROAD_SIZE, D), (ATT_W // 4) ** -0.5, 0.1875, ((0, 4),))
    residual = centred(key_list[10], (SEQUENCE_LENGTH, D), 1.0, 6.0, ((0, 8),))
    norm_gain = jnp.clip(1.0 + 0.18 * jax.random.normal(key_list[11], (D,), jnp.float32), 0.1, 1.9)
    route_ids_keys = jax.random.split(jax.random.fold_in(key_list[12], 1), SEQUENCE_LENGTH // TOK_SUB)
    route_ids_turns = jax.random.permutation(jax.random.fold_in(key_list[12], 3), SEQUENCE_LENGTH // TOK_SUB)
    route_ids = jax.vmap(lambda own, number: shared_out(jax.random.fold_in(key_list[12], 2), own, number, TOK_SUB, EXPERTS, TOP, CAP, 1))(route_ids_keys, route_ids_turns).reshape((SEQUENCE_LENGTH, TOP))
    route_weight = jnp.clip(jnp.exp(math.log(1.2) - 1.7917595 * jax.random.uniform(key_list[13], (SEQUENCE_LENGTH, TOP), jnp.float32) ** block_scale(key_list[13], (SEQUENCE_LENGTH, TOP), ((0, 32),), -0.2, 0.2)), 0.2, 1.2)
    expert_gate = centred(key_list[14], (EXPERTS, D, EXPERT_WIDTH), D ** -0.5, 0.09375, ((0, 32),))
    expert_up = centred(key_list[15], (EXPERTS, D, EXPERT_WIDTH), D ** -0.5, 0.09375, ((0, 32),))
    expert_down = centred(key_list[16], (EXPERTS, EXPERT_WIDTH, D), EXPERT_WIDTH ** -0.5, 0.375, ((0, 32),))
    shared_gate = centred(key_list[17], (D, SHARED_WIDTH), D ** -0.5, 0.09375, ((1, 4),))
    shared_up = centred(key_list[18], (D, SHARED_WIDTH), D ** -0.5, 0.09375, ((1, 4),))
    shared_down = centred(key_list[19], (SHARED_WIDTH, D), SHARED_WIDTH ** -0.5, 0.1875, ((0, 4),))
    return {"query_narrow": query_narrow, "key_narrow": key_narrow, "value_narrow": value_narrow, "gates_narrow": gates_narrow, "query_broad": query_broad, "key_broad": key_broad, "value_broad": value_broad, "gates_broad": gates_broad, "project_narrow": project_narrow, "project_broad": project_broad, "residual": residual, "norm_gain": norm_gain, "route_ids": route_ids, "route_weight": route_weight, "expert_gate": expert_gate, "expert_up": expert_up, "expert_down": expert_down, "shared_gate": shared_gate, "shared_up": shared_up, "shared_down": shared_down}


norm_epsilon = 1e-06

def group_attention(queries, key_rows, value_rows, gate_totals, head_count, kv_heads, head_size):
    group_size = head_count // kv_heads
    query_block = 256
    scaling = head_size ** (-0.5)
    outputs = []
    for first_query in range(0, SEQUENCE_LENGTH, query_block):
        last_key = first_query + query_block
        query_heads = queries[first_query:last_key].astype(jnp.float32).reshape(query_block, kv_heads, group_size, head_size)
        key_heads = key_rows[:last_key].astype(jnp.float32).reshape(last_key, kv_heads, head_size)
        value_heads = value_rows[:last_key].astype(jnp.float32).reshape(last_key, kv_heads, head_size)
        scores = jnp.einsum('tkgd,skd->kgts', query_heads, key_heads) * scaling
        query_gates = gate_totals[first_query:last_key].reshape(query_block, kv_heads, group_size).transpose(1, 2, 0)
        key_gates = gate_totals[:last_key].T.reshape(kv_heads, group_size, 1, last_key)
        scores = scores + query_gates[..., None] - key_gates
        allowed = jnp.arange(last_key)[None, :] <= (first_query + jnp.arange(query_block))[:, None]
        scores = jnp.where(allowed, scores, -jnp.inf)
        highest = lax.optimization_barrier(jnp.max(scores, axis=-1, keepdims=True))
        weights = jnp.exp(scores - highest)
        totals = lax.optimization_barrier(jnp.sum(weights, axis=-1))
        rounded = lax.optimization_barrier(weights.astype(jnp.bfloat16)).astype(jnp.float32)
        blended = jnp.einsum('kgts,skd->tkgd', rounded, value_heads) / totals.transpose(2, 0, 1)[..., None]
        outputs.append(blended.reshape(query_block, head_count * head_size).astype(jnp.bfloat16))
    return jnp.concatenate(outputs, axis=0)

def routed_experts(normed, route_ids, route_weight, expert_gate, expert_up, expert_down):
    top_count = route_ids.shape[1]
    flat_ids = route_ids.reshape(-1)
    flat_weight = lax.optimization_barrier(route_weight.reshape(-1).astype(jnp.bfloat16)).astype(jnp.float32)
    most_rows = N_SP * N_TP * CAP

    def one_expert(carried, expert):
        chosen = flat_ids == expert
        picked = jnp.nonzero(chosen, size=most_rows, fill_value=0)[0].astype(jnp.int32)
        live = jnp.arange(most_rows) < jnp.sum(chosen.astype(jnp.int32))
        token_index = picked // top_count
        rows = normed[token_index]
        gate_out = jnp.dot(rows, expert_gate[expert], preferred_element_type=jnp.float32)
        up_out = jnp.dot(rows, expert_up[expert], preferred_element_type=jnp.float32)
        hidden = (jax.nn.silu(gate_out) * up_out).astype(jnp.bfloat16)
        output = jnp.dot(hidden, expert_down[expert], preferred_element_type=jnp.float32)
        output = lax.optimization_barrier(output.astype(jnp.bfloat16)).astype(jnp.float32)
        contribution = jnp.where(live[:, None], flat_weight[picked][:, None] * output, jnp.zeros((), jnp.float32))
        return (carried.at[token_index].add(contribution), None)
    routed, ignored = lax.scan(one_expert, jnp.zeros((SEQUENCE_LENGTH, D), jnp.float32), jnp.arange(EXPERTS, dtype=jnp.int32))
    return routed

def reference(query_narrow, key_narrow, value_narrow, gates_narrow, query_broad, key_broad, value_broad, gates_broad, project_narrow, project_broad, residual, norm_gain, route_ids, route_weight, expert_gate, expert_up, expert_down, shared_gate, shared_up, shared_down):
    narrow = group_attention(query_narrow, key_narrow, value_narrow, gates_narrow, NARROW_HEADS, NARROW_KV, NARROW_SIZE)
    broad = group_attention(query_broad, key_broad, value_broad, gates_broad, BROAD_HEADS, BROAD_KV, BROAD_SIZE)
    width_narrow = NARROW_HEADS * NARROW_SIZE // N_TP
    width_broad = BROAD_HEADS * BROAD_SIZE // N_TP
    mixture = jnp.zeros((SEQUENCE_LENGTH, D), jnp.float32)
    for member in range(N_TP):
        low_n, high_n = (member * width_narrow, (member + 1) * width_narrow)
        low_b, high_b = (member * width_broad, (member + 1) * width_broad)
        portion = jnp.dot(narrow[:, low_n:high_n], project_narrow[low_n:high_n], preferred_element_type=jnp.float32)
        portion = portion + jnp.dot(broad[:, low_b:high_b], project_broad[low_b:high_b], preferred_element_type=jnp.float32)
        mixture = mixture + lax.optimization_barrier(portion.astype(jnp.bfloat16)).astype(jnp.float32)
    stream = residual.astype(jnp.float32) + mixture
    normed = (stream * lax.rsqrt(lax.optimization_barrier(jnp.mean(stream * stream, axis=-1, keepdims=True)) + norm_epsilon) * norm_gain).astype(jnp.bfloat16)
    shared_hidden = (jax.nn.silu(jnp.dot(normed, shared_gate, preferred_element_type=jnp.float32)) * jnp.dot(normed, shared_up, preferred_element_type=jnp.float32)).astype(jnp.bfloat16)
    width_shared = SHARED_WIDTH // N_TP
    shared = jnp.zeros((SEQUENCE_LENGTH, D), jnp.float32)
    for member in range(N_TP):
        low_s, high_s = (member * width_shared, (member + 1) * width_shared)
        portion = jnp.dot(shared_hidden[:, low_s:high_s], shared_down[low_s:high_s], preferred_element_type=jnp.float32)
        shared = shared + lax.optimization_barrier(portion.astype(jnp.bfloat16)).astype(jnp.float32)
    routed = routed_experts(normed, route_ids, route_weight, expert_gate, expert_up, expert_down)
    return (stream + shared + routed).astype(jnp.bfloat16)
```

```python
import functools
import math

import jax
import jax.numpy as jnp
from jax import lax
from jax.experimental import pallas as pl
from jax.experimental.pallas import tpu as pltpu
from jax.sharding import PartitionSpec as P

MESH = pl.DeviceIdType.MESH

NARROW_SIZE = 128
BROAD_SIZE = 256


norm_epsilon = 1e-06


def attend_kernel(
    q_narrow, q_broad, g_narrow, g_broad, k_narrow, k_broad, pairs_ref, o_narrow, o_broad
):
    tokens, length = q_narrow.shape[0], pairs_ref.shape[0]
    first_row = lax.axis_index("sp") * tokens
    key_place = lax.broadcasted_iota(jnp.int32, (tokens, length), 1)
    query_place = first_row + lax.broadcasted_iota(jnp.int32, (tokens, length), 0)
    allowed = key_place <= query_place
    rows = pl.ds(pl.multiple_of(first_row, tokens), tokens)
    value_first = pairs_ref.shape[1] // 2
    column = 0
    for queries, gates, key_gates, outputs, head_size in (
        (q_narrow, g_narrow, k_narrow, o_narrow, NARROW_SIZE),
        (q_broad, g_broad, k_broad, o_broad, BROAD_SIZE),
    ):
        heads = queries.shape[1] // head_size
        widest = value_first * head_size // (NARROW_SIZE + BROAD_SIZE)
        group_size = heads * head_size // widest
        own_gates = gates[rows, :]
        for kv in range(widest // head_size):
            keys = pairs_ref[:, column : column + head_size]
            values = pairs_ref[:, value_first + column : value_first + column + head_size]
            reachable = (
                lax.broadcasted_iota(jnp.int32, (length, head_size), 0) < first_row + tokens
            )
            values = jnp.where(reachable, values.astype(jnp.float32), 0.0).astype(jnp.bfloat16)
            column += head_size
            for member in range(group_size):
                head = kv * group_size + member
                span = slice(head * head_size, (head + 1) * head_size)
                scores = lax.dot_general(
                    queries[:, span],
                    keys,
                    (((1,), (1,)), ((), ())),
                    preferred_element_type=jnp.float32,
                )
                scores = scores * head_size ** (-0.5)
                scores = scores + own_gates[:, head : head + 1] - key_gates[head : head + 1, :]
                scores = jnp.where(allowed, scores, -jnp.inf)
                weights = jnp.exp(scores - jnp.max(scores, axis=1, keepdims=True))
                total = jnp.sum(weights, axis=1, keepdims=True)
                blended = jnp.dot(
                    weights.astype(jnp.bfloat16), values, preferred_element_type=jnp.float32
                )
                outputs[:, span] = (blended / total).astype(jnp.bfloat16)


def add_kernel(stream_ref, shared_ref, routed_ref, out_ref):
    total = stream_ref[...]
    for parts in (shared_ref, routed_ref):
        for index in range(parts.shape[0]):
            total = total + parts[index].astype(jnp.float32)
    out_ref[...] = total.astype(jnp.bfloat16)


def norm_kernel(portions_ref, residual_ref, gain_ref, stream_ref, normed_ref):
    count = stream_ref.shape[0]
    first = lax.axis_index("tp") * count
    stream = residual_ref[pl.ds(pl.multiple_of(first, count), count), :].astype(jnp.float32)
    for index in range(portions_ref.shape[0]):
        stream = stream + portions_ref[index].astype(jnp.float32)
    stream_ref[...] = stream
    scale = lax.rsqrt(jnp.mean(stream * stream, axis=1, keepdims=True) + norm_epsilon)
    normed_ref[...] = (stream * scale * gain_ref[...]).astype(jnp.bfloat16)


class Groups:
    def __init__(self, n_sp, n_tp):
        self.n_sp, self.n_tp = n_sp, n_tp
        self.outer = math.gcd(n_sp, 4)
        self.inner = n_sp // self.outer
        self.plane = self.inner * n_tp

    def size(self, kind):
        return {"tp": self.n_tp, "outer": self.outer, "plane": self.plane}[kind]

    def place(self):
        sp, tp = lax.axis_index("sp"), lax.axis_index("tp")
        return sp // self.inner, sp % self.inner, tp

    def mine(self, kind):
        z, y, t = self.place()
        return {"tp": t, "outer": z, "plane": y * self.n_tp + t}[kind]

    def device(self, kind, index):
        z, y, t = self.place()
        if kind == "tp":
            return (z * self.inner + y, index)
        if kind == "outer":
            return (index * self.inner + y, t)
        return (z * self.inner + index // self.n_tp, index % self.n_tp)


def swap_kernel(groups, plans, *refs):
    count = len(plans)
    sources, targets, sems = refs[:count], refs[count : 2 * count], refs[2 * count :]
    barrier = pltpu.get_barrier_semaphore()
    greeted = 0
    for kind in sorted({plan[0] for plan in plans}):
        size, me = groups.size(kind), groups.mine(kind)
        for step in range(1, size):
            pl.semaphore_signal(
                barrier,
                inc=1,
                device_id=groups.device(kind, (me + step) % size),
                device_id_type=MESH,
            )
            greeted += 1
    pl.semaphore_wait(barrier, greeted)

    def cut(ref, axis, index):
        if axis is None:
            return ref
        return ref.at[index] if axis == 0 else ref.at[:, index]

    started, local_copies = [], []
    for number, (kind, source_axis, target_axis) in enumerate(plans):
        send, recv, keep = sems[3 * number : 3 * number + 3]
        size, me = groups.size(kind), groups.mine(kind)
        for step in range(1, size):
            peer = (me + step) % size
            copy = pltpu.make_async_remote_copy(
                src_ref=cut(sources[number], source_axis, peer),
                dst_ref=cut(targets[number], target_axis, me),
                send_sem=send.at[step],
                recv_sem=recv.at[step],
                device_id=groups.device(kind, peer),
                device_id_type=MESH,
            )
            copy.start()
            started.append(copy)
        own = pltpu.make_async_copy(
            cut(sources[number], source_axis, me), cut(targets[number], target_axis, me), keep
        )
        own.start()
        local_copies.append(own)
    for own in local_copies:
        own.wait()
    for copy in started:
        copy.wait()


def swap(groups, collective_id, *moves):
    plans, shapes, scratch = [], [], []
    for array, kind, source_axis, target_axis in moves:
        size = groups.size(kind)
        plans.append((kind, source_axis, target_axis))
        block = list(array.shape)
        if source_axis is not None:
            del block[source_axis]
        block.insert(target_axis, size)
        shapes.append(jax.ShapeDtypeStruct(tuple(block), array.dtype))
        scratch += [
            pltpu.SemaphoreType.DMA((size,)),
            pltpu.SemaphoreType.DMA((size,)),
            pltpu.SemaphoreType.DMA,
        ]
    return pl.pallas_call(
        functools.partial(swap_kernel, groups, tuple(plans)),
        out_shape=tuple(shapes),
        in_specs=[pl.BlockSpec(memory_space=pl.ANY)] * len(moves),
        out_specs=tuple([pl.BlockSpec(memory_space=pl.ANY)] * len(moves)),
        scratch_shapes=scratch,
        compiler_params=pltpu.CompilerParams(collective_id=collective_id, has_side_effects=True),
        name=f"swap_{collective_id}",
    )(*[move[0] for move in moves])


def gather_kernel(groups, own_ref, notes_ref, all_ref, all_notes_ref, *sems):
    line_send, line_recv, side_send, side_recv, note_send, note_recv, keep = sems
    outer, inner = groups.outer, groups.inner
    z, y, t = groups.place()
    barrier = pltpu.get_barrier_semaphore()
    for step in range(1, outer):
        pl.semaphore_signal(
            barrier, inc=1, device_id=groups.device("outer", (z + step) % outer), device_id_type=MESH
        )
    for step in range(1, inner):
        pl.semaphore_signal(
            barrier, inc=1, device_id=(z * inner + (y + step) % inner, t), device_id_type=MESH
        )
    pl.semaphore_wait(barrier, outer + inner - 2)

    def slot(far, side):
        return all_ref.at[(z - far) * inner + side]

    def upward(far):
        source = own_ref if far == 0 else slot(far, y)
        return pltpu.make_async_remote_copy(
            src_ref=source,
            dst_ref=slot(far, y),
            send_sem=line_send.at[far],
            recv_sem=line_recv.at[far + 1],
            device_id=((z + 1) * inner + y, t),
            device_id_type=MESH,
        )

    def sideways(far, step):
        source = own_ref if far == 0 else slot(far, y)
        return pltpu.make_async_remote_copy(
            src_ref=source,
            dst_ref=slot(far, y),
            send_sem=side_send.at[far, step],
            recv_sem=side_recv.at[far, step],
            device_id=(z * inner + (y + step) % inner, t),
            device_id_type=MESH,
        )

    def from_below(far):
        return pltpu.make_async_remote_copy(
            src_ref=slot(far, y),
            dst_ref=slot(far, y),
            send_sem=line_send.at[0],
            recv_sem=line_recv.at[far],
            device_id=((z + 1) * inner + y, t),
            device_id_type=MESH,
        )

    def from_side(far, step):
        side = (y + inner - step) % inner
        return pltpu.make_async_remote_copy(
            src_ref=slot(far, side),
            dst_ref=slot(far, side),
            send_sem=side_send.at[0, step],
            recv_sem=side_recv.at[far, step],
            device_id=(z * inner + (y + step) % inner, t),
            device_id_type=MESH,
        )

    def note(step):
        return pltpu.make_async_remote_copy(
            src_ref=notes_ref,
            dst_ref=all_notes_ref.at[z],
            send_sem=note_send.at[step],
            recv_sem=note_recv.at[step],
            device_id=groups.device("outer", (z + step) % outer),
            device_id_type=MESH,
        )

    def later_side(step):
        return (y + step) % inner > y

    def earlier_side(step):
        return (y + inner - step) % inner < y

    has_above = z < outer - 1
    pl.when(has_above)(lambda: upward(0).start())
    for step in range(1, inner):
        pl.when(later_side(step))(lambda step=step: sideways(0, step).start())
    for step in range(1, outer):
        note(step).start()
    own_copy = pltpu.make_async_copy(own_ref, all_ref.at[z * inner + y], keep.at[0])
    own_note = pltpu.make_async_copy(notes_ref, all_notes_ref.at[z], keep.at[1])
    own_copy.start()
    own_note.start()
    for far in range(1, outer):

        @pl.when(z >= far)
        def _(far=far):
            from_below(far).wait_recv()
            if far < outer - 1:
                pl.when(has_above)(lambda: upward(far).start())
            for step in range(1, inner):
                sideways(far, step).start()

    for far in range(outer):

        @pl.when(z >= far)
        def _(far=far):
            for step in range(1, inner):
                if far == 0:
                    pl.when(earlier_side(step))(lambda: from_side(far, step).wait_recv())
                    pl.when(later_side(step))(lambda: sideways(far, step).wait_send())
                else:
                    from_side(far, step).wait_recv()
                    sideways(far, step).wait_send()
            if far < outer - 1:
                pl.when(has_above)(lambda: upward(far).wait_send())

    for step in range(1, outer):
        note(step).wait()
    own_copy.wait()
    own_note.wait()


def gather(groups, collective_id, own, notes):
    outer, inner = groups.outer, groups.inner
    dma = pltpu.SemaphoreType.DMA
    return pl.pallas_call(
        functools.partial(gather_kernel, groups),
        out_shape=(
            jax.ShapeDtypeStruct((groups.n_sp,) + own.shape, own.dtype),
            jax.ShapeDtypeStruct((outer,) + notes.shape, notes.dtype),
        ),
        in_specs=[pl.BlockSpec(memory_space=pl.ANY)] * 2,
        out_specs=(pl.BlockSpec(memory_space=pl.ANY),) * 2,
        scratch_shapes=[
            dma((outer + 1,)),
            dma((outer + 1,)),
            dma((outer, inner)),
            dma((outer, inner)),
            dma((outer,)),
            dma((outer,)),
            dma((2,)),
        ],
        compiler_params=pltpu.CompilerParams(collective_id=collective_id, has_side_effects=True),
        name="gather",
    )(own, notes)


def dispatch_kernel(
    groups, own_ref, select_ref, all_ref, inbound_ref, line_ref, out_ref, *sems
):
    up_send, up_recv, down_send, down_recv, tp_send, tp_recv, plane_send, plane_recv, keep = sems
    outer, inner, n_tp, plane = groups.outer, groups.inner, groups.n_tp, groups.plane
    z, y, t = groups.place()
    pairs = n_tp // 2
    high, low = t // 2, t % 2
    partner = (z * inner + y, high * 2 + 1 - low)
    me = groups.mine("plane")
    barrier = pltpu.get_barrier_semaphore()
    for kind in ("outer", "plane"):
        for step in range(1, groups.size(kind)):
            pl.semaphore_signal(
                barrier,
                inc=1,
                device_id=groups.device(kind, (groups.mine(kind) + step) % groups.size(kind)),
                device_id_type=MESH,
            )
    pl.semaphore_wait(barrier, outer + plane - 2)

    def remote(source, target, send, recv, device):
        return pltpu.make_async_remote_copy(
            src_ref=source,
            dst_ref=target,
            send_sem=send,
            recv_sem=recv,
            device_id=device,
            device_id_type=MESH,
        )

    def along(far, direction):
        send, recv = (up_send, up_recv) if direction > 0 else (down_send, down_recv)
        block = z - direction * far
        source = own_ref if far == 0 else line_ref.at[block]
        return remote(
            source,
            line_ref.at[block],
            send.at[far],
            recv.at[far + 1],
            ((z + direction) * inner + y, t),
        )

    def arrived(far, direction):
        send, recv = (up_send, up_recv) if direction > 0 else (down_send, down_recv)
        block = line_ref.at[z - direction * far]
        return remote(
            block, block, send.at[0], recv.at[far], ((z + direction) * inner + y, t)
        )

    def outward(lane, block, step):
        peer = (me + step) % plane
        return remote(
            out_ref.at[block, peer],
            inbound_ref.at[me, block],
            plane_send.at[lane, step],
            plane_recv.at[lane, step],
            groups.device("plane", peer),
        )

    def inward(lane, block, step):
        peer = (me + plane - step) % plane
        target = inbound_ref.at[peer, block]
        return remote(
            target,
            target,
            plane_send.at[lane, step],
            plane_recv.at[lane, step],
            groups.device("plane", peer),
        )

    def keep_own(lane, block):
        return pltpu.make_async_copy(
            out_ref.at[block, me], inbound_ref.at[me, block], keep.at[1 + lane]
        )

    def work(lane, block, rows_ref):
        chosen = jnp.dot(select_ref[block], rows_ref[...], preferred_element_type=jnp.float32)
        out_ref[block] = chosen.reshape(out_ref.shape[1:]).astype(jnp.bfloat16)
        for step in range(1, plane):
            outward(lane, block, step).start()
        keep_own(lane, block).start()

    def finish(lane, block):
        keep_own(lane, block).wait()
        for step in range(1, plane):
            inward(lane, block, step).wait_recv()
            outward(lane, block, step).wait_send()

    def to_side(step):
        return remote(
            own_ref,
            all_ref.at[t],
            tp_send.at[step],
            tp_recv.at[step],
            (z * inner + y, ((high + step) % pairs) * 2 + low),
        )

    def to_partner(step):
        block = ((high + pairs - step) % pairs) * 2 + low
        source = own_ref if step == 0 else all_ref.at[block]
        target = all_ref.at[t] if step == 0 else all_ref.at[block]
        return remote(
            source, target, tp_send.at[pairs + step], tp_recv.at[pairs + step], partner
        )

    has_above, has_below = z < outer - 1, z > 0
    pl.when(has_above)(lambda: along(0, 1).start())
    pl.when(has_below)(lambda: along(0, -1).start())
    for step in range(1, pairs):
        to_side(step).start()
    to_partner(0).start()
    own_copy = pltpu.make_async_copy(own_ref, all_ref.at[t], keep.at[0])
    own_copy.start()
    work(0, z, own_ref)
    directions = ((1, has_above, 0), (-1, has_below, outer - 1))
    for far in range(1, outer):
        for direction, onward, base in directions:
            present = z >= far if direction > 0 else z + far < outer

            @pl.when(present)
            def _(far=far, direction=direction, onward=onward):
                arrived(far, direction).wait_recv()
                if far < outer - 1:
                    pl.when(onward)(lambda: along(far, direction).start())

        if far == 1:
            for step in range(1, pairs):
                side = all_ref.at[((high + pairs - step) % pairs) * 2 + low]
                remote(side, side, tp_send.at[step], tp_recv.at[step], partner).wait_recv()
                to_partner(step).start()
        for direction, onward, base in directions:
            present = z >= far if direction > 0 else z + far < outer

            @pl.when(present)
            def _(far=far, direction=direction, base=base):
                block = z - direction * far
                work(base + far, block, line_ref.at[block])

    finish(0, z)
    for far in range(1, outer):
        for direction, onward, base in directions:
            present = z >= far if direction > 0 else z + far < outer

            @pl.when(present)
            def _(far=far, direction=direction, onward=onward, base=base):
                finish(base + far, z - direction * far)
                if far < outer - 1:
                    pl.when(onward)(lambda: along(far, direction).wait_send())

    pl.when(has_above)(lambda: along(0, 1).wait_send())
    pl.when(has_below)(lambda: along(0, -1).wait_send())
    for step in range(1, pairs):
        to_side(step).wait_send()
    for step in range(pairs):
        to_partner(step).wait_send()
        block = all_ref.at[((high + pairs - step) % pairs) * 2 + 1 - low]
        remote(
            block, block, tp_send.at[pairs + step], tp_recv.at[pairs + step], partner
        ).wait_recv()
    own_copy.wait()


def dispatch_rows(groups, collective_id, own, select, seats):
    outer, plane, n_tp = groups.outer, groups.plane, groups.n_tp
    dma, kind = pltpu.SemaphoreType.DMA, own.dtype
    lanes = 2 * outer - 1
    vmem, anywhere = pl.BlockSpec(memory_space=pltpu.VMEM), pl.BlockSpec(memory_space=pl.ANY)
    return pl.pallas_call(
        functools.partial(dispatch_kernel, groups),
        out_shape=(
            jax.ShapeDtypeStruct((n_tp,) + own.shape, kind),
            jax.ShapeDtypeStruct((plane, outer, seats, own.shape[1]), kind),
        ),
        in_specs=[vmem, vmem],
        out_specs=(anywhere, anywhere),
        scratch_shapes=[
            pltpu.VMEM((outer,) + own.shape, kind),
            pltpu.VMEM((outer, plane, seats, own.shape[1]), kind),
            dma((outer + 1,)),
            dma((outer + 1,)),
            dma((outer + 1,)),
            dma((outer + 1,)),
            dma((n_tp,)),
            dma((n_tp,)),
            dma((lanes, plane)),
            dma((lanes, plane)),
            dma((lanes + 1,)),
        ],
        compiler_params=pltpu.CompilerParams(collective_id=collective_id, has_side_effects=True),
        name="dispatch_rows",
    )(own, select)


def flip(value, mask):
    bit = 1
    while bit <= mask:
        if mask & bit:
            value = value + bit - 2 * bit * ((value // bit) % 2)
        bit *= 2
    return value


def combine_kernel(
    groups, result_ref, mix_ref, shared_ref, routed_ref, parts_ref, back_ref, sum_ref, *sems
):
    plane_send, plane_recv, line_send, line_recv, tp_send, tp_recv, keep = sems
    outer, inner, n_tp, plane = groups.outer, groups.inner, groups.n_tp, groups.plane
    z, y, t = groups.place()
    me = groups.mine("plane")
    barrier = pltpu.get_barrier_semaphore()
    for kind in ("outer", "plane"):
        for step in range(1, groups.size(kind)):
            pl.semaphore_signal(
                barrier,
                inc=1,
                device_id=groups.device(kind, (groups.mine(kind) + step) % groups.size(kind)),
                device_id_type=MESH,
            )
    pl.semaphore_wait(barrier, outer + plane - 2)

    def remote(source, target, send, recv, device):
        return pltpu.make_async_remote_copy(
            src_ref=source,
            dst_ref=target,
            send_sem=send,
            recv_sem=recv,
            device_id=device,
            device_id_type=MESH,
        )

    def outward(mask, step):
        peer, block = (me + step) % plane, flip(z, mask)
        return remote(
            result_ref.at[peer, block],
            back_ref.at[block, me],
            plane_send.at[mask, step],
            plane_recv.at[mask, step],
            groups.device("plane", peer),
        )

    def inward(mask, step):
        peer, block = (me + plane - step) % plane, flip(z, mask)
        target = back_ref.at[block, peer]
        return remote(
            target,
            target,
            plane_send.at[mask, step],
            plane_recv.at[mask, step],
            groups.device("plane", peer),
        )

    def keep_own(mask):
        block = flip(z, mask)
        return pltpu.make_async_copy(
            result_ref.at[me, block], back_ref.at[block, me], keep.at[mask]
        )

    def issue(mask):
        for step in range(1, plane):
            outward(mask, step).start()
        keep_own(mask).start()

    def to_line(mask):
        block = flip(z, mask)
        return remote(
            sum_ref.at[block],
            routed_ref.at[z],
            line_send.at[mask],
            line_recv.at[mask],
            groups.device("outer", block),
        )

    def from_line(mask):
        block = routed_ref.at[flip(z, mask)]
        return remote(
            block,
            block,
            line_send.at[mask],
            line_recv.at[mask],
            groups.device("outer", flip(z, mask)),
        )

    def to_side(step):
        peer = (t + step) % n_tp
        return remote(
            shared_ref.at[peer],
            parts_ref.at[t],
            tp_send.at[step],
            tp_recv.at[step],
            groups.device("tp", peer),
        )

    def from_side(step):
        peer = (t + n_tp - step) % n_tp
        block = parts_ref.at[peer]
        return remote(
            block, block, tp_send.at[step], tp_recv.at[step], groups.device("tp", peer)
        )

    own_shared = pltpu.make_async_copy(shared_ref.at[t], parts_ref.at[t], keep.at[outer])
    own_shared.start()
    masks = list(range(outer - 1, -1, -1))
    for mask in masks[:2]:
        issue(mask)
    for number, mask in enumerate(masks):
        keep_own(mask).wait()
        for step in range(1, plane):
            inward(mask, step).wait_recv()
        if number + 2 < len(masks):
            issue(masks[number + 2])
        if number + 2 == len(masks) or len(masks) == 1:
            for step in range(1, n_tp):
                to_side(step).start()
        block = flip(z, mask)
        rows = back_ref[block].astype(jnp.float32)
        rows = rows.reshape(mix_ref.shape[2], rows.shape[-1]).astype(jnp.bfloat16)
        sum_ref[block] = jnp.dot(
            mix_ref[block], rows, preferred_element_type=jnp.float32
        ).astype(jnp.bfloat16)
        if mask:
            to_line(mask).start()
    own_sum = pltpu.make_async_copy(sum_ref.at[z], routed_ref.at[z], keep.at[outer + 1])
    own_sum.start()
    for mask in masks:
        for step in range(1, plane):
            outward(mask, step).wait_send()
        if mask:
            to_line(mask).wait_send()
            from_line(mask).wait_recv()
    for step in range(1, n_tp):
        to_side(step).wait_send()
        from_side(step).wait_recv()
    own_shared.wait()
    own_sum.wait()


def combine_rows(groups, collective_id, result, mix, shared):
    outer, plane, n_tp = groups.outer, groups.plane, groups.n_tp
    dma, kind = pltpu.SemaphoreType.DMA, result.dtype
    seats, width = result.shape[2:]
    vmem, anywhere = pl.BlockSpec(memory_space=pltpu.VMEM), pl.BlockSpec(memory_space=pl.ANY)
    return pl.pallas_call(
        functools.partial(combine_kernel, groups),
        out_shape=(
            jax.ShapeDtypeStruct((outer, mix.shape[1], width), kind),
            jax.ShapeDtypeStruct(shared.shape, kind),
        ),
        in_specs=[anywhere, vmem, anywhere],
        out_specs=(anywhere, anywhere),
        scratch_shapes=[
            pltpu.VMEM((outer, plane, seats, width), kind),
            pltpu.VMEM((outer, mix.shape[1], width), kind),
            dma((outer, plane)),
            dma((outer, plane)),
            dma((outer,)),
            dma((outer,)),
            dma((n_tp,)),
            dma((n_tp,)),
            dma((outer + 2,)),
        ],
        compiler_params=pltpu.CompilerParams(collective_id=collective_id, has_side_effects=True),
        name="combine_rows",
    )(result, mix, shared)


def layer_kernel(
    groups,
    chunks,
    seats,
    heads_narrow,
    heads_broad,
    ids_ref,
    strength_ref,
    gain_ref,
    project_narrow,
    project_broad,
    residual_ref,
    gate_ref,
    up_ref,
    down_ref,
    shared_gate_ref,
    shared_up_ref,
    shared_down_ref,
    out_ref,
    wp_narrow,
    wp_broad,
    w_gate,
    w_up,
    w_down,
    ws_gate,
    ws_up,
    ws_down,
    rows_own,
    notes,
    select,
    mixer,
    stream,
    tok,
    inbox,
    asked,
    acc_gate,
    acc_up,
    hidden,
    acc_sgate,
    acc_sup,
    shared_hidden,
    back,
    answer,
    parts,
    from_partner,
    kept,
    to_peer,
    from_peer,
    to_owner,
    from_owner,
    final,
    load_sem,
    note_send,
    note_recv,
    z_send,
    z_recv,
    x_send,
    x_recv,
    p_send,
    p_recv,
    y_send,
    y_recv,
    r_send,
    r_recv,
    d_send,
    d_recv,
    s_send,
    s_recv,
    o_send,
    o_recv,
):
    outer, inner, n_tp = groups.outer, groups.inner, groups.n_tp
    z, y, t = groups.place()
    pairs = n_tp // 2
    high, low = t // 2, t % 2
    width = gain_ref.shape[1]
    span = width // chunks
    units = outer * chunks
    count = rows_own.shape[0]
    group_rows = n_tp * count
    seat_rows = n_tp * seats
    bf16, f32 = jnp.bfloat16, jnp.float32
    partner = (z * inner + y, high * 2 + 1 - low)

    def remote(source, target, send, recv, device):
        return pltpu.make_async_remote_copy(
            src_ref=source,
            dst_ref=target,
            send_sem=send,
            recv_sem=recv,
            device_id=device,
            device_id_type=MESH,
        )

    def columns(piece):
        return pl.ds(pl.multiple_of(piece * span, span), span)

    def load(index):
        if index < chunks:
            return (
                pltpu.make_async_copy(
                    project_narrow.at[:, columns(index)], wp_narrow.at[index], load_sem.at[index, 0]
                ),
                pltpu.make_async_copy(
                    project_broad.at[:, columns(index)], wp_broad.at[index], load_sem.at[index, 1]
                ),
            )
        if index == chunks:
            first = pl.multiple_of(t * count, count)
            return (
                pltpu.make_async_copy(
                    residual_ref.at[pl.ds(first, count), :], rows_own, load_sem.at[index, 0]
                ),
            )
        if index == chunks + 1:
            return (
                pltpu.make_async_copy(gate_ref.at[0], w_gate, load_sem.at[index, 0]),
                pltpu.make_async_copy(up_ref.at[0], w_up, load_sem.at[index, 1]),
            )
        if index == chunks + 2:
            return (
                pltpu.make_async_copy(shared_gate_ref, ws_gate, load_sem.at[index, 0]),
                pltpu.make_async_copy(shared_up_ref, ws_up, load_sem.at[index, 1]),
            )
        return (
            pltpu.make_async_copy(down_ref.at[0], w_down, load_sem.at[index, 0]),
            pltpu.make_async_copy(shared_down_ref, ws_down, load_sem.at[index, 1]),
        )

    for index in range(chunks + 4):
        for copy in load(index):
            copy.start()

    barrier = pltpu.get_barrier_semaphore()
    greeted = 0
    for far in range(outer):
        for step in range(n_tp):
            if far or step:
                pl.semaphore_signal(
                    barrier,
                    inc=1,
                    device_id=(((z + far) % outer) * inner + y, (t + step) % n_tp),
                    device_id_type=MESH,
                )
                greeted += 1
    for step in range(1, inner):
        pl.semaphore_signal(
            barrier, inc=1, device_id=(z * inner + (y + step) % inner, t), device_id_type=MESH
        )
        greeted += 1
    pl.semaphore_wait(barrier, greeted)

    def note(far, step):
        number = far * n_tp + step
        return remote(
            notes.at[z, t],
            notes.at[z, t],
            note_send.at[number],
            note_recv.at[number],
            (((z + far) % outer) * inner + y, (t + step) % n_tp),
        )

    others = [(far, step) for far in range(outer) for step in range(n_tp) if far or step]
    notes[z, t, 0] = ids_ref[...].astype(f32)
    notes[z, t, 1] = strength_ref[...].astype(bf16).astype(f32)
    for far, step in others:
        note(far, step).start()

    def across(unit):
        return remote(
            parts.at[unit, 1 - low],
            from_partner.at[unit],
            d_send.at[unit],
            d_recv.at[unit],
            partner,
        )

    def sideways(unit, step):
        return remote(
            to_peer.at[unit, step - 1],
            from_peer.at[unit, step - 1],
            s_send.at[unit, step - 1],
            s_recv.at[unit, step - 1],
            (z * inner + y, ((high + step) % pairs) * 2 + low),
        )

    def reduce_start(unit, value):
        for place in range(n_tp):
            parts[unit, place % 2, place // 2] = value[
                place * count : (place + 1) * count
            ].astype(bf16)
        across(unit).start()

    def reduce_pass(unit):
        across(unit).wait_recv()
        for step in range(1, pairs):
            other = (high + step) % pairs
            to_peer[unit, step - 1] = (
                parts[unit, low, other].astype(f32) + from_partner[unit, other].astype(f32)
            ).astype(bf16)
            sideways(unit, step).start()
        kept[unit] = parts[unit, low, high].astype(f32) + from_partner[unit, high].astype(f32)

    def reduce_end(unit):
        total = kept[unit]
        for step in range(1, pairs):
            sideways(unit, step).wait_recv()
            total = total + from_peer[unit, step - 1].astype(f32)
        return total

    for piece in range(chunks):
        for copy in load(piece):
            copy.wait()
        value = jnp.dot(heads_narrow[...], wp_narrow[piece], preferred_element_type=f32)
        value = value + jnp.dot(heads_broad[...], wp_broad[piece], preferred_element_type=f32)
        reduce_start(piece, value)
        if piece:
            reduce_pass(piece - 1)
    reduce_pass(chunks - 1)

    for far, step in others:
        note(far, step).wait_recv()
    lanes = mixer.shape[2]
    token = lax.broadcasted_iota(jnp.int32, (group_rows, lanes), 0)
    lane = lax.broadcasted_iota(jnp.int32, (group_rows, lanes), 1)
    token_before = lax.broadcasted_iota(jnp.int32, (group_rows, group_rows), 1)
    token_after = lax.broadcasted_iota(jnp.int32, (group_rows, group_rows), 0)
    earlier = (token_before < token_after) & (token_before // count == token_after // count)
    earlier = jnp.where(earlier, 1.0, 0.0).astype(bf16)
    seat_block = lane // seat_rows
    seat_place = (lane % seat_rows) // seats
    seat_number = (lane % seats).astype(f32)
    for block in range(outer):
        names = notes[block, :, 0].reshape(group_rows, notes.shape[4])
        loads = notes[block, :, 1].reshape(group_rows, notes.shape[4])
        chosen = jnp.zeros((group_rows, lanes), f32)
        strength = jnp.zeros((group_rows, lanes), f32)
        for step in range(inner):
            expert = ((z * inner + (y + step) % inner) * n_tp + t).astype(f32)
            match = names == expert
            here = seat_block == step
            taken = jnp.sum(jnp.where(match, 1.0, 0.0), axis=1, keepdims=True)
            load_of = jnp.sum(jnp.where(match, loads, 0.0), axis=1, keepdims=True)
            chosen = jnp.where(here, taken, chosen)
            strength = jnp.where(here, load_of, strength)
        rank = jnp.dot(earlier, chosen.astype(bf16), preferred_element_type=f32)
        seated = (chosen > 0.5) & (rank == seat_number) & (seat_place == token // count)
        mixer[block] = jnp.where(seated, strength, 0.0).astype(bf16)
        select[block] = jnp.transpose(jnp.where(seated, 1.0, 0.0)).astype(bf16)

    for copy in load(chunks):
        copy.wait()
    square = jnp.zeros((count, 1), f32)
    for piece in range(chunks):
        value = reduce_end(piece) + rows_own[:, piece * span : (piece + 1) * span].astype(f32)
        stream[piece] = value
        square = square + jnp.sum(value * value, axis=1, keepdims=True)
    scale = lax.rsqrt(square * (1.0 / width) + norm_epsilon)
    for piece in range(chunks):
        gain = gain_ref[:, piece * span : (piece + 1) * span]
        tok[z, piece, t] = (stream[piece] * scale * gain).astype(bf16)
    for index in range(chunks + 1, chunks + 3):
        for copy in load(index):
            copy.wait()

    def block_at(far):
        value, bit = 0, 1
        while bit < outer:
            value = value + bit * ((z // bit + far // bit) % 2)
            bit *= 2
        return value

    def along(block, piece, direction):
        return remote(
            tok.at[block, piece, t],
            tok.at[block, piece, t],
            z_send.at[block, piece, (direction + 1) // 2],
            z_recv.at[block, piece],
            ((z + direction) * inner + y, t),
        )

    def to_chip(block, piece, step):
        return remote(
            tok.at[block, piece, t],
            tok.at[block, piece, t],
            x_send.at[block, piece, step - 1],
            x_recv.at[block, piece, step - 1],
            (z * inner + y, ((high + step) % pairs) * 2 + low),
        )

    def from_chip(block, piece, step):
        place = tok.at[block, piece, ((high + pairs - step) % pairs) * 2 + low]
        return remote(
            place,
            place,
            x_send.at[block, piece, step - 1],
            x_recv.at[block, piece, step - 1],
            (z * inner + y, ((high + step) % pairs) * 2 + low),
        )

    def to_partner(block, piece, step):
        place = tok.at[block, piece, ((high + pairs - step) % pairs) * 2 + low]
        return remote(
            place, place, p_send.at[block, piece, step], p_recv.at[block, piece, step], partner
        )

    def from_other_core(block, piece, step):
        place = tok.at[block, piece, ((high + pairs - step) % pairs) * 2 + 1 - low]
        return remote(
            place, place, p_send.at[block, piece, step], p_recv.at[block, piece, step], partner
        )

    def ask(block, piece, step):
        return remote(
            asked.at[block, piece, step - 1],
            inbox.at[block, piece, step],
            y_send.at[block, piece, step - 1],
            y_recv.at[block, piece, step - 1],
            (z * inner + (y + step) % inner, t),
        )

    def reply(block, piece, step):
        return remote(
            answer.at[block, piece, step - 1],
            back.at[block, piece, step],
            r_send.at[block, piece, step - 1],
            r_recv.at[block, piece, step - 1],
            (z * inner + (y + inner - step) % inner, t),
        )

    def to_line(block, piece):
        return remote(
            to_owner.at[block, piece],
            from_owner.at[z, piece],
            o_send.at[block, piece],
            o_recv.at[z, piece],
            (block * inner + y, t),
        )

    def from_line(block, piece):
        return remote(
            from_owner.at[block, piece],
            from_owner.at[block, piece],
            o_send.at[block, piece],
            o_recv.at[block, piece],
            (block * inner + y, t),
        )

    directions = ((1, z < outer - 1), (-1, z > 0))

    def arrive(unit):
        far, piece = unit // chunks, unit % chunks
        for direction, onward in directions:
            block = z - direction * far
            present = (block >= 0) & (block < outer)

            @pl.when(present & (far > 0))
            def _(block=block, direction=direction):
                along(block, piece, direction).wait_recv()

            @pl.when(present & onward)
            def _(block=block, direction=direction):
                along(block, piece, direction).start()

        block = block_at(far)
        for step in range(1, pairs):
            to_chip(block, piece, step).start()
        to_partner(block, piece, 0).start()

    def spread(unit):
        block, piece = block_at(unit // chunks), unit % chunks
        for step in range(1, pairs):
            from_chip(block, piece, step).wait_recv()
            to_partner(block, piece, step).start()

    def choose(unit):
        block, piece = block_at(unit // chunks), unit % chunks
        for step in range(pairs):
            from_other_core(block, piece, step).wait_recv()
        rows = tok[block, piece].reshape(group_rows, span)
        picked = jnp.dot(
            select[block, : inner * seat_rows], rows, preferred_element_type=f32
        ).astype(bf16)
        for step in range(1, inner):
            asked[block, piece, step - 1] = picked[step * seat_rows : (step + 1) * seat_rows]
            ask(block, piece, step).start()
        inbox[block, piece, 0] = picked[:seat_rows]

    def expand(unit):
        far = unit // chunks
        block, piece = block_at(far), unit % chunks
        for step in range(1, inner):
            ask(block, piece, step).wait_recv()
        rows = inbox[block, piece].reshape(inner * seat_rows, span)
        part_gate = jnp.dot(rows, w_gate[columns(piece), :], preferred_element_type=f32)
        part_up = jnp.dot(rows, w_up[columns(piece), :], preferred_element_type=f32)

        @pl.when(piece == 0)
        def _():
            acc_gate[...] = part_gate
            acc_up[...] = part_up

        @pl.when(piece > 0)
        def _():
            acc_gate[...] += part_gate
            acc_up[...] += part_up

        @pl.when(piece == chunks - 1)
        def _():
            hidden[block] = (jax.nn.silu(acc_gate[...]) * acc_up[...]).astype(bf16)

    def expand_shared(piece):
        rows = tok[z, piece].reshape(group_rows, span)
        part_gate = jnp.dot(rows, ws_gate[columns(piece), :], preferred_element_type=f32)
        part_up = jnp.dot(rows, ws_up[columns(piece), :], preferred_element_type=f32)

        @pl.when(piece == 0)
        def _():
            acc_sgate[...] = part_gate
            acc_sup[...] = part_up

        @pl.when(piece > 0)
        def _():
            acc_sgate[...] += part_gate
            acc_sup[...] += part_up

        @pl.when(piece == chunks - 1)
        def _():
            shared_hidden[...] = (jax.nn.silu(acc_sgate[...]) * acc_sup[...]).astype(bf16)

    def within(number, first, last):
        return (number >= first) & (number < last)

    late_spread, late_choose, late_expand = DISPATCH_LAGS

    def outward(unit, carried):
        pl.when(within(unit, 0, units))(lambda: arrive(unit))
        one = unit - late_spread
        pl.when(within(one, 0, units))(lambda: spread(one))
        two = unit - late_choose
        pl.when(within(two, 0, units))(lambda: choose(two))
        pl.when(within(two, 0, chunks))(lambda: expand_shared(two))
        three = unit - late_expand
        pl.when(within(three, 0, units))(lambda: expand(three))
        return carried

    lax.fori_loop(0, units + late_expand, outward, 0)
    for copy in load(chunks + 3):
        copy.wait()

    def back_unit(unit):
        far = outer - 1 - unit // chunks
        return far, block_at(far), unit % chunks

    def produce(unit):
        far, block, piece = back_unit(unit)
        made = jnp.dot(hidden[block], w_down[:, columns(piece)], preferred_element_type=f32)
        made = made.astype(bf16)
        for step in range(1, inner):
            answer[block, piece, step - 1] = made[step * seat_rows : (step + 1) * seat_rows]
            reply(block, piece, step).start()
        back[block, piece, 0] = made[:seat_rows]

    def blend(unit):
        far, block, piece = back_unit(unit)
        for step in range(1, inner):
            reply(block, piece, step).wait_recv()
        rows = back[block, piece].reshape(inner * seat_rows, span)
        value = jnp.dot(
            mixer[block][:, : inner * seat_rows], rows, preferred_element_type=f32
        )

        @pl.when(far > 0)
        def _():
            reduce_start(chunks + unit, value)

        @pl.when(far == 0)
        def _():
            shared_part = jnp.dot(
                shared_hidden[...], ws_down[:, columns(piece)], preferred_element_type=f32
            )
            reduce_start(chunks + unit, value + shared_part)

    def deliver(unit):
        far, block, piece = back_unit(unit)
        total = reduce_end(chunks + unit)

        @pl.when(far > 0)
        def _():
            to_owner[block, piece] = total.astype(bf16)
            to_line(block, piece).start()

        @pl.when(far == 0)
        def _():
            final[piece] = total

    late_blend, late_pass, late_deliver = COMBINE_LAGS

    def inward(unit, carried):
        pl.when(within(unit, 0, units))(lambda: produce(unit))
        one = unit - late_blend
        pl.when(within(one, 0, units))(lambda: blend(one))
        two = unit - late_pass
        pl.when(within(two, 0, units))(lambda: reduce_pass(chunks + two))
        three = unit - late_deliver
        pl.when(within(three, 0, units))(lambda: deliver(three))
        return carried

    lax.fori_loop(0, units + late_deliver, inward, 0)

    for piece in range(chunks):
        total = stream[piece] + final[piece]
        for far in range(1, outer):
            block = block_at(far)
            from_line(block, piece).wait_recv()
            total = total + from_owner[block, piece].astype(f32)
        out_ref[:, piece * span : (piece + 1) * span] = total.astype(bf16)

    for far, step in others:
        note(far, step).wait_send()

    def drain(unit, carried):
        block, piece = unit // chunks, unit % chunks
        for direction, onward in directions:
            has = (block <= z) if direction > 0 else (block >= z)

            @pl.when(has & onward)
            def _(direction=direction):
                along(block, piece, direction).wait_send()

        for step in range(1, pairs):
            to_chip(block, piece, step).wait_send()
        for step in range(pairs):
            to_partner(block, piece, step).wait_send()
        for step in range(1, inner):
            ask(block, piece, step).wait_send()
            reply(block, piece, step).wait_send()
        pl.when(block != z)(lambda: to_line(block, piece).wait_send())
        return carried

    lax.fori_loop(0, units, drain, 0)

    def drain_sums(unit, carried):
        across(unit).wait_send()
        for step in range(1, pairs):
            sideways(unit, step).wait_send()
        return carried

    lax.fori_loop(0, chunks + units, drain_sums, 0)


DISPATCH_LAGS = (3, 4, 7)
COMBINE_LAGS = (3, 4, 7)


def layer_rows(
    groups,
    collective_id,
    seats,
    heads_narrow,
    heads_broad,
    project_narrow,
    project_broad,
    residual,
    norm_gain,
    route_ids,
    route_weight,
    expert_gate,
    expert_up,
    expert_down,
    shared_gate,
    shared_up,
    shared_down,
):
    outer, inner, n_tp = groups.outer, groups.inner, groups.n_tp
    dma = pltpu.SemaphoreType.DMA
    width = residual.shape[1]
    chunks = width // math.gcd(width, 1024)
    span = width // chunks
    count, top = route_ids.shape
    group_rows = n_tp * count
    seat_rows = n_tp * seats
    pairs = n_tp // 2
    units = outer * chunks
    sums = chunks + units
    lanes = -(-inner * seat_rows // 128) * 128
    bf16, f32 = jnp.bfloat16, jnp.float32
    expert_width, shared_width = expert_gate.shape[2], shared_gate.shape[1]
    vmem, anywhere = pl.BlockSpec(memory_space=pltpu.VMEM), pl.BlockSpec(memory_space=pl.ANY)
    return pl.pallas_call(
        functools.partial(layer_kernel, groups, chunks, seats),
        out_shape=jax.ShapeDtypeStruct((count, width), bf16),
        in_specs=[vmem] * 5 + [anywhere] * 9,
        out_specs=vmem,
        scratch_shapes=[
            pltpu.VMEM((chunks, project_narrow.shape[0], span), bf16),
            pltpu.VMEM((chunks, project_broad.shape[0], span), bf16),
            pltpu.VMEM((width, expert_width), bf16),
            pltpu.VMEM((width, expert_width), bf16),
            pltpu.VMEM((expert_width, width), bf16),
            pltpu.VMEM((width, shared_width), bf16),
            pltpu.VMEM((width, shared_width), bf16),
            pltpu.VMEM((shared_width, width), bf16),
            pltpu.VMEM((count, width), bf16),
            pltpu.VMEM((outer, n_tp, 2, count, top), f32),
            pltpu.VMEM((outer, lanes, group_rows), bf16),
            pltpu.VMEM((outer, group_rows, lanes), bf16),
            pltpu.VMEM((chunks, count, span), f32),
            pltpu.VMEM((outer, chunks, n_tp, count, span), bf16),
            pltpu.VMEM((outer, chunks, inner, seat_rows, span), bf16),
            pltpu.VMEM((outer, chunks, inner - 1, seat_rows, span), bf16),
            pltpu.VMEM((inner * seat_rows, expert_width), f32),
            pltpu.VMEM((inner * seat_rows, expert_width), f32),
            pltpu.VMEM((outer, inner * seat_rows, expert_width), bf16),
            pltpu.VMEM((group_rows, shared_width), f32),
            pltpu.VMEM((group_rows, shared_width), f32),
            pltpu.VMEM((group_rows, shared_width), bf16),
            pltpu.VMEM((outer, chunks, inner, seat_rows, span), bf16),
            pltpu.VMEM((outer, chunks, inner - 1, seat_rows, span), bf16),
            pltpu.VMEM((sums, 2, pairs, count, span), bf16),
            pltpu.VMEM((sums, pairs, count, span), bf16),
            pltpu.VMEM((sums, count, span), f32),
            pltpu.VMEM((sums, pairs - 1, count, span), bf16),
            pltpu.VMEM((sums, pairs - 1, count, span), bf16),
            pltpu.VMEM((outer, chunks, count, span), bf16),
            pltpu.VMEM((outer, chunks, count, span), bf16),
            pltpu.VMEM((chunks, count, span), f32),
            dma((chunks + 4, 2)),
            dma((outer * n_tp,)),
            dma((outer * n_tp,)),
            dma((outer, chunks, 2)),
            dma((outer, chunks)),
            dma((outer, chunks, pairs - 1)),
            dma((outer, chunks, pairs - 1)),
            dma((outer, chunks, pairs)),
            dma((outer, chunks, pairs)),
            dma((outer, chunks, inner - 1)),
            dma((outer, chunks, inner - 1)),
            dma((outer, chunks, inner - 1)),
            dma((outer, chunks, inner - 1)),
            dma((sums,)),
            dma((sums,)),
            dma((sums, pairs - 1)),
            dma((sums, pairs - 1)),
            dma((outer, chunks)),
            dma((outer, chunks)),
        ],
        compiler_params=pltpu.CompilerParams(
            collective_id=collective_id, has_side_effects=True, vmem_limit_bytes=62 * 2**20
        ),
        name="layer_rows",
    )(
        heads_narrow,
        heads_broad,
        route_ids,
        route_weight,
        norm_gain.reshape(1, width),
        project_narrow,
        project_broad,
        residual,
        expert_gate,
        expert_up,
        expert_down,
        shared_gate,
        shared_up,
        shared_down,
    )


def local(
    groups,
    query_narrow,
    key_narrow,
    value_narrow,
    gates_narrow,
    query_broad,
    key_broad,
    value_broad,
    gates_broad,
    project_narrow,
    project_broad,
    residual,
    norm_gain,
    route_ids,
    route_weight,
    expert_gate,
    expert_up,
    expert_down,
    shared_gate,
    shared_up,
    shared_down,
):
    tokens = query_narrow.shape[0]
    notes = jnp.concatenate(
        [
            route_ids.astype(jnp.float32).T,
            route_weight.astype(jnp.bfloat16).astype(jnp.float32).T,
        ],
        axis=0,
    )
    own_pairs = jnp.concatenate([key_narrow, key_broad, value_narrow, value_broad], axis=1)
    all_pairs, all_notes = gather(groups, 0, own_pairs, notes)
    all_pairs = all_pairs.reshape(-1, own_pairs.shape[1])
    vmem = pl.BlockSpec(memory_space=pltpu.VMEM)
    heads_out = pl.pallas_call(
        attend_kernel,
        out_shape=(
            jax.ShapeDtypeStruct(query_narrow.shape, jnp.bfloat16),
            jax.ShapeDtypeStruct(query_broad.shape, jnp.bfloat16),
        ),
        in_specs=[vmem] * 7,
        out_specs=(vmem, vmem),
        name="attend",
    )(
        query_narrow,
        query_broad,
        gates_narrow,
        gates_broad,
        gates_narrow.T,
        gates_broad.T,
        all_pairs,
    )
    n_tp, inner = groups.n_tp, groups.inner
    spots = 2 * route_ids.size // (groups.n_sp * n_tp * expert_gate.shape[0])
    if spots % 8 == 0 and n_tp == 4 and inner == 2 and expert_gate.shape[0] == 1:
        return layer_rows(
            groups,
            1,
            spots,
            heads_out[0],
            heads_out[1],
            project_narrow,
            project_broad,
            residual,
            norm_gain,
            route_ids,
            route_weight,
            expert_gate,
            expert_up,
            expert_down,
            shared_gate,
            shared_up,
            shared_down,
        )
    partial_value = jnp.dot(heads_out[0], project_narrow, preferred_element_type=jnp.float32)
    partial_value = partial_value + jnp.dot(
        heads_out[1], project_broad, preferred_element_type=jnp.float32
    )
    n_tp, outer, plane = groups.n_tp, groups.outer, groups.plane
    sub_rows, width = route_ids.shape[0], residual.shape[1]
    (portions,) = swap(
        groups, 1, (partial_value.astype(jnp.bfloat16).reshape(n_tp, sub_rows, width), "tp", 0, 0)
    )
    stream, own_normed = pl.pallas_call(
        norm_kernel,
        out_shape=(
            jax.ShapeDtypeStruct((sub_rows, width), jnp.float32),
            jax.ShapeDtypeStruct((sub_rows, width), jnp.bfloat16),
        ),
        in_specs=[vmem] * 3,
        out_specs=(vmem, vmem),
        name="norm",
    )(portions, residual, norm_gain.reshape(1, width))
    top_count = route_ids.shape[1]
    local_experts = expert_gate.shape[0]
    expert_total = groups.n_sp * n_tp * local_experts
    capacity = 2 * sub_rows * top_count // expert_total
    seat_rows = local_experts * capacity
    fused = seat_rows % 8 == 0 and n_tp % 2 == 0
    plane_experts = plane * local_experts
    first_expert = groups.mine("outer") * plane_experts
    line_ids = all_notes[:, :top_count].astype(jnp.int32)
    line_weights = all_notes[:, top_count:]
    named = (
        line_ids[:, None]
        == first_expert + jnp.arange(plane_experts, dtype=jnp.int32)[None, :, None, None]
    )
    chosen = jnp.any(named, axis=2)
    strength = jnp.sum(jnp.where(named, line_weights[:, None], 0.0), axis=2)
    before = jnp.arange(sub_rows)[:, None] < jnp.arange(sub_rows)[None, :]
    rank = jnp.sum(jnp.where(chosen[:, :, :, None] & before, 1, 0), axis=2)
    seats = chosen[:, :, None, :] & (
        rank[:, :, None, :] == jnp.arange(capacity, dtype=jnp.int32)[None, None, :, None]
    )
    dispatch = seats.astype(jnp.bfloat16).reshape(outer, plane_experts * capacity, sub_rows)
    combiner = (
        jnp.where(seats, strength[:, :, None, :], 0.0)
        .astype(jnp.bfloat16)
        .reshape(outer, plane_experts * capacity, sub_rows)
    )
    if fused:
        normed, inbound = dispatch_rows(groups, 2, own_normed, dispatch, seat_rows)
    else:
        normed, line_normed = swap(
            groups, 2, (own_normed, "tp", None, 0), (own_normed, "outer", None, 0)
        )
        outbound = jnp.einsum("zct,ztd->zcd", dispatch, line_normed, preferred_element_type=jnp.float32)
        outbound = outbound.astype(jnp.bfloat16).reshape(
            outer, plane, local_experts * capacity, width
        )
        (inbound,) = swap(groups, 3, (outbound, "plane", 1, 0))
    normed = normed.reshape(tokens, width)
    grouped = inbound.reshape(plane * outer, local_experts, capacity, width)
    gate_out = jnp.einsum(
        "secd,edh->sech", grouped, expert_gate, preferred_element_type=jnp.float32
    )
    up_out = jnp.einsum("secd,edh->sech", grouped, expert_up, preferred_element_type=jnp.float32)
    hidden = (jax.nn.silu(gate_out) * up_out).astype(jnp.bfloat16)
    result = jnp.einsum(
        "sech,ehd->secd", hidden, expert_down, preferred_element_type=jnp.float32
    ).astype(jnp.bfloat16)
    shared_hidden = (
        jax.nn.silu(jnp.dot(normed, shared_gate, preferred_element_type=jnp.float32))
        * jnp.dot(normed, shared_up, preferred_element_type=jnp.float32)
    ).astype(jnp.bfloat16)
    shared_out = jnp.dot(shared_hidden, shared_down, preferred_element_type=jnp.float32).astype(
        jnp.bfloat16
    )
    shared_out = shared_out.reshape(n_tp, sub_rows, width)
    if fused:
        routed_parts, shared_parts = combine_rows(
            groups, 4, result.reshape(inbound.shape), combiner.transpose(0, 2, 1), shared_out
        )
    else:
        (returned,) = swap(groups, 4, (result.reshape(inbound.shape), "plane", 0, 1))
        returned = returned.reshape(outer, plane_experts * capacity, width)
        line_routed = jnp.einsum(
            "zct,zcd->ztd", combiner, returned, preferred_element_type=jnp.float32
        ).astype(jnp.bfloat16)
        routed_parts, shared_parts = swap(
            groups,
            5,
            (line_routed, "outer", 0, 0),
            (shared_out, "tp", 0, 0),
        )
    tile = math.gcd(width, 1024)
    return pl.pallas_call(
        add_kernel,
        grid=(width // tile,),
        out_shape=jax.ShapeDtypeStruct((sub_rows, width), jnp.bfloat16),
        in_specs=[
            pl.BlockSpec((sub_rows, tile), lambda i: (0, i)),
            pl.BlockSpec((n_tp, sub_rows, tile), lambda i: (0, 0, i)),
            pl.BlockSpec((outer, sub_rows, tile), lambda i: (0, 0, i)),
        ],
        out_specs=pl.BlockSpec((sub_rows, tile), lambda i: (0, i)),
        name="add_parts",
    )(stream, shared_parts, routed_parts)


def solution(mesh):
    placed = (
        P("sp", "tp"),
        P("sp", "tp"),
        P("sp", "tp"),
        P(None, "tp"),
        P("sp", "tp"),
        P("sp", "tp"),
        P("sp", "tp"),
        P(None, "tp"),
        P("tp", None),
        P("tp", None),
        P("sp", None),
        P(),
        P(("sp", "tp"), None),
        P(("sp", "tp"), None),
        P(("sp", "tp"), None, None),
        P(("sp", "tp"), None, None),
        P(("sp", "tp"), None, None),
        P(None, "tp"),
        P(None, "tp"),
        P("tp", None),
    )
    groups = Groups(mesh.shape["sp"], mesh.shape["tp"])
    return jax.shard_map(
        functools.partial(local, groups), mesh=mesh, in_specs=placed, out_specs=P(("sp", "tp"), None), check_vma=False
    )
```

```python
import functools
import math

import jax
import jax.numpy as jnp
from jax import lax
from jax.experimental import pallas as pl
from jax.experimental.pallas import tpu as pltpu
from jax.sharding import PartitionSpec as P

MESH = pl.DeviceIdType.MESH

NARROW_SIZE = 128
BROAD_SIZE = 256


norm_epsilon = 1e-06


def attend_kernel(
    q_narrow, q_broad, g_narrow, g_broad, k_narrow, k_broad, pairs_ref, o_narrow, o_broad
):
    tokens, length = q_narrow.shape[0], pairs_ref.shape[0]
    first_row = lax.axis_index("sp") * tokens
    key_place = lax.broadcasted_iota(jnp.int32, (tokens, length), 1)
    query_place = first_row + lax.broadcasted_iota(jnp.int32, (tokens, length), 0)
    allowed = key_place <= query_place
    rows = pl.ds(pl.multiple_of(first_row, tokens), tokens)
    value_first = pairs_ref.shape[1] // 2
    column = 0
    for queries, gates, key_gates, outputs, head_size in (
        (q_narrow, g_narrow, k_narrow, o_narrow, NARROW_SIZE),
        (q_broad, g_broad, k_broad, o_broad, BROAD_SIZE),
    ):
        heads = queries.shape[1] // head_size
        widest = value_first * head_size // (NARROW_SIZE + BROAD_SIZE)
        group_size = heads * head_size // widest
        own_gates = gates[rows, :]
        for kv in range(widest // head_size):
            keys = pairs_ref[:, column : column + head_size]
            values = pairs_ref[:, value_first + column : value_first + column + head_size]
            reachable = (
                lax.broadcasted_iota(jnp.int32, (length, head_size), 0) < first_row + tokens
            )
            values = jnp.where(reachable, values.astype(jnp.float32), 0.0).astype(jnp.bfloat16)
            column += head_size
            for member in range(group_size):
                head = kv * group_size + member
                span = slice(head * head_size, (head + 1) * head_size)
                scores = lax.dot_general(
                    queries[:, span],
                    keys,
                    (((1,), (1,)), ((), ())),
                    preferred_element_type=jnp.float32,
                )
                scores = scores * head_size ** (-0.5)
                scores = scores + own_gates[:, head : head + 1] - key_gates[head : head + 1, :]
                scores = jnp.where(allowed, scores, -jnp.inf)
                weights = jnp.exp(scores - jnp.max(scores, axis=1, keepdims=True))
                total = jnp.sum(weights, axis=1, keepdims=True)
                blended = jnp.dot(
                    weights.astype(jnp.bfloat16), values, preferred_element_type=jnp.float32
                )
                outputs[:, span] = (blended / total).astype(jnp.bfloat16)


def add_kernel(stream_ref, shared_ref, routed_ref, out_ref):
    total = stream_ref[...]
    for parts in (shared_ref, routed_ref):
        for index in range(parts.shape[0]):
            total = total + parts[index].astype(jnp.float32)
    out_ref[...] = total.astype(jnp.bfloat16)


def norm_kernel(portions_ref, residual_ref, gain_ref, stream_ref, normed_ref):
    count = stream_ref.shape[0]
    first = lax.axis_index("tp") * count
    stream = residual_ref[pl.ds(pl.multiple_of(first, count), count), :].astype(jnp.float32)
    for index in range(portions_ref.shape[0]):
        stream = stream + portions_ref[index].astype(jnp.float32)
    stream_ref[...] = stream
    scale = lax.rsqrt(jnp.mean(stream * stream, axis=1, keepdims=True) + norm_epsilon)
    normed_ref[...] = (stream * scale * gain_ref[...]).astype(jnp.bfloat16)


class Groups:
    def __init__(self, n_sp, n_tp):
        self.n_sp, self.n_tp = n_sp, n_tp
        self.outer = math.gcd(n_sp, 4)
        self.inner = n_sp // self.outer
        self.plane = self.inner * n_tp

    def size(self, kind):
        return {"tp": self.n_tp, "outer": self.outer, "plane": self.plane}[kind]

    def place(self):
        sp, tp = lax.axis_index("sp"), lax.axis_index("tp")
        return sp // self.inner, sp % self.inner, tp

    def mine(self, kind):
        z, y, t = self.place()
        return {"tp": t, "outer": z, "plane": y * self.n_tp + t}[kind]

    def device(self, kind, index):
        z, y, t = self.place()
        if kind == "tp":
            return (z * self.inner + y, index)
        if kind == "outer":
            return (index * self.inner + y, t)
        return (z * self.inner + index // self.n_tp, index % self.n_tp)


def swap_kernel(groups, plans, *refs):
    count = len(plans)
    sources, targets, sems = refs[:count], refs[count : 2 * count], refs[2 * count :]
    barrier = pltpu.get_barrier_semaphore()
    greeted = 0
    for kind in sorted({plan[0] for plan in plans}):
        size, me = groups.size(kind), groups.mine(kind)
        for step in range(1, size):
            pl.semaphore_signal(
                barrier,
                inc=1,
                device_id=groups.device(kind, (me + step) % size),
                device_id_type=MESH,
            )
            greeted += 1
    pl.semaphore_wait(barrier, greeted)

    def cut(ref, axis, index):
        if axis is None:
            return ref
        return ref.at[index] if axis == 0 else ref.at[:, index]

    started, local_copies = [], []
    for number, (kind, source_axis, target_axis) in enumerate(plans):
        send, recv, keep = sems[3 * number : 3 * number + 3]
        size, me = groups.size(kind), groups.mine(kind)
        for step in range(1, size):
            peer = (me + step) % size
            copy = pltpu.make_async_remote_copy(
                src_ref=cut(sources[number], source_axis, peer),
                dst_ref=cut(targets[number], target_axis, me),
                send_sem=send.at[step],
                recv_sem=recv.at[step],
                device_id=groups.device(kind, peer),
                device_id_type=MESH,
            )
            copy.start()
            started.append(copy)
        own = pltpu.make_async_copy(
            cut(sources[number], source_axis, me), cut(targets[number], target_axis, me), keep
        )
        own.start()
        local_copies.append(own)
    for own in local_copies:
        own.wait()
    for copy in started:
        copy.wait()


def swap(groups, collective_id, *moves):
    plans, shapes, scratch = [], [], []
    for array, kind, source_axis, target_axis in moves:
        size = groups.size(kind)
        plans.append((kind, source_axis, target_axis))
        block = list(array.shape)
        if source_axis is not None:
            del block[source_axis]
        block.insert(target_axis, size)
        shapes.append(jax.ShapeDtypeStruct(tuple(block), array.dtype))
        scratch += [
            pltpu.SemaphoreType.DMA((size,)),
            pltpu.SemaphoreType.DMA((size,)),
            pltpu.SemaphoreType.DMA,
        ]
    return pl.pallas_call(
        functools.partial(swap_kernel, groups, tuple(plans)),
        out_shape=tuple(shapes),
        in_specs=[pl.BlockSpec(memory_space=pl.ANY)] * len(moves),
        out_specs=tuple([pl.BlockSpec(memory_space=pl.ANY)] * len(moves)),
        scratch_shapes=scratch,
        compiler_params=pltpu.CompilerParams(collective_id=collective_id, has_side_effects=True),
        name=f"swap_{collective_id}",
    )(*[move[0] for move in moves])


def gather_kernel(groups, own_ref, notes_ref, all_ref, all_notes_ref, *sems):
    line_send, line_recv, side_send, side_recv, note_send, note_recv, keep = sems
    outer, inner = groups.outer, groups.inner
    z, y, t = groups.place()
    barrier = pltpu.get_barrier_semaphore()
    for step in range(1, outer):
        pl.semaphore_signal(
            barrier, inc=1, device_id=groups.device("outer", (z + step) % outer), device_id_type=MESH
        )
    for step in range(1, inner):
        pl.semaphore_signal(
            barrier, inc=1, device_id=(z * inner + (y + step) % inner, t), device_id_type=MESH
        )
    pl.semaphore_wait(barrier, outer + inner - 2)

    def slot(far, side):
        return all_ref.at[(z - far) * inner + side]

    def upward(far):
        source = own_ref if far == 0 else slot(far, y)
        return pltpu.make_async_remote_copy(
            src_ref=source,
            dst_ref=slot(far, y),
            send_sem=line_send.at[far],
            recv_sem=line_recv.at[far + 1],
            device_id=((z + 1) * inner + y, t),
            device_id_type=MESH,
        )

    def sideways(far, step):
        source = own_ref if far == 0 else slot(far, y)
        return pltpu.make_async_remote_copy(
            src_ref=source,
            dst_ref=slot(far, y),
            send_sem=side_send.at[far, step],
            recv_sem=side_recv.at[far, step],
            device_id=(z * inner + (y + step) % inner, t),
            device_id_type=MESH,
        )

    def from_below(far):
        return pltpu.make_async_remote_copy(
            src_ref=slot(far, y),
            dst_ref=slot(far, y),
            send_sem=line_send.at[0],
            recv_sem=line_recv.at[far],
            device_id=((z + 1) * inner + y, t),
            device_id_type=MESH,
        )

    def from_side(far, step):
        side = (y + inner - step) % inner
        return pltpu.make_async_remote_copy(
            src_ref=slot(far, side),
            dst_ref=slot(far, side),
            send_sem=side_send.at[0, step],
            recv_sem=side_recv.at[far, step],
            device_id=(z * inner + (y + step) % inner, t),
            device_id_type=MESH,
        )

    def note(step):
        return pltpu.make_async_remote_copy(
            src_ref=notes_ref,
            dst_ref=all_notes_ref.at[z],
            send_sem=note_send.at[step],
            recv_sem=note_recv.at[step],
            device_id=groups.device("outer", (z + step) % outer),
            device_id_type=MESH,
        )

    def later_side(step):
        return (y + step) % inner > y

    def earlier_side(step):
        return (y + inner - step) % inner < y

    has_above = z < outer - 1
    pl.when(has_above)(lambda: upward(0).start())
    for step in range(1, inner):
        pl.when(later_side(step))(lambda step=step: sideways(0, step).start())
    for step in range(1, outer):
        note(step).start()
    own_copy = pltpu.make_async_copy(own_ref, all_ref.at[z * inner + y], keep.at[0])
    own_note = pltpu.make_async_copy(notes_ref, all_notes_ref.at[z], keep.at[1])
    own_copy.start()
    own_note.start()
    for far in range(1, outer):

        @pl.when(z >= far)
        def _(far=far):
            from_below(far).wait_recv()
            if far < outer - 1:
                pl.when(has_above)(lambda: upward(far).start())
            for step in range(1, inner):
                sideways(far, step).start()

    for far in range(outer):

        @pl.when(z >= far)
        def _(far=far):
            for step in range(1, inner):
                if far == 0:
                    pl.when(earlier_side(step))(lambda: from_side(far, step).wait_recv())
                    pl.when(later_side(step))(lambda: sideways(far, step).wait_send())
                else:
                    from_side(far, step).wait_recv()
                    sideways(far, step).wait_send()
            if far < outer - 1:
                pl.when(has_above)(lambda: upward(far).wait_send())

    for step in range(1, outer):
        note(step).wait()
    own_copy.wait()
    own_note.wait()


def gather(groups, collective_id, own, notes):
    outer, inner = groups.outer, groups.inner
    dma = pltpu.SemaphoreType.DMA
    return pl.pallas_call(
        functools.partial(gather_kernel, groups),
        out_shape=(
            jax.ShapeDtypeStruct((groups.n_sp,) + own.shape, own.dtype),
            jax.ShapeDtypeStruct((outer,) + notes.shape, notes.dtype),
        ),
        in_specs=[pl.BlockSpec(memory_space=pl.ANY)] * 2,
        out_specs=(pl.BlockSpec(memory_space=pl.ANY),) * 2,
        scratch_shapes=[
            dma((outer + 1,)),
            dma((outer + 1,)),
            dma((outer, inner)),
            dma((outer, inner)),
            dma((outer,)),
            dma((outer,)),
            dma((2,)),
        ],
        compiler_params=pltpu.CompilerParams(collective_id=collective_id, has_side_effects=True),
        name="gather",
    )(own, notes)


def dispatch_kernel(
    groups, own_ref, select_ref, all_ref, inbound_ref, line_ref, out_ref, *sems
):
    up_send, up_recv, down_send, down_recv, tp_send, tp_recv, plane_send, plane_recv, keep = sems
    outer, inner, n_tp, plane = groups.outer, groups.inner, groups.n_tp, groups.plane
    z, y, t = groups.place()
    pairs = n_tp // 2
    high, low = t // 2, t % 2
    partner = (z * inner + y, high * 2 + 1 - low)
    me = groups.mine("plane")
    barrier = pltpu.get_barrier_semaphore()
    for kind in ("outer", "plane"):
        for step in range(1, groups.size(kind)):
            pl.semaphore_signal(
                barrier,
                inc=1,
                device_id=groups.device(kind, (groups.mine(kind) + step) % groups.size(kind)),
                device_id_type=MESH,
            )
    pl.semaphore_wait(barrier, outer + plane - 2)

    def remote(source, target, send, recv, device):
        return pltpu.make_async_remote_copy(
            src_ref=source,
            dst_ref=target,
            send_sem=send,
            recv_sem=recv,
            device_id=device,
            device_id_type=MESH,
        )

    def along(far, direction):
        send, recv = (up_send, up_recv) if direction > 0 else (down_send, down_recv)
        block = z - direction * far
        source = own_ref if far == 0 else line_ref.at[block]
        return remote(
            source,
            line_ref.at[block],
            send.at[far],
            recv.at[far + 1],
            ((z + direction) * inner + y, t),
        )

    def arrived(far, direction):
        send, recv = (up_send, up_recv) if direction > 0 else (down_send, down_recv)
        block = line_ref.at[z - direction * far]
        return remote(
            block, block, send.at[0], recv.at[far], ((z + direction) * inner + y, t)
        )

    def outward(lane, block, step):
        peer = (me + step) % plane
        return remote(
            out_ref.at[block, peer],
            inbound_ref.at[me, block],
            plane_send.at[lane, step],
            plane_recv.at[lane, step],
            groups.device("plane", peer),
        )

    def inward(lane, block, step):
        peer = (me + plane - step) % plane
        target = inbound_ref.at[peer, block]
        return remote(
            target,
            target,
            plane_send.at[lane, step],
            plane_recv.at[lane, step],
            groups.device("plane", peer),
        )

    def keep_own(lane, block):
        return pltpu.make_async_copy(
            out_ref.at[block, me], inbound_ref.at[me, block], keep.at[1 + lane]
        )

    def work(lane, block, rows_ref):
        chosen = jnp.dot(select_ref[block], rows_ref[...], preferred_element_type=jnp.float32)
        out_ref[block] = chosen.reshape(out_ref.shape[1:]).astype(jnp.bfloat16)
        for step in range(1, plane):
            outward(lane, block, step).start()
        keep_own(lane, block).start()

    def finish(lane, block):
        keep_own(lane, block).wait()
        for step in range(1, plane):
            inward(lane, block, step).wait_recv()
            outward(lane, block, step).wait_send()

    def to_side(step):
        return remote(
            own_ref,
            all_ref.at[t],
            tp_send.at[step],
            tp_recv.at[step],
            (z * inner + y, ((high + step) % pairs) * 2 + low),
        )

    def to_partner(step):
        block = ((high + pairs - step) % pairs) * 2 + low
        source = own_ref if step == 0 else all_ref.at[block]
        target = all_ref.at[t] if step == 0 else all_ref.at[block]
        return remote(
            source, target, tp_send.at[pairs + step], tp_recv.at[pairs + step], partner
        )

    has_above, has_below = z < outer - 1, z > 0
    pl.when(has_above)(lambda: along(0, 1).start())
    pl.when(has_below)(lambda: along(0, -1).start())
    for step in range(1, pairs):
        to_side(step).start()
    to_partner(0).start()
    own_copy = pltpu.make_async_copy(own_ref, all_ref.at[t], keep.at[0])
    own_copy.start()
    work(0, z, own_ref)
    directions = ((1, has_above, 0), (-1, has_below, outer - 1))
    for far in range(1, outer):
        for direction, onward, base in directions:
            present = z >= far if direction > 0 else z + far < outer

            @pl.when(present)
            def _(far=far, direction=direction, onward=onward):
                arrived(far, direction).wait_recv()
                if far < outer - 1:
                    pl.when(onward)(lambda: along(far, direction).start())

        if far == 1:
            for step in range(1, pairs):
                side = all_ref.at[((high + pairs - step) % pairs) * 2 + low]
                remote(side, side, tp_send.at[step], tp_recv.at[step], partner).wait_recv()
                to_partner(step).start()
        for direction, onward, base in directions:
            present = z >= far if direction > 0 else z + far < outer

            @pl.when(present)
            def _(far=far, direction=direction, base=base):
                block = z - direction * far
                work(base + far, block, line_ref.at[block])

    finish(0, z)
    for far in range(1, outer):
        for direction, onward, base in directions:
            present = z >= far if direction > 0 else z + far < outer

            @pl.when(present)
            def _(far=far, direction=direction, onward=onward, base=base):
                finish(base + far, z - direction * far)
                if far < outer - 1:
                    pl.when(onward)(lambda: along(far, direction).wait_send())

    pl.when(has_above)(lambda: along(0, 1).wait_send())
    pl.when(has_below)(lambda: along(0, -1).wait_send())
    for step in range(1, pairs):
        to_side(step).wait_send()
    for step in range(pairs):
        to_partner(step).wait_send()
        block = all_ref.at[((high + pairs - step) % pairs) * 2 + 1 - low]
        remote(
            block, block, tp_send.at[pairs + step], tp_recv.at[pairs + step], partner
        ).wait_recv()
    own_copy.wait()


def dispatch_rows(groups, collective_id, own, select, seats):
    outer, plane, n_tp = groups.outer, groups.plane, groups.n_tp
    dma, kind = pltpu.SemaphoreType.DMA, own.dtype
    lanes = 2 * outer - 1
    vmem, anywhere = pl.BlockSpec(memory_space=pltpu.VMEM), pl.BlockSpec(memory_space=pl.ANY)
    return pl.pallas_call(
        functools.partial(dispatch_kernel, groups),
        out_shape=(
            jax.ShapeDtypeStruct((n_tp,) + own.shape, kind),
            jax.ShapeDtypeStruct((plane, outer, seats, own.shape[1]), kind),
        ),
        in_specs=[vmem, vmem],
        out_specs=(anywhere, anywhere),
        scratch_shapes=[
            pltpu.VMEM((outer,) + own.shape, kind),
            pltpu.VMEM((outer, plane, seats, own.shape[1]), kind),
            dma((outer + 1,)),
            dma((outer + 1,)),
            dma((outer + 1,)),
            dma((outer + 1,)),
            dma((n_tp,)),
            dma((n_tp,)),
            dma((lanes, plane)),
            dma((lanes, plane)),
            dma((lanes + 1,)),
        ],
        compiler_params=pltpu.CompilerParams(collective_id=collective_id, has_side_effects=True),
        name="dispatch_rows",
    )(own, select)


def flip(value, mask):
    bit = 1
    while bit <= mask:
        if mask & bit:
            value = value + bit - 2 * bit * ((value // bit) % 2)
        bit *= 2
    return value


def combine_kernel(
    groups, result_ref, mix_ref, shared_ref, routed_ref, parts_ref, back_ref, sum_ref, *sems
):
    plane_send, plane_recv, line_send, line_recv, tp_send, tp_recv, keep = sems
    outer, inner, n_tp, plane = groups.outer, groups.inner, groups.n_tp, groups.plane
    z, y, t = groups.place()
    me = groups.mine("plane")
    barrier = pltpu.get_barrier_semaphore()
    for kind in ("outer", "plane"):
        for step in range(1, groups.size(kind)):
            pl.semaphore_signal(
                barrier,
                inc=1,
                device_id=groups.device(kind, (groups.mine(kind) + step) % groups.size(kind)),
                device_id_type=MESH,
            )
    pl.semaphore_wait(barrier, outer + plane - 2)

    def remote(source, target, send, recv, device):
        return pltpu.make_async_remote_copy(
            src_ref=source,
            dst_ref=target,
            send_sem=send,
            recv_sem=recv,
            device_id=device,
            device_id_type=MESH,
        )

    def outward(mask, step):
        peer, block = (me + step) % plane, flip(z, mask)
        return remote(
            result_ref.at[peer, block],
            back_ref.at[block, me],
            plane_send.at[mask, step],
            plane_recv.at[mask, step],
            groups.device("plane", peer),
        )

    def inward(mask, step):
        peer, block = (me + plane - step) % plane, flip(z, mask)
        target = back_ref.at[block, peer]
        return remote(
            target,
            target,
            plane_send.at[mask, step],
            plane_recv.at[mask, step],
            groups.device("plane", peer),
        )

    def keep_own(mask):
        block = flip(z, mask)
        return pltpu.make_async_copy(
            result_ref.at[me, block], back_ref.at[block, me], keep.at[mask]
        )

    def issue(mask):
        for step in range(1, plane):
            outward(mask, step).start()
        keep_own(mask).start()

    def to_line(mask):
        block = flip(z, mask)
        return remote(
            sum_ref.at[block],
            routed_ref.at[z],
            line_send.at[mask],
            line_recv.at[mask],
            groups.device("outer", block),
        )

    def from_line(mask):
        block = routed_ref.at[flip(z, mask)]
        return remote(
            block,
            block,
            line_send.at[mask],
            line_recv.at[mask],
            groups.device("outer", flip(z, mask)),
        )

    def to_side(step):
        peer = (t + step) % n_tp
        return remote(
            shared_ref.at[peer],
            parts_ref.at[t],
            tp_send.at[step],
            tp_recv.at[step],
            groups.device("tp", peer),
        )

    def from_side(step):
        peer = (t + n_tp - step) % n_tp
        block = parts_ref.at[peer]
        return remote(
            block, block, tp_send.at[step], tp_recv.at[step], groups.device("tp", peer)
        )

    own_shared = pltpu.make_async_copy(shared_ref.at[t], parts_ref.at[t], keep.at[outer])
    own_shared.start()
    masks = list(range(outer - 1, -1, -1))
    for mask in masks[:2]:
        issue(mask)
    for number, mask in enumerate(masks):
        keep_own(mask).wait()
        for step in range(1, plane):
            inward(mask, step).wait_recv()
        if number + 2 < len(masks):
            issue(masks[number + 2])
        if number + 2 == len(masks) or len(masks) == 1:
            for step in range(1, n_tp):
                to_side(step).start()
        block = flip(z, mask)
        rows = back_ref[block].astype(jnp.float32)
        rows = rows.reshape(mix_ref.shape[2], rows.shape[-1]).astype(jnp.bfloat16)
        sum_ref[block] = jnp.dot(
            mix_ref[block], rows, preferred_element_type=jnp.float32
        ).astype(jnp.bfloat16)
        if mask:
            to_line(mask).start()
    own_sum = pltpu.make_async_copy(sum_ref.at[z], routed_ref.at[z], keep.at[outer + 1])
    own_sum.start()
    for mask in masks:
        for step in range(1, plane):
            outward(mask, step).wait_send()
        if mask:
            to_line(mask).wait_send()
            from_line(mask).wait_recv()
    for step in range(1, n_tp):
        to_side(step).wait_send()
        from_side(step).wait_recv()
    own_shared.wait()
    own_sum.wait()


def combine_rows(groups, collective_id, result, mix, shared):
    outer, plane, n_tp = groups.outer, groups.plane, groups.n_tp
    dma, kind = pltpu.SemaphoreType.DMA, result.dtype
    seats, width = result.shape[2:]
    vmem, anywhere = pl.BlockSpec(memory_space=pltpu.VMEM), pl.BlockSpec(memory_space=pl.ANY)
    return pl.pallas_call(
        functools.partial(combine_kernel, groups),
        out_shape=(
            jax.ShapeDtypeStruct((outer, mix.shape[1], width), kind),
            jax.ShapeDtypeStruct(shared.shape, kind),
        ),
        in_specs=[anywhere, vmem, anywhere],
        out_specs=(anywhere, anywhere),
        scratch_shapes=[
            pltpu.VMEM((outer, plane, seats, width), kind),
            pltpu.VMEM((outer, mix.shape[1], width), kind),
            dma((outer, plane)),
            dma((outer, plane)),
            dma((outer,)),
            dma((outer,)),
            dma((n_tp,)),
            dma((n_tp,)),
            dma((outer + 2,)),
        ],
        compiler_params=pltpu.CompilerParams(collective_id=collective_id, has_side_effects=True),
        name="combine_rows",
    )(result, mix, shared)


def layer_kernel(
    groups,
    chunks,
    seats,
    q_narrow_ref,
    k_narrow_ref,
    v_narrow_ref,
    g_narrow_ref,
    q_broad_ref,
    k_broad_ref,
    v_broad_ref,
    g_broad_ref,
    ids_ref,
    strength_ref,
    gain_hbm,
    project_narrow,
    project_broad,
    residual_ref,
    gate_ref,
    up_ref,
    down_ref,
    shared_gate_ref,
    shared_up_ref,
    shared_down_ref,
    out_ref,
    pairs_ref,
    q_narrow,
    q_broad,
    g_narrow,
    g_broad,
    own_ids,
    own_strength,
    gain_ref,
    gates_narrow,
    gates_broad,
    highest_narrow,
    highest_broad,
    totals_narrow,
    totals_broad,
    mixed_narrow,
    mixed_broad,
    heads_narrow,
    heads_broad,
    wp_narrow,
    wp_broad,
    w_gate,
    w_up,
    w_down,
    ws_gate,
    ws_up,
    ws_down,
    rows_own,
    notes,
    select,
    mixer,
    stream,
    tok,
    inbox,
    asked,
    acc_gate,
    acc_up,
    hidden,
    acc_sgate,
    acc_sup,
    shared_hidden,
    back,
    answer,
    parts,
    from_partner,
    kept,
    to_peer,
    from_peer,
    to_owner,
    relayed,
    from_owner,
    final,
    load_sem,
    first_sem,
    k_up_send,
    k_up_recv,
    k_side_send,
    k_side_recv,
    note_send,
    note_recv,
    z_send,
    z_recv,
    x_send,
    x_recv,
    p_send,
    p_recv,
    y_send,
    y_recv,
    r_send,
    r_recv,
    d_send,
    d_recv,
    s_send,
    s_recv,
    o_send,
    o_recv,
    i_recv,
):
    outer, inner, n_tp = groups.outer, groups.inner, groups.n_tp
    z, y, t = groups.place()
    pairs = n_tp // 2
    high, low = t // 2, t % 2
    width = gain_ref.shape[1]
    span = width // chunks
    units = outer * chunks
    count = rows_own.shape[0]
    group_rows = n_tp * count
    seat_rows = n_tp * seats
    bf16, f32 = jnp.bfloat16, jnp.float32
    partner = (z * inner + y, high * 2 + 1 - low)

    def remote(source, target, send, recv, device):
        return pltpu.make_async_remote_copy(
            src_ref=source,
            dst_ref=target,
            send_sem=send,
            recv_sem=recv,
            device_id=device,
            device_id_type=MESH,
        )

    def columns(piece):
        return pl.ds(pl.multiple_of(piece * span, span), span)

    def load(index):
        if index < chunks:
            return (
                pltpu.make_async_copy(
                    project_narrow.at[:, columns(index)], wp_narrow.at[index], load_sem.at[index, 0]
                ),
                pltpu.make_async_copy(
                    project_broad.at[:, columns(index)], wp_broad.at[index], load_sem.at[index, 1]
                ),
            )
        if index == chunks:
            first = pl.multiple_of(t * count, count)
            return (
                pltpu.make_async_copy(
                    residual_ref.at[pl.ds(first, count), :], rows_own, load_sem.at[index, 0]
                ),
            )
        if index == chunks + 1:
            return (
                pltpu.make_async_copy(gate_ref.at[0], w_gate, load_sem.at[index, 0]),
                pltpu.make_async_copy(up_ref.at[0], w_up, load_sem.at[index, 1]),
            )
        if index == chunks + 2:
            return (
                pltpu.make_async_copy(shared_gate_ref, ws_gate, load_sem.at[index, 0]),
                pltpu.make_async_copy(shared_up_ref, ws_up, load_sem.at[index, 1]),
            )
        return (
            pltpu.make_async_copy(down_ref.at[0], w_down, load_sem.at[index, 0]),
            pltpu.make_async_copy(shared_down_ref, ws_down, load_sem.at[index, 1]),
        )

    tokens = q_narrow.shape[1]
    place_of = z * inner + y
    narrow, broad = k_narrow_ref.shape[1], k_broad_ref.shape[1]
    own = pairs_ref.at[place_of]
    first_loads = [
        pltpu.make_async_copy(source, target, first_sem.at[number])
        for number, (source, target) in enumerate(
            (
                (k_narrow_ref, own.at[0, :, pl.ds(0, narrow)]),
                (v_narrow_ref, own.at[0, :, pl.ds(narrow, narrow)]),
                (k_broad_ref, own.at[1]),
                (v_broad_ref, own.at[2]),
            )
            + tuple(
                (queries.at[:, pl.ds(head * held.shape[2], held.shape[2])], held.at[head])
                for queries, held in ((q_narrow_ref, q_narrow), (q_broad_ref, q_broad))
                for head in range(held.shape[0])
            )
            + (
                (g_narrow_ref, g_narrow),
                (g_broad_ref, g_broad),
                (ids_ref, own_ids),
                (strength_ref, own_strength),
                (gain_hbm, gain_ref),
            )
        )
    ]
    for copy in first_loads:
        copy.start()

    barrier = pltpu.get_barrier_semaphore()
    greeted = 0
    for far in range(outer):
        for step in range(n_tp):
            if far or step:
                pl.semaphore_signal(
                    barrier,
                    inc=1,
                    device_id=(((z + far) % outer) * inner + y, (t + step) % n_tp),
                    device_id_type=MESH,
                )
                greeted += 1
    for step in range(1, inner):
        pl.semaphore_signal(
            barrier, inc=1, device_id=(z * inner + (y + step) % inner, t), device_id_type=MESH
        )
        greeted += 1
    pl.semaphore_wait(barrier, greeted)

    def slot(far, side):
        return pairs_ref.at[(z - far) * inner + side]

    def upward(far, piece):
        return remote(
            slot(far, y).at[piece],
            slot(far, y).at[piece],
            k_up_send.at[far, piece],
            k_up_recv.at[far + 1, piece],
            ((z + 1) * inner + y, t),
        )

    def from_below(far, piece):
        return remote(
            slot(far, y).at[piece],
            slot(far, y).at[piece],
            k_up_send.at[far, piece],
            k_up_recv.at[far, piece],
            ((z + 1) * inner + y, t),
        )

    def aside(far, step, piece):
        return remote(
            slot(far, y).at[piece],
            slot(far, y).at[piece],
            k_side_send.at[far, step - 1, piece],
            k_side_recv.at[far, step - 1, piece],
            (z * inner + (y + step) % inner, t),
        )

    def from_aside(far, step, piece):
        side = (y + inner - step) % inner
        return remote(
            slot(far, side).at[piece],
            slot(far, side).at[piece],
            k_side_send.at[far, step - 1, piece],
            k_side_recv.at[far, step - 1, piece],
            (z * inner + (y + step) % inner, t),
        )

    def later_side(step):
        return (y + step) % inner > y

    def earlier_side(step):
        return (y + inner - step) % inner < y

    has_above = z < outer - 1
    pieces = pairs_ref.shape[1]
    for piece in range(pieces):
        for copy in first_loads[:2] if piece == 0 else first_loads[piece + 1 : piece + 2]:
            copy.wait()
        pl.when(has_above)(lambda piece=piece: upward(0, piece).start())
        for step in range(1, inner):
            pl.when(later_side(step))(
                lambda step=step, piece=piece: aside(0, step, piece).start()
            )
    for copy in first_loads[pieces + 1 :]:
        copy.wait()

    def note(far, step):
        number = far * n_tp + step
        return remote(
            notes.at[z, t],
            notes.at[z, t],
            note_send.at[number],
            note_recv.at[number],
            (((z + far) % outer) * inner + y, (t + step) % n_tp),
        )

    others = [(far, step) for far in range(outer) for step in range(n_tp) if far or step]
    top = own_ids.shape[0]
    spread_out = jnp.where(
        lax.broadcasted_iota(jnp.int32, (count, group_rows), 1)
        == t * count + lax.broadcasted_iota(jnp.int32, (count, group_rows), 0),
        1.0,
        0.0,
    ).astype(bf16)
    notes[z, t, 0] = jnp.dot(
        own_ids[...].astype(f32).astype(bf16), spread_out, preferred_element_type=f32
    )
    notes[z, t, 1] = jnp.dot(
        own_strength[...].astype(bf16), spread_out, preferred_element_type=f32
    )
    for far, step in others:
        note(far, step).start()
    for index in range(chunks + 4):
        for copy in load(index):
            copy.start()

    first_row = pl.multiple_of(place_of * tokens, tokens)
    groups_of_heads = (
        (q_narrow, g_narrow, gates_narrow, highest_narrow, totals_narrow, mixed_narrow, 0, 0, narrow),
        (q_broad, g_broad, gates_broad, highest_broad, totals_broad, mixed_broad, 1, 2, 0),
    )
    for held, gates, own_gates, _, _, _, _, _, _ in groups_of_heads:
        heads = held.shape[0]
        turned = jnp.transpose(
            jnp.concatenate(
                [gates[:, pl.ds(first_row, tokens)], jnp.zeros((tokens - heads, tokens), f32)],
                axis=0,
            )
        )
        for head in range(heads):
            own_gates[head] = jnp.broadcast_to(turned[:, head : head + 1], (tokens, tokens))

    def make_tables():
        for far, step in others:
            note(far, step).wait_recv()
        lanes = mixer.shape[2]
        token = lax.broadcasted_iota(jnp.int32, (group_rows, lanes), 0)
        lane = lax.broadcasted_iota(jnp.int32, (group_rows, lanes), 1)
        token_before = lax.broadcasted_iota(jnp.int32, (group_rows, group_rows), 1)
        token_after = lax.broadcasted_iota(jnp.int32, (group_rows, group_rows), 0)
        earlier = (token_before < token_after) & (token_before // count == token_after // count)
        earlier = jnp.where(earlier, 1.0, 0.0).astype(bf16)
        seat_block = lane // seat_rows
        seat_place = (lane % seat_rows) // seats
        seat_number = (lane % seats).astype(f32)
        for block in range(outer):
            listed = notes[block, 0]
            for place in range(1, n_tp):
                listed = listed + notes[block, place]
            listed = jnp.transpose(
                jnp.concatenate(
                    [listed[0], listed[1], jnp.zeros((group_rows - 2 * top, group_rows), f32)], axis=0
                )
            )
            names, loads = listed[:, :top], listed[:, top : 2 * top]
            chosen = jnp.zeros((group_rows, lanes), f32)
            strength = jnp.zeros((group_rows, lanes), f32)
            for step in range(inner):
                expert = ((z * inner + (y + step) % inner) * n_tp + t).astype(f32)
                match = names == expert
                here = seat_block == step
                taken = jnp.sum(jnp.where(match, 1.0, 0.0), axis=1, keepdims=True)
                load_of = jnp.sum(jnp.where(match, loads, 0.0), axis=1, keepdims=True)
                chosen = jnp.where(here, taken, chosen)
                strength = jnp.where(here, load_of, strength)
            rank = jnp.dot(earlier, chosen.astype(bf16), preferred_element_type=f32)
            seated = (chosen > 0.5) & (rank == seat_number) & (seat_place == token // count)
            mixer[block] = jnp.where(seated, strength, 0.0).astype(bf16)
            select[block] = jnp.transpose(jnp.where(seated, 1.0, 0.0)).astype(bf16)

    def attend(block, blocks, own_block):
        length = blocks * tokens
        key_rows = pl.ds(pl.multiple_of(block * tokens, tokens), length)
        for held, gates, own_gates, highest, totals, mixed, key_at, value_at, value_from in groups_of_heads:
            heads, _, size = held.shape
            keys = pairs_ref[pl.ds(block, blocks), key_at, :, :size].reshape(length, size)
            values = pairs_ref[
                pl.ds(block, blocks), value_at, :, value_from : value_from + size
            ].reshape(length, size)
            scores = lax.dot_general(
                held[...].reshape(heads * tokens, size),
                keys,
                (((1,), (1,)), ((), ())),
                preferred_element_type=f32,
            ).reshape(heads, tokens, length)
            key_gates = gates[:, key_rows].reshape(heads, 1, length)
            pieces_of = []
            for part in range(blocks):
                at = slice(part * tokens, (part + 1) * tokens)
                piece = scores[:, :, at] * size ** (-0.5)
                piece = piece + own_gates[...] - key_gates[:, :, at]
                if own_block:
                    row = lax.broadcasted_iota(jnp.int32, (heads, tokens, tokens), 1)
                    column = lax.broadcasted_iota(jnp.int32, (heads, tokens, tokens), 2)
                    piece = jnp.where(column <= row, piece, -jnp.inf)
                pieces_of.append(piece)
            most = functools.reduce(jnp.maximum, pieces_of)
            peak = jnp.broadcast_to(jnp.max(most, axis=2, keepdims=True), most.shape)
            if not own_block:
                before = highest[...]
                peak = jnp.maximum(before, peak)
            weights = [jnp.exp(piece - peak) for piece in pieces_of]
            total = functools.reduce(jnp.add, weights)
            rounded = [piece.astype(bf16) for piece in weights]
            blended = jnp.dot(
                jnp.concatenate(rounded, axis=2).reshape(heads * tokens, length),
                values,
                preferred_element_type=f32,
            ).reshape(heads, tokens, size)
            if own_block:
                totals[...] = total
                mixed[...] = blended
            else:
                fade = jnp.exp(before - peak)
                totals[...] = totals[...] * fade + total
                mixed[...] = mixed[...] * jnp.concatenate([fade] * (size // tokens), axis=2) + blended
            highest[...] = peak

    attend(place_of, 1, True)

    def take_side():
        for step in range(1, inner):

            @pl.when(earlier_side(step))
            def _(step=step):
                for piece in range(pieces):
                    from_aside(0, step, piece).wait_recv()
                attend(z * inner + (y + inner - step) % inner, 1, False)

    def take_row(far):
        for step in range(1, inner):
            for piece in range(pieces):
                from_aside(far, step, piece).wait_recv()
        attend((z - far) * inner, inner, False)

    def climb_up(far):
        @pl.when(z >= far)
        def _():
            for piece in range(pieces):
                from_below(far, piece).wait_recv()
                pl.when(has_above & (far < outer - 1))(lambda piece=piece: upward(far, piece).start())
                for step in range(1, inner):
                    aside(far, step, piece).start()

    def climb(far, carried):
        climb_up(far)
        pl.when(z >= far - 1)(lambda: take_row(far - 1))
        return carried

    climb_up(1)
    take_side()
    climb_up(2)
    make_tables()
    pl.when(z >= 1)(lambda: take_row(1))
    lax.fori_loop(3, outer, climb, 0)
    pl.when(z >= outer - 1)(lambda: take_row(outer - 1))
    for mixed, totals, heads_out in (
        (mixed_narrow, totals_narrow, heads_narrow),
        (mixed_broad, totals_broad, heads_broad),
    ):
        heads, _, size = mixed.shape
        for head in range(heads):
            heads_out[:, head * size : (head + 1) * size] = (
                mixed[head] / jnp.sum(totals[head], axis=1, keepdims=True)
            ).astype(bf16)

    def across(unit):
        return remote(
            parts.at[unit, 1 - low],
            from_partner.at[unit],
            d_send.at[unit],
            d_recv.at[unit],
            partner,
        )

    def sideways(unit, step):
        return remote(
            to_peer.at[unit, step - 1],
            from_peer.at[unit, step - 1],
            s_send.at[unit, step - 1],
            s_recv.at[unit, step - 1],
            (z * inner + y, ((high + step) % pairs) * 2 + low),
        )

    def reduce_start(unit, value):
        for place in range(n_tp):
            parts[unit, place % 2, place // 2] = value[
                place * count : (place + 1) * count
            ].astype(bf16)
        across(unit).start()

    def reduce_pass(unit):
        across(unit).wait_recv()
        for step in range(1, pairs):
            other = (high + step) % pairs
            to_peer[unit, step - 1] = (
                parts[unit, low, other].astype(f32) + from_partner[unit, other].astype(f32)
            ).astype(bf16)
            sideways(unit, step).start()
        kept[unit] = parts[unit, low, high].astype(f32) + from_partner[unit, high].astype(f32)

    def reduce_end(unit):
        total = kept[unit]
        for step in range(1, pairs):
            sideways(unit, step).wait_recv()
            total = total + from_peer[unit, step - 1].astype(f32)
        return total

    for piece in range(chunks):
        for copy in load(piece):
            copy.wait()
        value = jnp.dot(heads_narrow[...], wp_narrow[piece], preferred_element_type=f32)
        value = value + jnp.dot(heads_broad[...], wp_broad[piece], preferred_element_type=f32)
        reduce_start(piece, value)
        if piece:
            reduce_pass(piece - 1)
    reduce_pass(chunks - 1)

    directions = ((1, has_above), (-1, z > 0))

    def along(block, piece, direction):
        return remote(
            tok.at[block, piece, t],
            tok.at[block, piece, t],
            z_send.at[block, piece, (direction + 1) // 2],
            z_recv.at[block, piece],
            ((z + direction) * inner + y, t),
        )

    for copy in load(chunks):
        copy.wait()
    square = jnp.zeros((count, 1), f32)
    for piece in range(chunks):
        value = reduce_end(piece) + rows_own[:, piece * span : (piece + 1) * span].astype(f32)
        stream[piece] = value
        square = square + jnp.sum(value * value, axis=1, keepdims=True)
    scale = lax.rsqrt(square * (1.0 / width) + norm_epsilon)
    for piece in range(chunks):
        gain = gain_ref[:, piece * span : (piece + 1) * span]
        tok[z, piece, t] = (stream[piece] * scale * gain).astype(bf16)
        for direction, onward in directions:
            pl.when(onward)(
                lambda piece=piece, direction=direction: along(z, piece, direction).start()
            )
    for index in range(chunks + 1, chunks + 3):
        for copy in load(index):
            copy.wait()

    in_low = z < outer // 2
    mate = z + 1 - 2 * (z % 2)
    near = jnp.where(in_low, outer // 2, outer // 2 - 1)
    distant = jnp.where(in_low, outer - 1, 0)
    is_edge = (z == 0) | (z == outer - 1)

    def pick(number, one, two, three, four):
        low_pair = jnp.where(number == 0, one, two)
        return jnp.where(number < 2, low_pair, jnp.where(number == 2, three, four))

    def going(unit):
        return pick(unit // chunks, z, mate, near, distant), unit % chunks

    def coming(unit):
        return pick(unit // chunks, near, distant, mate, z), unit % chunks

    def to_chip(block, piece, step):
        return remote(
            tok.at[block, piece, t],
            tok.at[block, piece, t],
            x_send.at[block, piece, step - 1],
            x_recv.at[block, piece, step - 1],
            (z * inner + y, ((high + step) % pairs) * 2 + low),
        )

    def from_chip(block, piece, step):
        place = tok.at[block, piece, ((high + pairs - step) % pairs) * 2 + low]
        return remote(
            place,
            place,
            x_send.at[block, piece, step - 1],
            x_recv.at[block, piece, step - 1],
            (z * inner + y, ((high + step) % pairs) * 2 + low),
        )

    def to_partner(block, piece, step):
        place = tok.at[block, piece, ((high + pairs - step) % pairs) * 2 + low]
        return remote(
            place, place, p_send.at[block, piece, step], p_recv.at[block, piece, step], partner
        )

    def from_other_core(block, piece, step):
        place = tok.at[block, piece, ((high + pairs - step) % pairs) * 2 + 1 - low]
        return remote(
            place, place, p_send.at[block, piece, step], p_recv.at[block, piece, step], partner
        )

    def ask(block, piece, step):
        return remote(
            asked.at[block, piece, step - 1],
            inbox.at[block, piece, step],
            y_send.at[block, piece, step - 1],
            y_recv.at[block, piece, step - 1],
            (z * inner + (y + step) % inner, t),
        )

    def reply(block, piece, step):
        return remote(
            answer.at[block, piece, step - 1],
            back.at[block, piece, step],
            r_send.at[block, piece, step - 1],
            r_recv.at[block, piece, step - 1],
            (z * inner + (y + inner - step) % inner, t),
        )

    def to_inner(number, piece):
        return remote(
            to_owner.at[number, piece],
            relayed.at[number, piece],
            o_send.at[number, piece],
            i_recv.at[number, piece],
            (mate * inner + y, t),
        )

    def to_other(number, piece):
        return remote(
            to_owner.at[number, piece],
            from_owner.at[1, piece],
            o_send.at[number, piece],
            o_recv.at[1, piece],
            (jnp.where(number == 0, near, distant) * inner + y, t),
        )

    def to_mate(piece):
        return remote(
            to_owner.at[2, piece],
            from_owner.at[0, piece],
            o_send.at[2, piece],
            o_recv.at[0, piece],
            (mate * inner + y, t),
        )

    def receive(block, piece):
        for direction, onward in directions:
            passes = (block < z) if direction > 0 else (block > z)

            @pl.when(passes)
            def _(direction=direction, onward=onward):
                along(block, piece, direction).wait_recv()
                pl.when(onward)(lambda: along(block, piece, direction).start())

    def arrive(unit):
        block, piece = going(unit)
        number = unit // chunks
        later = jnp.where(is_edge, number, number + 1)
        pl.when(number == 1)(lambda: receive(mate, piece))
        pl.when((number > 0) & (later == 2))(lambda: receive(near, piece))
        pl.when((number > 0) & (later == 3))(lambda: receive(distant, piece))
        for step in range(1, pairs):
            to_chip(block, piece, step).start()
        to_partner(block, piece, 0).start()

    def spread(unit):
        block, piece = going(unit)
        for step in range(1, pairs):
            from_chip(block, piece, step).wait_recv()
            to_partner(block, piece, step).start()

    def choose(unit):
        block, piece = going(unit)
        for step in range(pairs):
            from_other_core(block, piece, step).wait_recv()
        rows = tok[block, piece].reshape(group_rows, span)
        picked = jnp.dot(
            select[block, : inner * seat_rows], rows, preferred_element_type=f32
        ).astype(bf16)
        for step in range(1, inner):
            asked[block, piece, step - 1] = picked[step * seat_rows : (step + 1) * seat_rows]
            ask(block, piece, step).start()
        inbox[block, piece, 0] = picked[:seat_rows]

    def expand(unit):
        block, piece = going(unit)
        for step in range(1, inner):
            ask(block, piece, step).wait_recv()
        rows = inbox[block, piece].reshape(inner * seat_rows, span)
        part_gate = jnp.dot(rows, w_gate[columns(piece), :], preferred_element_type=f32)
        part_up = jnp.dot(rows, w_up[columns(piece), :], preferred_element_type=f32)

        @pl.when(piece == 0)
        def _():
            acc_gate[...] = part_gate
            acc_up[...] = part_up

        @pl.when(piece > 0)
        def _():
            acc_gate[...] += part_gate
            acc_up[...] += part_up

        @pl.when(piece == chunks - 1)
        def _():
            hidden[block] = (jax.nn.silu(acc_gate[...]) * acc_up[...]).astype(bf16)

    def expand_shared(piece):
        rows = tok[z, piece].reshape(group_rows, span)
        part_gate = jnp.dot(rows, ws_gate[columns(piece), :], preferred_element_type=f32)
        part_up = jnp.dot(rows, ws_up[columns(piece), :], preferred_element_type=f32)

        @pl.when(piece == 0)
        def _():
            acc_sgate[...] = part_gate
            acc_sup[...] = part_up

        @pl.when(piece > 0)
        def _():
            acc_sgate[...] += part_gate
            acc_sup[...] += part_up

        @pl.when(piece == chunks - 1)
        def _():
            shared_hidden[...] = (jax.nn.silu(acc_sgate[...]) * acc_sup[...]).astype(bf16)

    def within(number, first, last):
        return (number >= first) & (number < last)

    def produce(unit):
        block, piece = coming(unit)
        made = jnp.dot(hidden[block], w_down[:, columns(piece)], preferred_element_type=f32)
        made = made.astype(bf16)
        for step in range(1, inner):
            answer[block, piece, step - 1] = made[step * seat_rows : (step + 1) * seat_rows]
            reply(block, piece, step).start()
        back[block, piece, 0] = made[:seat_rows]

    def blend(unit):
        block, piece = coming(unit)
        for step in range(1, inner):
            reply(block, piece, step).wait_recv()
        rows = back[block, piece].reshape(inner * seat_rows, span)
        value = jnp.dot(
            mixer[block][:, : inner * seat_rows], rows, preferred_element_type=f32
        )

        @pl.when(block != z)
        def _():
            reduce_start(chunks + unit, value)

        @pl.when(block == z)
        def _():
            shared_part = jnp.dot(
                shared_hidden[...], ws_down[:, columns(piece)], preferred_element_type=f32
            )
            reduce_start(chunks + unit, value + shared_part)

    def deliver(unit):
        number, piece = unit // chunks, unit % chunks
        total = reduce_end(chunks + unit)

        @pl.when((number < 2) & is_edge)
        def _():
            to_owner[number, piece] = total.astype(bf16)
            to_inner(number, piece).start()

        @pl.when((number < 2) & jnp.logical_not(is_edge))
        def _():
            kept[chunks + unit] = total

        @pl.when(number == 2)
        def _():
            to_owner[2, piece] = total.astype(bf16)
            to_mate(piece).start()

        @pl.when(number == 3)
        def _():
            final[piece] = total

    def relay(unit):
        number, piece = unit // chunks, unit % chunks
        to_inner(number, piece).wait_recv()
        to_owner[number, piece] = (
            kept[chunks + unit] + relayed[number, piece].astype(f32)
        ).astype(bf16)
        to_other(number, piece).start()

    (
        late_spread,
        late_choose,
        late_expand,
        late_produce,
        late_blend,
        late_pass,
        late_deliver,
        late_relay,
    ) = LAGS
    for copy in load(chunks + 3):
        copy.wait()

    def step_all(unit, carried):
        pl.when(within(unit, 0, units))(lambda: arrive(unit))
        one = unit - late_spread
        pl.when(within(one, 0, units))(lambda: spread(one))
        two = unit - late_choose
        pl.when(within(two, 0, units))(lambda: choose(two))
        pl.when(within(two, 0, chunks))(lambda: expand_shared(two))
        three = unit - late_expand
        pl.when(within(three, 0, units))(lambda: expand(three))
        four = unit - late_produce
        pl.when(within(four, 0, units))(lambda: produce(four))
        five = unit - late_blend
        pl.when(within(five, 0, units))(lambda: blend(five))
        six = unit - late_pass
        pl.when(within(six, 0, units))(lambda: reduce_pass(chunks + six))
        seven = unit - late_deliver
        pl.when(within(seven, 0, units))(lambda: deliver(seven))
        eight = unit - late_relay
        pl.when(within(eight, 0, 2 * chunks) & jnp.logical_not(is_edge))(lambda: relay(eight))
        return carried

    lax.fori_loop(0, units + late_deliver, step_all, 0)

    for piece in range(chunks):
        total = stream[piece] + final[piece]
        for place, copy in enumerate((to_mate(piece), to_other(0, piece))):
            copy.wait_recv()
            total = total + from_owner[place, piece].astype(f32)
        out_ref[:, piece * span : (piece + 1) * span] = total.astype(bf16)

    for far, step in others:
        note(far, step).wait_send()

    def drain(unit, carried):
        block, piece = unit // chunks, unit % chunks
        for direction, onward in directions:
            has = (block <= z) if direction > 0 else (block >= z)

            @pl.when(has & onward)
            def _(direction=direction):
                along(block, piece, direction).wait_send()

        for step in range(1, pairs):
            to_chip(block, piece, step).wait_send()
        for step in range(pairs):
            to_partner(block, piece, step).wait_send()
        for step in range(1, inner):
            ask(block, piece, step).wait_send()
            reply(block, piece, step).wait_send()
        pl.when(block < 2)(lambda: to_inner(block, piece).wait_send())
        pl.when(block == 2)(lambda: to_mate(piece).wait_send())
        return carried

    lax.fori_loop(0, units, drain, 0)

    for far in range(outer):

        @pl.when(z >= far)
        def _(far=far):
            for piece in range(pieces):
                for step in range(1, inner):
                    sent = (far > 0) | later_side(step)
                    pl.when(sent)(
                        lambda step=step, piece=piece: aside(far, step, piece).wait_send()
                    )
                if far < outer - 1:
                    pl.when(has_above)(lambda piece=piece: upward(far, piece).wait_send())

    def drain_sums(unit, carried):
        across(unit).wait_send()
        for step in range(1, pairs):
            sideways(unit, step).wait_send()
        return carried

    lax.fori_loop(0, chunks + units, drain_sums, 0)


LAGS = (3, 5, 8, 20, 23, 24, 27, 30)


def layer_rows(
    groups,
    collective_id,
    seats,
    query_narrow,
    key_narrow,
    value_narrow,
    gates_narrow,
    query_broad,
    key_broad,
    value_broad,
    gates_broad,
    project_narrow,
    project_broad,
    residual,
    norm_gain,
    route_ids,
    route_weight,
    expert_gate,
    expert_up,
    expert_down,
    shared_gate,
    shared_up,
    shared_down,
):
    outer, inner, n_tp = groups.outer, groups.inner, groups.n_tp
    dma = pltpu.SemaphoreType.DMA
    width = residual.shape[1]
    chunks = width // math.gcd(width, 1024)
    span = width // chunks
    count, top = route_ids.shape
    tokens = query_narrow.shape[0]
    heads_n, heads_b = gates_narrow.shape[1], gates_broad.shape[1]
    group_rows = n_tp * count
    seat_rows = n_tp * seats
    pairs = n_tp // 2
    units = outer * chunks
    sums = chunks + units
    lanes = -(-inner * seat_rows // 128) * 128
    bf16, f32 = jnp.bfloat16, jnp.float32
    expert_width, shared_width = expert_gate.shape[2], shared_gate.shape[1]
    vmem, anywhere = pl.BlockSpec(memory_space=pltpu.VMEM), pl.BlockSpec(memory_space=pl.ANY)
    return pl.pallas_call(
        functools.partial(layer_kernel, groups, chunks, seats),
        out_shape=jax.ShapeDtypeStruct((count, width), bf16),
        in_specs=[anywhere] * 20,
        out_specs=vmem,
        scratch_shapes=[
            pltpu.VMEM((groups.n_sp, 3, tokens, key_broad.shape[1]), bf16),
            pltpu.VMEM((heads_n, tokens, NARROW_SIZE), bf16),
            pltpu.VMEM((heads_b, tokens, BROAD_SIZE), bf16),
            pltpu.VMEM(gates_narrow.shape[::-1], f32),
            pltpu.VMEM(gates_broad.shape[::-1], f32),
            pltpu.VMEM((top, count), jnp.int32),
            pltpu.VMEM((top, count), f32),
            pltpu.VMEM((1, width), f32),
            *[pltpu.VMEM((number, tokens, tokens), f32) for _ in range(3) for number in (heads_n, heads_b)],
            pltpu.VMEM((heads_n, tokens, NARROW_SIZE), f32),
            pltpu.VMEM((heads_b, tokens, BROAD_SIZE), f32),
            pltpu.VMEM(query_narrow.shape, bf16),
            pltpu.VMEM(query_broad.shape, bf16),
            pltpu.VMEM((chunks, project_narrow.shape[0], span), bf16),
            pltpu.VMEM((chunks, project_broad.shape[0], span), bf16),
            pltpu.VMEM((width, expert_width), bf16),
            pltpu.VMEM((width, expert_width), bf16),
            pltpu.VMEM((expert_width, width), bf16),
            pltpu.VMEM((width, shared_width), bf16),
            pltpu.VMEM((width, shared_width), bf16),
            pltpu.VMEM((shared_width, width), bf16),
            pltpu.VMEM((count, width), bf16),
            pltpu.VMEM((outer, n_tp, 2, top, group_rows), f32),
            pltpu.VMEM((outer, lanes, group_rows), bf16),
            pltpu.VMEM((outer, group_rows, lanes), bf16),
            pltpu.VMEM((chunks, count, span), f32),
            pltpu.VMEM((outer, chunks, n_tp, count, span), bf16),
            pltpu.VMEM((outer, chunks, inner, seat_rows, span), bf16),
            pltpu.VMEM((outer, chunks, inner - 1, seat_rows, span), bf16),
            pltpu.VMEM((inner * seat_rows, expert_width), f32),
            pltpu.VMEM((inner * seat_rows, expert_width), f32),
            pltpu.VMEM((outer, inner * seat_rows, expert_width), bf16),
            pltpu.VMEM((group_rows, shared_width), f32),
            pltpu.VMEM((group_rows, shared_width), f32),
            pltpu.VMEM((group_rows, shared_width), bf16),
            pltpu.VMEM((outer, chunks, inner, seat_rows, span), bf16),
            pltpu.VMEM((outer, chunks, inner - 1, seat_rows, span), bf16),
            pltpu.VMEM((sums, 2, pairs, count, span), bf16),
            pltpu.VMEM((sums, pairs, count, span), bf16),
            pltpu.VMEM((sums, count, span), f32),
            pltpu.VMEM((sums, pairs - 1, count, span), bf16),
            pltpu.VMEM((sums, pairs - 1, count, span), bf16),
            pltpu.VMEM((3, chunks, count, span), bf16),
            pltpu.VMEM((2, chunks, count, span), bf16),
            pltpu.VMEM((2, chunks, count, span), bf16),
            pltpu.VMEM((chunks, count, span), f32),
            dma((chunks + 4, 2)),
            dma((9 + heads_n + heads_b,)),
            dma((outer, 3)),
            dma((outer + 1, 3)),
            dma((outer, inner - 1, 3)),
            dma((outer, inner - 1, 3)),
            dma((outer * n_tp,)),
            dma((outer * n_tp,)),
            dma((outer, chunks, 2)),
            dma((outer, chunks)),
            dma((outer, chunks, pairs - 1)),
            dma((outer, chunks, pairs - 1)),
            dma((outer, chunks, pairs)),
            dma((outer, chunks, pairs)),
            dma((outer, chunks, inner - 1)),
            dma((outer, chunks, inner - 1)),
            dma((outer, chunks, inner - 1)),
            dma((outer, chunks, inner - 1)),
            dma((sums,)),
            dma((sums,)),
            dma((sums, pairs - 1)),
            dma((sums, pairs - 1)),
            dma((3, chunks)),
            dma((2, chunks)),
            dma((2, chunks)),
        ],
        compiler_params=pltpu.CompilerParams(
            collective_id=collective_id, has_side_effects=True, vmem_limit_bytes=62 * 2**20
        ),
        name="layer_rows",
    )(
        query_narrow,
        key_narrow,
        value_narrow,
        gates_narrow.T,
        query_broad,
        key_broad,
        value_broad,
        gates_broad.T,
        route_ids.T,
        route_weight.T,
        norm_gain.reshape(1, width),
        project_narrow,
        project_broad,
        residual,
        expert_gate,
        expert_up,
        expert_down,
        shared_gate,
        shared_up,
        shared_down,
    )


def local(
    groups,
    query_narrow,
    key_narrow,
    value_narrow,
    gates_narrow,
    query_broad,
    key_broad,
    value_broad,
    gates_broad,
    project_narrow,
    project_broad,
    residual,
    norm_gain,
    route_ids,
    route_weight,
    expert_gate,
    expert_up,
    expert_down,
    shared_gate,
    shared_up,
    shared_down,
):
    spots = 2 * route_ids.size // (groups.n_sp * groups.n_tp * expert_gate.shape[0])
    if (
        spots % 8 == 0
        and groups.n_tp == 4
        and groups.inner == 2
        and groups.outer == 4
        and expert_gate.shape[0] == 1
        and 2 * key_narrow.shape[1] == key_broad.shape[1]
    ):
        return layer_rows(
            groups,
            0,
            spots,
            query_narrow,
            key_narrow,
            value_narrow,
            gates_narrow,
            query_broad,
            key_broad,
            value_broad,
            gates_broad,
            project_narrow,
            project_broad,
            residual,
            norm_gain,
            route_ids,
            route_weight,
            expert_gate,
            expert_up,
            expert_down,
            shared_gate,
            shared_up,
            shared_down,
        )
    tokens = query_narrow.shape[0]
    notes = jnp.concatenate(
        [
            route_ids.astype(jnp.float32).T,
            route_weight.astype(jnp.bfloat16).astype(jnp.float32).T,
        ],
        axis=0,
    )
    own_pairs = jnp.concatenate([key_narrow, key_broad, value_narrow, value_broad], axis=1)
    all_pairs, all_notes = gather(groups, 0, own_pairs, notes)
    all_pairs = all_pairs.reshape(-1, own_pairs.shape[1])
    vmem = pl.BlockSpec(memory_space=pltpu.VMEM)
    heads_out = pl.pallas_call(
        attend_kernel,
        out_shape=(
            jax.ShapeDtypeStruct(query_narrow.shape, jnp.bfloat16),
            jax.ShapeDtypeStruct(query_broad.shape, jnp.bfloat16),
        ),
        in_specs=[vmem] * 7,
        out_specs=(vmem, vmem),
        name="attend",
    )(
        query_narrow,
        query_broad,
        gates_narrow,
        gates_broad,
        gates_narrow.T,
        gates_broad.T,
        all_pairs,
    )
    partial_value = jnp.dot(heads_out[0], project_narrow, preferred_element_type=jnp.float32)
    partial_value = partial_value + jnp.dot(
        heads_out[1], project_broad, preferred_element_type=jnp.float32
    )
    n_tp, outer, plane = groups.n_tp, groups.outer, groups.plane
    sub_rows, width = route_ids.shape[0], residual.shape[1]
    (portions,) = swap(
        groups, 1, (partial_value.astype(jnp.bfloat16).reshape(n_tp, sub_rows, width), "tp", 0, 0)
    )
    stream, own_normed = pl.pallas_call(
        norm_kernel,
        out_shape=(
            jax.ShapeDtypeStruct((sub_rows, width), jnp.float32),
            jax.ShapeDtypeStruct((sub_rows, width), jnp.bfloat16),
        ),
        in_specs=[vmem] * 3,
        out_specs=(vmem, vmem),
        name="norm",
    )(portions, residual, norm_gain.reshape(1, width))
    top_count = route_ids.shape[1]
    local_experts = expert_gate.shape[0]
    expert_total = groups.n_sp * n_tp * local_experts
    capacity = 2 * sub_rows * top_count // expert_total
    seat_rows = local_experts * capacity
    fused = seat_rows % 8 == 0 and n_tp % 2 == 0
    plane_experts = plane * local_experts
    first_expert = groups.mine("outer") * plane_experts
    line_ids = all_notes[:, :top_count].astype(jnp.int32)
    line_weights = all_notes[:, top_count:]
    named = (
        line_ids[:, None]
        == first_expert + jnp.arange(plane_experts, dtype=jnp.int32)[None, :, None, None]
    )
    chosen = jnp.any(named, axis=2)
    strength = jnp.sum(jnp.where(named, line_weights[:, None], 0.0), axis=2)
    before = jnp.arange(sub_rows)[:, None] < jnp.arange(sub_rows)[None, :]
    rank = jnp.sum(jnp.where(chosen[:, :, :, None] & before, 1, 0), axis=2)
    seats = chosen[:, :, None, :] & (
        rank[:, :, None, :] == jnp.arange(capacity, dtype=jnp.int32)[None, None, :, None]
    )
    dispatch = seats.astype(jnp.bfloat16).reshape(outer, plane_experts * capacity, sub_rows)
    combiner = (
        jnp.where(seats, strength[:, :, None, :], 0.0)
        .astype(jnp.bfloat16)
        .reshape(outer, plane_experts * capacity, sub_rows)
    )
    if fused:
        normed, inbound = dispatch_rows(groups, 2, own_normed, dispatch, seat_rows)
    else:
        normed, line_normed = swap(
            groups, 2, (own_normed, "tp", None, 0), (own_normed, "outer", None, 0)
        )
        outbound = jnp.einsum("zct,ztd->zcd", dispatch, line_normed, preferred_element_type=jnp.float32)
        outbound = outbound.astype(jnp.bfloat16).reshape(
            outer, plane, local_experts * capacity, width
        )
        (inbound,) = swap(groups, 3, (outbound, "plane", 1, 0))
    normed = normed.reshape(tokens, width)
    grouped = inbound.reshape(plane * outer, local_experts, capacity, width)
    gate_out = jnp.einsum(
        "secd,edh->sech", grouped, expert_gate, preferred_element_type=jnp.float32
    )
    up_out = jnp.einsum("secd,edh->sech", grouped, expert_up, preferred_element_type=jnp.float32)
    hidden = (jax.nn.silu(gate_out) * up_out).astype(jnp.bfloat16)
    result = jnp.einsum(
        "sech,ehd->secd", hidden, expert_down, preferred_element_type=jnp.float32
    ).astype(jnp.bfloat16)
    shared_hidden = (
        jax.nn.silu(jnp.dot(normed, shared_gate, preferred_element_type=jnp.float32))
        * jnp.dot(normed, shared_up, preferred_element_type=jnp.float32)
    ).astype(jnp.bfloat16)
    shared_out = jnp.dot(shared_hidden, shared_down, preferred_element_type=jnp.float32).astype(
        jnp.bfloat16
    )
    shared_out = shared_out.reshape(n_tp, sub_rows, width)
    if fused:
        routed_parts, shared_parts = combine_rows(
            groups, 4, result.reshape(inbound.shape), combiner.transpose(0, 2, 1), shared_out
        )
    else:
        (returned,) = swap(groups, 4, (result.reshape(inbound.shape), "plane", 0, 1))
        returned = returned.reshape(outer, plane_experts * capacity, width)
        line_routed = jnp.einsum(
            "zct,zcd->ztd", combiner, returned, preferred_element_type=jnp.float32
        ).astype(jnp.bfloat16)
        routed_parts, shared_parts = swap(
            groups,
            5,
            (line_routed, "outer", 0, 0),
            (shared_out, "tp", 0, 0),
        )
    tile = math.gcd(width, 1024)
    return pl.pallas_call(
        add_kernel,
        grid=(width // tile,),
        out_shape=jax.ShapeDtypeStruct((sub_rows, width), jnp.bfloat16),
        in_specs=[
            pl.BlockSpec((sub_rows, tile), lambda i: (0, i)),
            pl.BlockSpec((n_tp, sub_rows, tile), lambda i: (0, 0, i)),
            pl.BlockSpec((outer, sub_rows, tile), lambda i: (0, 0, i)),
        ],
        out_specs=pl.BlockSpec((sub_rows, tile), lambda i: (0, i)),
        name="add_parts",
    )(stream, shared_parts, routed_parts)


def solution(mesh):
    placed = (
        P("sp", "tp"),
        P("sp", "tp"),
        P("sp", "tp"),
        P(None, "tp"),
        P("sp", "tp"),
        P("sp", "tp"),
        P("sp", "tp"),
        P(None, "tp"),
        P("tp", None),
        P("tp", None),
        P("sp", None),
        P(),
        P(("sp", "tp"), None),
        P(("sp", "tp"), None),
        P(("sp", "tp"), None, None),
        P(("sp", "tp"), None, None),
        P(("sp", "tp"), None, None),
        P(None, "tp"),
        P(None, "tp"),
        P("tp", None),
    )
    groups = Groups(mesh.shape["sp"], mesh.shape["tp"])
    return jax.shard_map(
        functools.partial(local, groups), mesh=mesh, in_specs=placed, out_specs=P(("sp", "tp"), None), check_vma=False
    )
```

```python
import functools
import math

import jax
import jax.numpy as jnp
from jax import lax
from jax.experimental import pallas as pl
from jax.experimental.pallas import tpu as pltpu
from jax.sharding import PartitionSpec as P

MESH = pl.DeviceIdType.MESH

NARROW_SIZE = 128
BROAD_SIZE = 256


norm_epsilon = 1e-06


def attend_kernel(
    q_narrow, q_broad, g_narrow, g_broad, k_narrow, k_broad, pairs_ref, o_narrow, o_broad
):
    tokens, length = q_narrow.shape[0], pairs_ref.shape[0]
    first_row = lax.axis_index("sp") * tokens
    key_place = lax.broadcasted_iota(jnp.int32, (tokens, length), 1)
    query_place = first_row + lax.broadcasted_iota(jnp.int32, (tokens, length), 0)
    allowed = key_place <= query_place
    rows = pl.ds(pl.multiple_of(first_row, tokens), tokens)
    value_first = pairs_ref.shape[1] // 2
    column = 0
    for queries, gates, key_gates, outputs, head_size in (
        (q_narrow, g_narrow, k_narrow, o_narrow, NARROW_SIZE),
        (q_broad, g_broad, k_broad, o_broad, BROAD_SIZE),
    ):
        heads = queries.shape[1] // head_size
        widest = value_first * head_size // (NARROW_SIZE + BROAD_SIZE)
        group_size = heads * head_size // widest
        own_gates = gates[rows, :]
        for kv in range(widest // head_size):
            keys = pairs_ref[:, column : column + head_size]
            values = pairs_ref[:, value_first + column : value_first + column + head_size]
            reachable = (
                lax.broadcasted_iota(jnp.int32, (length, head_size), 0) < first_row + tokens
            )
            values = jnp.where(reachable, values.astype(jnp.float32), 0.0).astype(jnp.bfloat16)
            column += head_size
            for member in range(group_size):
                head = kv * group_size + member
                span = slice(head * head_size, (head + 1) * head_size)
                scores = lax.dot_general(
                    queries[:, span],
                    keys,
                    (((1,), (1,)), ((), ())),
                    preferred_element_type=jnp.float32,
                )
                scores = scores * head_size ** (-0.5)
                scores = scores + own_gates[:, head : head + 1] - key_gates[head : head + 1, :]
                scores = jnp.where(allowed, scores, -jnp.inf)
                weights = jnp.exp(scores - jnp.max(scores, axis=1, keepdims=True))
                total = jnp.sum(weights, axis=1, keepdims=True)
                blended = jnp.dot(
                    weights.astype(jnp.bfloat16), values, preferred_element_type=jnp.float32
                )
                outputs[:, span] = (blended / total).astype(jnp.bfloat16)


def add_kernel(stream_ref, shared_ref, routed_ref, out_ref):
    total = stream_ref[...]
    for parts in (shared_ref, routed_ref):
        for index in range(parts.shape[0]):
            total = total + parts[index].astype(jnp.float32)
    out_ref[...] = total.astype(jnp.bfloat16)


def norm_kernel(portions_ref, residual_ref, gain_ref, stream_ref, normed_ref):
    count = stream_ref.shape[0]
    first = lax.axis_index("tp") * count
    stream = residual_ref[pl.ds(pl.multiple_of(first, count), count), :].astype(jnp.float32)
    for index in range(portions_ref.shape[0]):
        stream = stream + portions_ref[index].astype(jnp.float32)
    stream_ref[...] = stream
    scale = lax.rsqrt(jnp.mean(stream * stream, axis=1, keepdims=True) + norm_epsilon)
    normed_ref[...] = (stream * scale * gain_ref[...]).astype(jnp.bfloat16)


class Groups:
    def __init__(self, n_sp, n_tp):
        self.n_sp, self.n_tp = n_sp, n_tp
        self.outer = math.gcd(n_sp, 4)
        self.inner = n_sp // self.outer
        self.plane = self.inner * n_tp

    def size(self, kind):
        return {"tp": self.n_tp, "outer": self.outer, "plane": self.plane}[kind]

    def place(self):
        sp, tp = lax.axis_index("sp"), lax.axis_index("tp")
        return sp // self.inner, sp % self.inner, tp

    def mine(self, kind):
        z, y, t = self.place()
        return {"tp": t, "outer": z, "plane": y * self.n_tp + t}[kind]

    def device(self, kind, index):
        z, y, t = self.place()
        if kind == "tp":
            return (z * self.inner + y, index)
        if kind == "outer":
            return (index * self.inner + y, t)
        return (z * self.inner + index // self.n_tp, index % self.n_tp)


def swap_kernel(groups, plans, *refs):
    count = len(plans)
    sources, targets, sems = refs[:count], refs[count : 2 * count], refs[2 * count :]
    barrier = pltpu.get_barrier_semaphore()
    greeted = 0
    for kind in sorted({plan[0] for plan in plans}):
        size, me = groups.size(kind), groups.mine(kind)
        for step in range(1, size):
            pl.semaphore_signal(
                barrier,
                inc=1,
                device_id=groups.device(kind, (me + step) % size),
                device_id_type=MESH,
            )
            greeted += 1
    pl.semaphore_wait(barrier, greeted)

    def cut(ref, axis, index):
        if axis is None:
            return ref
        return ref.at[index] if axis == 0 else ref.at[:, index]

    started, local_copies = [], []
    for number, (kind, source_axis, target_axis) in enumerate(plans):
        send, recv, keep = sems[3 * number : 3 * number + 3]
        size, me = groups.size(kind), groups.mine(kind)
        for step in range(1, size):
            peer = (me + step) % size
            copy = pltpu.make_async_remote_copy(
                src_ref=cut(sources[number], source_axis, peer),
                dst_ref=cut(targets[number], target_axis, me),
                send_sem=send.at[step],
                recv_sem=recv.at[step],
                device_id=groups.device(kind, peer),
                device_id_type=MESH,
            )
            copy.start()
            started.append(copy)
        own = pltpu.make_async_copy(
            cut(sources[number], source_axis, me), cut(targets[number], target_axis, me), keep
        )
        own.start()
        local_copies.append(own)
    for own in local_copies:
        own.wait()
    for copy in started:
        copy.wait()


def swap(groups, collective_id, *moves):
    plans, shapes, scratch = [], [], []
    for array, kind, source_axis, target_axis in moves:
        size = groups.size(kind)
        plans.append((kind, source_axis, target_axis))
        block = list(array.shape)
        if source_axis is not None:
            del block[source_axis]
        block.insert(target_axis, size)
        shapes.append(jax.ShapeDtypeStruct(tuple(block), array.dtype))
        scratch += [
            pltpu.SemaphoreType.DMA((size,)),
            pltpu.SemaphoreType.DMA((size,)),
            pltpu.SemaphoreType.DMA,
        ]
    return pl.pallas_call(
        functools.partial(swap_kernel, groups, tuple(plans)),
        out_shape=tuple(shapes),
        in_specs=[pl.BlockSpec(memory_space=pl.ANY)] * len(moves),
        out_specs=tuple([pl.BlockSpec(memory_space=pl.ANY)] * len(moves)),
        scratch_shapes=scratch,
        compiler_params=pltpu.CompilerParams(collective_id=collective_id, has_side_effects=True),
        name=f"swap_{collective_id}",
    )(*[move[0] for move in moves])


def gather_kernel(groups, own_ref, notes_ref, all_ref, all_notes_ref, *sems):
    line_send, line_recv, side_send, side_recv, note_send, note_recv, keep = sems
    outer, inner = groups.outer, groups.inner
    z, y, t = groups.place()
    barrier = pltpu.get_barrier_semaphore()
    for step in range(1, outer):
        pl.semaphore_signal(
            barrier, inc=1, device_id=groups.device("outer", (z + step) % outer), device_id_type=MESH
        )
    for step in range(1, inner):
        pl.semaphore_signal(
            barrier, inc=1, device_id=(z * inner + (y + step) % inner, t), device_id_type=MESH
        )
    pl.semaphore_wait(barrier, outer + inner - 2)

    def slot(far, side):
        return all_ref.at[(z - far) * inner + side]

    def upward(far):
        source = own_ref if far == 0 else slot(far, y)
        return pltpu.make_async_remote_copy(
            src_ref=source,
            dst_ref=slot(far, y),
            send_sem=line_send.at[far],
            recv_sem=line_recv.at[far + 1],
            device_id=((z + 1) * inner + y, t),
            device_id_type=MESH,
        )

    def sideways(far, step):
        source = own_ref if far == 0 else slot(far, y)
        return pltpu.make_async_remote_copy(
            src_ref=source,
            dst_ref=slot(far, y),
            send_sem=side_send.at[far, step],
            recv_sem=side_recv.at[far, step],
            device_id=(z * inner + (y + step) % inner, t),
            device_id_type=MESH,
        )

    def from_below(far):
        return pltpu.make_async_remote_copy(
            src_ref=slot(far, y),
            dst_ref=slot(far, y),
            send_sem=line_send.at[0],
            recv_sem=line_recv.at[far],
            device_id=((z + 1) * inner + y, t),
            device_id_type=MESH,
        )

    def from_side(far, step):
        side = (y + inner - step) % inner
        return pltpu.make_async_remote_copy(
            src_ref=slot(far, side),
            dst_ref=slot(far, side),
            send_sem=side_send.at[0, step],
            recv_sem=side_recv.at[far, step],
            device_id=(z * inner + (y + step) % inner, t),
            device_id_type=MESH,
        )

    def note(step):
        return pltpu.make_async_remote_copy(
            src_ref=notes_ref,
            dst_ref=all_notes_ref.at[z],
            send_sem=note_send.at[step],
            recv_sem=note_recv.at[step],
            device_id=groups.device("outer", (z + step) % outer),
            device_id_type=MESH,
        )

    def later_side(step):
        return (y + step) % inner > y

    def earlier_side(step):
        return (y + inner - step) % inner < y

    has_above = z < outer - 1
    pl.when(has_above)(lambda: upward(0).start())
    for step in range(1, inner):
        pl.when(later_side(step))(lambda step=step: sideways(0, step).start())
    for step in range(1, outer):
        note(step).start()
    own_copy = pltpu.make_async_copy(own_ref, all_ref.at[z * inner + y], keep.at[0])
    own_note = pltpu.make_async_copy(notes_ref, all_notes_ref.at[z], keep.at[1])
    own_copy.start()
    own_note.start()
    for far in range(1, outer):

        @pl.when(z >= far)
        def _(far=far):
            from_below(far).wait_recv()
            if far < outer - 1:
                pl.when(has_above)(lambda: upward(far).start())
            for step in range(1, inner):
                sideways(far, step).start()

    for far in range(outer):

        @pl.when(z >= far)
        def _(far=far):
            for step in range(1, inner):
                if far == 0:
                    pl.when(earlier_side(step))(lambda: from_side(far, step).wait_recv())
                    pl.when(later_side(step))(lambda: sideways(far, step).wait_send())
                else:
                    from_side(far, step).wait_recv()
                    sideways(far, step).wait_send()
            if far < outer - 1:
                pl.when(has_above)(lambda: upward(far).wait_send())

    for step in range(1, outer):
        note(step).wait()
    own_copy.wait()
    own_note.wait()


def gather(groups, collective_id, own, notes):
    outer, inner = groups.outer, groups.inner
    dma = pltpu.SemaphoreType.DMA
    return pl.pallas_call(
        functools.partial(gather_kernel, groups),
        out_shape=(
            jax.ShapeDtypeStruct((groups.n_sp,) + own.shape, own.dtype),
            jax.ShapeDtypeStruct((outer,) + notes.shape, notes.dtype),
        ),
        in_specs=[pl.BlockSpec(memory_space=pl.ANY)] * 2,
        out_specs=(pl.BlockSpec(memory_space=pl.ANY),) * 2,
        scratch_shapes=[
            dma((outer + 1,)),
            dma((outer + 1,)),
            dma((outer, inner)),
            dma((outer, inner)),
            dma((outer,)),
            dma((outer,)),
            dma((2,)),
        ],
        compiler_params=pltpu.CompilerParams(collective_id=collective_id, has_side_effects=True),
        name="gather",
    )(own, notes)


def dispatch_kernel(
    groups, own_ref, select_ref, all_ref, inbound_ref, line_ref, out_ref, *sems
):
    up_send, up_recv, down_send, down_recv, tp_send, tp_recv, plane_send, plane_recv, keep = sems
    outer, inner, n_tp, plane = groups.outer, groups.inner, groups.n_tp, groups.plane
    z, y, t = groups.place()
    pairs = n_tp // 2
    high, low = t // 2, t % 2
    partner = (z * inner + y, high * 2 + 1 - low)
    me = groups.mine("plane")
    barrier = pltpu.get_barrier_semaphore()
    for kind in ("outer", "plane"):
        for step in range(1, groups.size(kind)):
            pl.semaphore_signal(
                barrier,
                inc=1,
                device_id=groups.device(kind, (groups.mine(kind) + step) % groups.size(kind)),
                device_id_type=MESH,
            )
    pl.semaphore_wait(barrier, outer + plane - 2)

    def remote(source, target, send, recv, device):
        return pltpu.make_async_remote_copy(
            src_ref=source,
            dst_ref=target,
            send_sem=send,
            recv_sem=recv,
            device_id=device,
            device_id_type=MESH,
        )

    def along(far, direction):
        send, recv = (up_send, up_recv) if direction > 0 else (down_send, down_recv)
        block = z - direction * far
        source = own_ref if far == 0 else line_ref.at[block]
        return remote(
            source,
            line_ref.at[block],
            send.at[far],
            recv.at[far + 1],
            ((z + direction) * inner + y, t),
        )

    def arrived(far, direction):
        send, recv = (up_send, up_recv) if direction > 0 else (down_send, down_recv)
        block = line_ref.at[z - direction * far]
        return remote(
            block, block, send.at[0], recv.at[far], ((z + direction) * inner + y, t)
        )

    def outward(lane, block, step):
        peer = (me + step) % plane
        return remote(
            out_ref.at[block, peer],
            inbound_ref.at[me, block],
            plane_send.at[lane, step],
            plane_recv.at[lane, step],
            groups.device("plane", peer),
        )

    def inward(lane, block, step):
        peer = (me + plane - step) % plane
        target = inbound_ref.at[peer, block]
        return remote(
            target,
            target,
            plane_send.at[lane, step],
            plane_recv.at[lane, step],
            groups.device("plane", peer),
        )

    def keep_own(lane, block):
        return pltpu.make_async_copy(
            out_ref.at[block, me], inbound_ref.at[me, block], keep.at[1 + lane]
        )

    def work(lane, block, rows_ref):
        chosen = jnp.dot(select_ref[block], rows_ref[...], preferred_element_type=jnp.float32)
        out_ref[block] = chosen.reshape(out_ref.shape[1:]).astype(jnp.bfloat16)
        for step in range(1, plane):
            outward(lane, block, step).start()
        keep_own(lane, block).start()

    def finish(lane, block):
        keep_own(lane, block).wait()
        for step in range(1, plane):
            inward(lane, block, step).wait_recv()
            outward(lane, block, step).wait_send()

    def to_side(step):
        return remote(
            own_ref,
            all_ref.at[t],
            tp_send.at[step],
            tp_recv.at[step],
            (z * inner + y, ((high + step) % pairs) * 2 + low),
        )

    def to_partner(step):
        block = ((high + pairs - step) % pairs) * 2 + low
        source = own_ref if step == 0 else all_ref.at[block]
        target = all_ref.at[t] if step == 0 else all_ref.at[block]
        return remote(
            source, target, tp_send.at[pairs + step], tp_recv.at[pairs + step], partner
        )

    has_above, has_below = z < outer - 1, z > 0
    pl.when(has_above)(lambda: along(0, 1).start())
    pl.when(has_below)(lambda: along(0, -1).start())
    for step in range(1, pairs):
        to_side(step).start()
    to_partner(0).start()
    own_copy = pltpu.make_async_copy(own_ref, all_ref.at[t], keep.at[0])
    own_copy.start()
    work(0, z, own_ref)
    directions = ((1, has_above, 0), (-1, has_below, outer - 1))
    for far in range(1, outer):
        for direction, onward, base in directions:
            present = z >= far if direction > 0 else z + far < outer

            @pl.when(present)
            def _(far=far, direction=direction, onward=onward):
                arrived(far, direction).wait_recv()
                if far < outer - 1:
                    pl.when(onward)(lambda: along(far, direction).start())

        if far == 1:
            for step in range(1, pairs):
                side = all_ref.at[((high + pairs - step) % pairs) * 2 + low]
                remote(side, side, tp_send.at[step], tp_recv.at[step], partner).wait_recv()
                to_partner(step).start()
        for direction, onward, base in directions:
            present = z >= far if direction > 0 else z + far < outer

            @pl.when(present)
            def _(far=far, direction=direction, base=base):
                block = z - direction * far
                work(base + far, block, line_ref.at[block])

    finish(0, z)
    for far in range(1, outer):
        for direction, onward, base in directions:
            present = z >= far if direction > 0 else z + far < outer

            @pl.when(present)
            def _(far=far, direction=direction, onward=onward, base=base):
                finish(base + far, z - direction * far)
                if far < outer - 1:
                    pl.when(onward)(lambda: along(far, direction).wait_send())

    pl.when(has_above)(lambda: along(0, 1).wait_send())
    pl.when(has_below)(lambda: along(0, -1).wait_send())
    for step in range(1, pairs):
        to_side(step).wait_send()
    for step in range(pairs):
        to_partner(step).wait_send()
        block = all_ref.at[((high + pairs - step) % pairs) * 2 + 1 - low]
        remote(
            block, block, tp_send.at[pairs + step], tp_recv.at[pairs + step], partner
        ).wait_recv()
    own_copy.wait()


def dispatch_rows(groups, collective_id, own, select, seats):
    outer, plane, n_tp = groups.outer, groups.plane, groups.n_tp
    dma, kind = pltpu.SemaphoreType.DMA, own.dtype
    lanes = 2 * outer - 1
    vmem, anywhere = pl.BlockSpec(memory_space=pltpu.VMEM), pl.BlockSpec(memory_space=pl.ANY)
    return pl.pallas_call(
        functools.partial(dispatch_kernel, groups),
        out_shape=(
            jax.ShapeDtypeStruct((n_tp,) + own.shape, kind),
            jax.ShapeDtypeStruct((plane, outer, seats, own.shape[1]), kind),
        ),
        in_specs=[vmem, vmem],
        out_specs=(anywhere, anywhere),
        scratch_shapes=[
            pltpu.VMEM((outer,) + own.shape, kind),
            pltpu.VMEM((outer, plane, seats, own.shape[1]), kind),
            dma((outer + 1,)),
            dma((outer + 1,)),
            dma((outer + 1,)),
            dma((outer + 1,)),
            dma((n_tp,)),
            dma((n_tp,)),
            dma((lanes, plane)),
            dma((lanes, plane)),
            dma((lanes + 1,)),
        ],
        compiler_params=pltpu.CompilerParams(collective_id=collective_id, has_side_effects=True),
        name="dispatch_rows",
    )(own, select)


def flip(value, mask):
    bit = 1
    while bit <= mask:
        if mask & bit:
            value = value + bit - 2 * bit * ((value // bit) % 2)
        bit *= 2
    return value


def combine_kernel(
    groups, result_ref, mix_ref, shared_ref, routed_ref, parts_ref, back_ref, sum_ref, *sems
):
    plane_send, plane_recv, line_send, line_recv, tp_send, tp_recv, keep = sems
    outer, inner, n_tp, plane = groups.outer, groups.inner, groups.n_tp, groups.plane
    z, y, t = groups.place()
    me = groups.mine("plane")
    barrier = pltpu.get_barrier_semaphore()
    for kind in ("outer", "plane"):
        for step in range(1, groups.size(kind)):
            pl.semaphore_signal(
                barrier,
                inc=1,
                device_id=groups.device(kind, (groups.mine(kind) + step) % groups.size(kind)),
                device_id_type=MESH,
            )
    pl.semaphore_wait(barrier, outer + plane - 2)

    def remote(source, target, send, recv, device):
        return pltpu.make_async_remote_copy(
            src_ref=source,
            dst_ref=target,
            send_sem=send,
            recv_sem=recv,
            device_id=device,
            device_id_type=MESH,
        )

    def outward(mask, step):
        peer, block = (me + step) % plane, flip(z, mask)
        return remote(
            result_ref.at[peer, block],
            back_ref.at[block, me],
            plane_send.at[mask, step],
            plane_recv.at[mask, step],
            groups.device("plane", peer),
        )

    def inward(mask, step):
        peer, block = (me + plane - step) % plane, flip(z, mask)
        target = back_ref.at[block, peer]
        return remote(
            target,
            target,
            plane_send.at[mask, step],
            plane_recv.at[mask, step],
            groups.device("plane", peer),
        )

    def keep_own(mask):
        block = flip(z, mask)
        return pltpu.make_async_copy(
            result_ref.at[me, block], back_ref.at[block, me], keep.at[mask]
        )

    def issue(mask):
        for step in range(1, plane):
            outward(mask, step).start()
        keep_own(mask).start()

    def to_line(mask):
        block = flip(z, mask)
        return remote(
            sum_ref.at[block],
            routed_ref.at[z],
            line_send.at[mask],
            line_recv.at[mask],
            groups.device("outer", block),
        )

    def from_line(mask):
        block = routed_ref.at[flip(z, mask)]
        return remote(
            block,
            block,
            line_send.at[mask],
            line_recv.at[mask],
            groups.device("outer", flip(z, mask)),
        )

    def to_side(step):
        peer = (t + step) % n_tp
        return remote(
            shared_ref.at[peer],
            parts_ref.at[t],
            tp_send.at[step],
            tp_recv.at[step],
            groups.device("tp", peer),
        )

    def from_side(step):
        peer = (t + n_tp - step) % n_tp
        block = parts_ref.at[peer]
        return remote(
            block, block, tp_send.at[step], tp_recv.at[step], groups.device("tp", peer)
        )

    own_shared = pltpu.make_async_copy(shared_ref.at[t], parts_ref.at[t], keep.at[outer])
    own_shared.start()
    masks = list(range(outer - 1, -1, -1))
    for mask in masks[:2]:
        issue(mask)
    for number, mask in enumerate(masks):
        keep_own(mask).wait()
        for step in range(1, plane):
            inward(mask, step).wait_recv()
        if number + 2 < len(masks):
            issue(masks[number + 2])
        if number + 2 == len(masks) or len(masks) == 1:
            for step in range(1, n_tp):
                to_side(step).start()
        block = flip(z, mask)
        rows = back_ref[block].astype(jnp.float32)
        rows = rows.reshape(mix_ref.shape[2], rows.shape[-1]).astype(jnp.bfloat16)
        sum_ref[block] = jnp.dot(
            mix_ref[block], rows, preferred_element_type=jnp.float32
        ).astype(jnp.bfloat16)
        if mask:
            to_line(mask).start()
    own_sum = pltpu.make_async_copy(sum_ref.at[z], routed_ref.at[z], keep.at[outer + 1])
    own_sum.start()
    for mask in masks:
        for step in range(1, plane):
            outward(mask, step).wait_send()
        if mask:
            to_line(mask).wait_send()
            from_line(mask).wait_recv()
    for step in range(1, n_tp):
        to_side(step).wait_send()
        from_side(step).wait_recv()
    own_shared.wait()
    own_sum.wait()


def combine_rows(groups, collective_id, result, mix, shared):
    outer, plane, n_tp = groups.outer, groups.plane, groups.n_tp
    dma, kind = pltpu.SemaphoreType.DMA, result.dtype
    seats, width = result.shape[2:]
    vmem, anywhere = pl.BlockSpec(memory_space=pltpu.VMEM), pl.BlockSpec(memory_space=pl.ANY)
    return pl.pallas_call(
        functools.partial(combine_kernel, groups),
        out_shape=(
            jax.ShapeDtypeStruct((outer, mix.shape[1], width), kind),
            jax.ShapeDtypeStruct(shared.shape, kind),
        ),
        in_specs=[anywhere, vmem, anywhere],
        out_specs=(anywhere, anywhere),
        scratch_shapes=[
            pltpu.VMEM((outer, plane, seats, width), kind),
            pltpu.VMEM((outer, mix.shape[1], width), kind),
            dma((outer, plane)),
            dma((outer, plane)),
            dma((outer,)),
            dma((outer,)),
            dma((n_tp,)),
            dma((n_tp,)),
            dma((outer + 2,)),
        ],
        compiler_params=pltpu.CompilerParams(collective_id=collective_id, has_side_effects=True),
        name="combine_rows",
    )(result, mix, shared)


def layer_kernel(
    groups,
    chunks,
    seats,
    q_narrow_ref,
    k_narrow_ref,
    v_narrow_ref,
    g_narrow_ref,
    q_broad_ref,
    k_broad_ref,
    v_broad_ref,
    g_broad_ref,
    ids_ref,
    strength_ref,
    gain_hbm,
    project_narrow,
    project_broad,
    residual_ref,
    gate_ref,
    up_ref,
    down_ref,
    shared_gate_ref,
    shared_up_ref,
    shared_down_ref,
    out_ref,
    pairs_ref,
    q_narrow,
    q_broad,
    g_narrow,
    g_broad,
    own_ids,
    own_strength,
    gain_ref,
    gates_narrow,
    gates_broad,
    highest_narrow,
    highest_broad,
    totals_narrow,
    totals_broad,
    mixed_narrow,
    mixed_broad,
    heads_narrow,
    heads_broad,
    wp_narrow,
    wp_broad,
    w_gate,
    w_up,
    w_down,
    ws_gate,
    ws_up,
    ws_down,
    rows_own,
    notes,
    select,
    mixer,
    stream,
    tok,
    inbox,
    asked,
    acc_gate,
    acc_up,
    hidden,
    acc_sgate,
    acc_sup,
    shared_hidden,
    back,
    answer,
    parts,
    from_partner,
    kept,
    to_peer,
    from_peer,
    to_owner,
    relayed,
    from_owner,
    final,
    load_sem,
    first_sem,
    k_up_send,
    k_up_recv,
    k_side_send,
    k_side_recv,
    note_send,
    note_recv,
    z_send,
    z_recv,
    x_send,
    x_recv,
    p_send,
    p_recv,
    y_send,
    y_recv,
    r_send,
    r_recv,
    d_send,
    d_recv,
    s_send,
    s_recv,
    o_send,
    o_recv,
    i_recv,
):
    outer, inner, n_tp = groups.outer, groups.inner, groups.n_tp
    z, y, t = groups.place()
    pairs = n_tp // 2
    high, low = t // 2, t % 2
    width = gain_ref.shape[1]
    span = width // chunks
    units = outer * chunks
    count = rows_own.shape[0]
    group_rows = n_tp * count
    seat_rows = n_tp * seats
    bf16, f32 = jnp.bfloat16, jnp.float32
    partner = (z * inner + y, high * 2 + 1 - low)

    def remote(source, target, send, recv, device):
        return pltpu.make_async_remote_copy(
            src_ref=source,
            dst_ref=target,
            send_sem=send,
            recv_sem=recv,
            device_id=device,
            device_id_type=MESH,
        )

    def columns(piece):
        return pl.ds(pl.multiple_of(piece * span, span), span)

    def load(index):
        if index < chunks:
            return (
                pltpu.make_async_copy(
                    project_narrow.at[:, columns(index)], wp_narrow.at[index], load_sem.at[index, 0]
                ),
                pltpu.make_async_copy(
                    project_broad.at[:, columns(index)], wp_broad.at[index], load_sem.at[index, 1]
                ),
            )
        if index == chunks:
            first = pl.multiple_of(t * count, count)
            return (
                pltpu.make_async_copy(
                    residual_ref.at[pl.ds(first, count), :], rows_own, load_sem.at[index, 0]
                ),
            )
        if index == chunks + 1:
            return (
                pltpu.make_async_copy(gate_ref.at[0], w_gate, load_sem.at[index, 0]),
                pltpu.make_async_copy(up_ref.at[0], w_up, load_sem.at[index, 1]),
            )
        if index == chunks + 2:
            return (
                pltpu.make_async_copy(shared_gate_ref, ws_gate, load_sem.at[index, 0]),
                pltpu.make_async_copy(shared_up_ref, ws_up, load_sem.at[index, 1]),
            )
        return (
            pltpu.make_async_copy(down_ref.at[0], w_down, load_sem.at[index, 0]),
            pltpu.make_async_copy(shared_down_ref, ws_down, load_sem.at[index, 1]),
        )

    tokens = q_narrow.shape[1]
    place_of = z * inner + y
    narrow, broad = k_narrow_ref.shape[1], k_broad_ref.shape[1]
    own = pairs_ref.at[place_of]
    first_loads = [
        pltpu.make_async_copy(source, target, first_sem.at[number])
        for number, (source, target) in enumerate(
            (
                (k_narrow_ref, own.at[0, :, pl.ds(0, narrow)]),
                (v_narrow_ref, own.at[0, :, pl.ds(narrow, narrow)]),
                (k_broad_ref, own.at[1]),
                (v_broad_ref, own.at[2]),
            )
            + tuple(
                (queries.at[:, pl.ds(head * held.shape[2], held.shape[2])], held.at[head])
                for queries, held in ((q_narrow_ref, q_narrow), (q_broad_ref, q_broad))
                for head in range(held.shape[0])
            )
            + (
                (g_narrow_ref, g_narrow),
                (g_broad_ref, g_broad),
                (ids_ref, own_ids),
                (strength_ref, own_strength),
                (gain_hbm, gain_ref),
            )
        )
    ]
    for copy in first_loads:
        copy.start()

    barrier = pltpu.get_barrier_semaphore()
    greeted = 0
    for far in range(outer):
        for step in range(n_tp):
            if far or step:
                pl.semaphore_signal(
                    barrier,
                    inc=1,
                    device_id=(((z + far) % outer) * inner + y, (t + step) % n_tp),
                    device_id_type=MESH,
                )
                greeted += 1
    for step in range(1, inner):
        pl.semaphore_signal(
            barrier, inc=1, device_id=(z * inner + (y + step) % inner, t), device_id_type=MESH
        )
        greeted += 1
    pl.semaphore_wait(barrier, greeted)

    def slot(far, side):
        return pairs_ref.at[(z - far) * inner + side]

    def upward(far, piece):
        return remote(
            slot(far, y).at[piece],
            slot(far, y).at[piece],
            k_up_send.at[far, piece],
            k_up_recv.at[far + 1, piece],
            ((z + 1) * inner + y, t),
        )

    def from_below(far, piece):
        return remote(
            slot(far, y).at[piece],
            slot(far, y).at[piece],
            k_up_send.at[far, piece],
            k_up_recv.at[far, piece],
            ((z + 1) * inner + y, t),
        )

    def aside(far, step, piece):
        return remote(
            slot(far, y).at[piece],
            slot(far, y).at[piece],
            k_side_send.at[far, step - 1, piece],
            k_side_recv.at[far, step - 1, piece],
            (z * inner + (y + step) % inner, t),
        )

    def from_aside(far, step, piece):
        side = (y + inner - step) % inner
        return remote(
            slot(far, side).at[piece],
            slot(far, side).at[piece],
            k_side_send.at[far, step - 1, piece],
            k_side_recv.at[far, step - 1, piece],
            (z * inner + (y + step) % inner, t),
        )

    def later_side(step):
        return (y + step) % inner > y

    def earlier_side(step):
        return (y + inner - step) % inner < y

    has_above = z < outer - 1
    pieces = pairs_ref.shape[1]
    for piece in range(pieces):
        for copy in first_loads[:2] if piece == 0 else first_loads[piece + 1 : piece + 2]:
            copy.wait()
        pl.when(has_above)(lambda piece=piece: upward(0, piece).start())
        for step in range(1, inner):
            pl.when(later_side(step))(
                lambda step=step, piece=piece: aside(0, step, piece).start()
            )
    for copy in first_loads[pieces + 1 :]:
        copy.wait()

    def note(far, step):
        number = far * n_tp + step
        return remote(
            notes.at[z, t],
            notes.at[z, t],
            note_send.at[number],
            note_recv.at[number],
            (((z + far) % outer) * inner + y, (t + step) % n_tp),
        )

    others = [(far, step) for far in range(outer) for step in range(n_tp) if far or step]
    top = own_ids.shape[0]
    spread_out = jnp.where(
        lax.broadcasted_iota(jnp.int32, (count, group_rows), 1)
        == t * count + lax.broadcasted_iota(jnp.int32, (count, group_rows), 0),
        1.0,
        0.0,
    ).astype(bf16)
    notes[z, t, 0] = jnp.dot(
        own_ids[...].astype(f32).astype(bf16), spread_out, preferred_element_type=f32
    )
    notes[z, t, 1] = jnp.dot(
        own_strength[...].astype(bf16), spread_out, preferred_element_type=f32
    )
    for far, step in others:
        note(far, step).start()
    for index in range(chunks + 4):
        for copy in load(index):
            copy.start()

    first_row = pl.multiple_of(place_of * tokens, tokens)
    groups_of_heads = (
        (q_narrow, g_narrow, gates_narrow, highest_narrow, totals_narrow, mixed_narrow, 0, 0, narrow),
        (q_broad, g_broad, gates_broad, highest_broad, totals_broad, mixed_broad, 1, 2, 0),
    )
    for held, gates, own_gates, _, _, _, _, _, _ in groups_of_heads:
        heads = held.shape[0]
        turned = jnp.transpose(
            jnp.concatenate(
                [gates[:, pl.ds(first_row, tokens)], jnp.zeros((tokens - heads, tokens), f32)],
                axis=0,
            )
        )
        for head in range(heads):
            own_gates[head] = jnp.broadcast_to(turned[:, head : head + 1], (tokens, tokens))

    def make_tables():
        for far, step in others:
            note(far, step).wait_recv()
        lanes = mixer.shape[2]
        token = lax.broadcasted_iota(jnp.int32, (group_rows, lanes), 0)
        lane = lax.broadcasted_iota(jnp.int32, (group_rows, lanes), 1)
        token_before = lax.broadcasted_iota(jnp.int32, (group_rows, group_rows), 1)
        token_after = lax.broadcasted_iota(jnp.int32, (group_rows, group_rows), 0)
        earlier = (token_before < token_after) & (token_before // count == token_after // count)
        earlier = jnp.where(earlier, 1.0, 0.0).astype(bf16)
        seat_block = lane // seat_rows
        seat_place = (lane % seat_rows) // seats
        seat_number = (lane % seats).astype(f32)
        for block in range(outer):
            listed = notes[block, 0]
            for place in range(1, n_tp):
                listed = listed + notes[block, place]
            listed = jnp.transpose(
                jnp.concatenate(
                    [listed[0], listed[1], jnp.zeros((group_rows - 2 * top, group_rows), f32)], axis=0
                )
            )
            names, loads = listed[:, :top], listed[:, top : 2 * top]
            chosen = jnp.zeros((group_rows, lanes), f32)
            strength = jnp.zeros((group_rows, lanes), f32)
            for step in range(inner):
                expert = ((z * inner + (y + step) % inner) * n_tp + t).astype(f32)
                match = names == expert
                here = seat_block == step
                taken = jnp.sum(jnp.where(match, 1.0, 0.0), axis=1, keepdims=True)
                load_of = jnp.sum(jnp.where(match, loads, 0.0), axis=1, keepdims=True)
                chosen = jnp.where(here, taken, chosen)
                strength = jnp.where(here, load_of, strength)
            rank = jnp.dot(earlier, chosen.astype(bf16), preferred_element_type=f32)
            seated = (chosen > 0.5) & (rank == seat_number) & (seat_place == token // count)
            mixer[block] = jnp.where(seated, strength, 0.0).astype(bf16)
            select[block] = jnp.transpose(jnp.where(seated, 1.0, 0.0)).astype(bf16)

    def attend(block, blocks, own_block):
        length = blocks * tokens
        key_rows = pl.ds(pl.multiple_of(block * tokens, tokens), length)
        for held, gates, own_gates, highest, totals, mixed, key_at, value_at, value_from in groups_of_heads:
            heads, _, size = held.shape
            keys = pairs_ref[pl.ds(block, blocks), key_at, :, :size].reshape(length, size)
            values = pairs_ref[
                pl.ds(block, blocks), value_at, :, value_from : value_from + size
            ].reshape(length, size)
            scores = lax.dot_general(
                held[...].reshape(heads * tokens, size),
                keys,
                (((1,), (1,)), ((), ())),
                preferred_element_type=f32,
            ).reshape(heads, tokens, length)
            key_gates = gates[:, key_rows].reshape(heads, 1, length)
            pieces_of = []
            for part in range(blocks):
                at = slice(part * tokens, (part + 1) * tokens)
                piece = scores[:, :, at] * size ** (-0.5)
                piece = piece + own_gates[...] - key_gates[:, :, at]
                if own_block:
                    row = lax.broadcasted_iota(jnp.int32, (heads, tokens, tokens), 1)
                    column = lax.broadcasted_iota(jnp.int32, (heads, tokens, tokens), 2)
                    piece = jnp.where(column <= row, piece, -jnp.inf)
                pieces_of.append(piece)
            most = functools.reduce(jnp.maximum, pieces_of)
            peak = jnp.broadcast_to(jnp.max(most, axis=2, keepdims=True), most.shape)
            if not own_block:
                before = highest[...]
                peak = jnp.maximum(before, peak)
            weights = [jnp.exp(piece - peak) for piece in pieces_of]
            total = functools.reduce(jnp.add, weights)
            rounded = [piece.astype(bf16) for piece in weights]
            blended = jnp.dot(
                jnp.concatenate(rounded, axis=2).reshape(heads * tokens, length),
                values,
                preferred_element_type=f32,
            ).reshape(heads, tokens, size)
            if own_block:
                totals[...] = total
                mixed[...] = blended
            else:
                fade = jnp.exp(before - peak)
                totals[...] = totals[...] * fade + total
                mixed[...] = mixed[...] * jnp.concatenate([fade] * (size // tokens), axis=2) + blended
            highest[...] = peak

    attend(place_of, 1, True)

    def take_side():
        for step in range(1, inner):

            @pl.when(earlier_side(step))
            def _(step=step):
                for piece in range(pieces):
                    from_aside(0, step, piece).wait_recv()
                attend(z * inner + (y + inner - step) % inner, 1, False)

    def take_row(far):
        for step in range(1, inner):
            for piece in range(pieces):
                from_aside(far, step, piece).wait_recv()
        attend((z - far) * inner, inner, False)

    def climb_up(far):
        @pl.when(z >= far)
        def _():
            for piece in range(pieces):
                from_below(far, piece).wait_recv()
                pl.when(has_above & (far < outer - 1))(lambda piece=piece: upward(far, piece).start())
                for step in range(1, inner):
                    aside(far, step, piece).start()

    def climb(far, carried):
        climb_up(far)
        pl.when(z >= far - 1)(lambda: take_row(far - 1))
        return carried

    climb_up(1)
    take_side()
    climb_up(2)
    make_tables()
    pl.when(z >= 1)(lambda: take_row(1))
    lax.fori_loop(3, outer, climb, 0)
    pl.when(z >= outer - 1)(lambda: take_row(outer - 1))
    for mixed, totals, heads_out in (
        (mixed_narrow, totals_narrow, heads_narrow),
        (mixed_broad, totals_broad, heads_broad),
    ):
        heads, _, size = mixed.shape
        for head in range(heads):
            heads_out[:, head * size : (head + 1) * size] = (
                mixed[head] / jnp.sum(totals[head], axis=1, keepdims=True)
            ).astype(bf16)

    def across(unit):
        return remote(
            parts.at[unit, 1 - low],
            from_partner.at[unit],
            d_send.at[unit],
            d_recv.at[unit],
            partner,
        )

    def sideways(unit, step):
        return remote(
            to_peer.at[unit, step - 1],
            from_peer.at[unit, step - 1],
            s_send.at[unit, step - 1],
            s_recv.at[unit, step - 1],
            (z * inner + y, ((high + step) % pairs) * 2 + low),
        )

    def reduce_start(unit, value):
        for place in range(n_tp):
            parts[unit, place % 2, place // 2] = value[
                place * count : (place + 1) * count
            ].astype(bf16)
        across(unit).start()

    def reduce_pass(unit):
        across(unit).wait_recv()
        for step in range(1, pairs):
            other = (high + step) % pairs
            to_peer[unit, step - 1] = (
                parts[unit, low, other].astype(f32) + from_partner[unit, other].astype(f32)
            ).astype(bf16)
            sideways(unit, step).start()
        kept[unit] = parts[unit, low, high].astype(f32) + from_partner[unit, high].astype(f32)

    def reduce_end(unit):
        total = kept[unit]
        for step in range(1, pairs):
            sideways(unit, step).wait_recv()
            total = total + from_peer[unit, step - 1].astype(f32)
        return total

    for piece in range(chunks):
        for copy in load(piece):
            copy.wait()
        value = jnp.dot(heads_narrow[...], wp_narrow[piece], preferred_element_type=f32)
        value = value + jnp.dot(heads_broad[...], wp_broad[piece], preferred_element_type=f32)
        reduce_start(piece, value)
        if piece:
            reduce_pass(piece - 1)
    reduce_pass(chunks - 1)

    directions = ((1, has_above), (-1, z > 0))

    def along(block, piece, direction):
        return remote(
            tok.at[block, piece, t],
            tok.at[block, piece, t],
            z_send.at[block, piece, (direction + 1) // 2],
            z_recv.at[block, piece],
            ((z + direction) * inner + y, t),
        )

    for copy in load(chunks):
        copy.wait()
    square = jnp.zeros((count, 1), f32)
    for piece in range(chunks):
        value = reduce_end(piece) + rows_own[:, piece * span : (piece + 1) * span].astype(f32)
        stream[piece] = value
        square = square + jnp.sum(value * value, axis=1, keepdims=True)
    scale = lax.rsqrt(square * (1.0 / width) + norm_epsilon)
    for piece in range(chunks):
        gain = gain_ref[:, piece * span : (piece + 1) * span]
        tok[z, piece, t] = (stream[piece] * scale * gain).astype(bf16)
        for direction, onward in directions:
            pl.when(onward)(
                lambda piece=piece, direction=direction: along(z, piece, direction).start()
            )
    for index in range(chunks + 1, chunks + 3):
        for copy in load(index):
            copy.wait()

    in_low = z < outer // 2
    mate = z + 1 - 2 * (z % 2)
    near = jnp.where(in_low, outer // 2, outer // 2 - 1)
    distant = jnp.where(in_low, outer - 1, 0)
    is_edge = (z == 0) | (z == outer - 1)

    def pick(number, one, two, three, four):
        low_pair = jnp.where(number == 0, one, two)
        return jnp.where(number < 2, low_pair, jnp.where(number == 2, three, four))

    def going(unit):
        return pick(unit // chunks, z, mate, near, distant), unit % chunks

    def coming(unit):
        return pick(unit // chunks, near, distant, mate, z), unit % chunks

    def to_chip(block, piece, step):
        return remote(
            tok.at[block, piece, t],
            tok.at[block, piece, t],
            x_send.at[block, piece, step - 1],
            x_recv.at[block, piece, step - 1],
            (z * inner + y, ((high + step) % pairs) * 2 + low),
        )

    def from_chip(block, piece, step):
        place = tok.at[block, piece, ((high + pairs - step) % pairs) * 2 + low]
        return remote(
            place,
            place,
            x_send.at[block, piece, step - 1],
            x_recv.at[block, piece, step - 1],
            (z * inner + y, ((high + step) % pairs) * 2 + low),
        )

    def to_partner(block, piece, step):
        place = tok.at[block, piece, ((high + pairs - step) % pairs) * 2 + low]
        return remote(
            place, place, p_send.at[block, piece, step], p_recv.at[block, piece, step], partner
        )

    def from_other_core(block, piece, step):
        place = tok.at[block, piece, ((high + pairs - step) % pairs) * 2 + 1 - low]
        return remote(
            place, place, p_send.at[block, piece, step], p_recv.at[block, piece, step], partner
        )

    def ask(block, piece, step):
        return remote(
            asked.at[block, piece, step - 1],
            inbox.at[block, piece, step],
            y_send.at[block, piece, step - 1],
            y_recv.at[block, piece, step - 1],
            (z * inner + (y + step) % inner, t),
        )

    def reply(block, piece, step):
        return remote(
            answer.at[block, piece, step - 1],
            back.at[block, piece, step],
            r_send.at[block, piece, step - 1],
            r_recv.at[block, piece, step - 1],
            (z * inner + (y + inner - step) % inner, t),
        )

    def to_inner(number, piece):
        return remote(
            to_owner.at[number, piece],
            relayed.at[number, piece],
            o_send.at[number, piece],
            i_recv.at[number, piece],
            (mate * inner + y, t),
        )

    def to_other(number, piece):
        return remote(
            to_owner.at[number, piece],
            from_owner.at[1, piece],
            o_send.at[number, piece],
            o_recv.at[1, piece],
            (jnp.where(number == 0, near, distant) * inner + y, t),
        )

    def to_mate(piece):
        return remote(
            to_owner.at[2, piece],
            from_owner.at[0, piece],
            o_send.at[2, piece],
            o_recv.at[0, piece],
            (mate * inner + y, t),
        )

    def receive(block, piece):
        for direction, onward in directions:
            passes = (block < z) if direction > 0 else (block > z)

            @pl.when(passes)
            def _(direction=direction, onward=onward):
                along(block, piece, direction).wait_recv()
                pl.when(onward)(lambda: along(block, piece, direction).start())

    def arrive(unit):
        block, piece = going(unit)
        number = unit // chunks
        later = jnp.where(is_edge, number, number + 1)
        pl.when(number == 1)(lambda: receive(mate, piece))
        pl.when((number > 0) & (later == 2))(lambda: receive(near, piece))
        pl.when((number > 0) & (later == 3))(lambda: receive(distant, piece))
        for step in range(1, pairs):
            to_chip(block, piece, step).start()
        to_partner(block, piece, 0).start()

    def spread(unit):
        block, piece = going(unit)
        for step in range(1, pairs):
            from_chip(block, piece, step).wait_recv()
            to_partner(block, piece, step).start()

    def choose(unit):
        block, piece = going(unit)
        for step in range(pairs):
            from_other_core(block, piece, step).wait_recv()
        rows = tok[block, piece].reshape(group_rows, span)
        picked = jnp.dot(
            select[block, : inner * seat_rows], rows, preferred_element_type=f32
        ).astype(bf16)
        for step in range(1, inner):
            asked[block, piece, step - 1] = picked[step * seat_rows : (step + 1) * seat_rows]
            ask(block, piece, step).start()
        inbox[block, piece, 0] = picked[:seat_rows]

    def expand(unit):
        block, piece = going(unit)
        for step in range(1, inner):
            ask(block, piece, step).wait_recv()
        rows = inbox[block, piece].reshape(inner * seat_rows, span)
        part_gate = jnp.dot(rows, w_gate[columns(piece), :], preferred_element_type=f32)
        part_up = jnp.dot(rows, w_up[columns(piece), :], preferred_element_type=f32)

        @pl.when(piece == 0)
        def _():
            acc_gate[...] = part_gate
            acc_up[...] = part_up

        @pl.when(piece > 0)
        def _():
            acc_gate[...] += part_gate
            acc_up[...] += part_up

        @pl.when(piece == chunks - 1)
        def _():
            hidden[block] = (jax.nn.silu(acc_gate[...]) * acc_up[...]).astype(bf16)

    def expand_shared(piece):
        rows = tok[z, piece].reshape(group_rows, span)
        part_gate = jnp.dot(rows, ws_gate[columns(piece), :], preferred_element_type=f32)
        part_up = jnp.dot(rows, ws_up[columns(piece), :], preferred_element_type=f32)

        @pl.when(piece == 0)
        def _():
            acc_sgate[...] = part_gate
            acc_sup[...] = part_up

        @pl.when(piece > 0)
        def _():
            acc_sgate[...] += part_gate
            acc_sup[...] += part_up

        @pl.when(piece == chunks - 1)
        def _():
            shared_hidden[...] = (jax.nn.silu(acc_sgate[...]) * acc_sup[...]).astype(bf16)

    def within(number, first, last):
        return (number >= first) & (number < last)

    def produce(unit):
        block, piece = coming(unit)
        made = jnp.dot(hidden[block], w_down[:, columns(piece)], preferred_element_type=f32)
        made = made.astype(bf16)
        for step in range(1, inner):
            answer[block, piece, step - 1] = made[step * seat_rows : (step + 1) * seat_rows]
            reply(block, piece, step).start()
        back[block, piece, 0] = made[:seat_rows]

    def blend(unit):
        block, piece = coming(unit)
        for step in range(1, inner):
            reply(block, piece, step).wait_recv()
        rows = back[block, piece].reshape(inner * seat_rows, span)
        value = jnp.dot(
            mixer[block][:, : inner * seat_rows], rows, preferred_element_type=f32
        )

        @pl.when(block != z)
        def _():
            reduce_start(chunks + unit, value)

        @pl.when(block == z)
        def _():
            shared_part = jnp.dot(
                shared_hidden[...], ws_down[:, columns(piece)], preferred_element_type=f32
            )
            reduce_start(chunks + unit, value + shared_part)

    def deliver(unit):
        number, piece = unit // chunks, unit % chunks
        total = reduce_end(chunks + unit)

        @pl.when((number < 2) & is_edge)
        def _():
            to_owner[number, piece] = total.astype(bf16)
            to_inner(number, piece).start()

        @pl.when((number < 2) & jnp.logical_not(is_edge))
        def _():
            kept[chunks + unit] = total

        @pl.when(number == 2)
        def _():
            to_owner[2, piece] = total.astype(bf16)
            to_mate(piece).start()

        @pl.when(number == 3)
        def _():
            final[piece] = total

    def relay(unit):
        number, piece = unit // chunks, unit % chunks
        to_inner(number, piece).wait_recv()
        to_owner[number, piece] = (
            kept[chunks + unit] + relayed[number, piece].astype(f32)
        ).astype(bf16)
        to_other(number, piece).start()

    (
        late_spread,
        late_choose,
        late_expand,
        late_produce,
        late_blend,
        late_pass,
        late_deliver,
        late_relay,
    ) = LAGS
    for copy in load(chunks + 3):
        copy.wait()

    def retire_early():
        for far, step in others:
            note(far, step).wait_send()
        for far in range(outer):

            @pl.when(z >= far)
            def _(far=far):
                for piece in range(pieces):
                    for step in range(1, inner):
                        sent = (far > 0) | later_side(step)
                        pl.when(sent)(
                            lambda step=step, piece=piece: aside(far, step, piece).wait_send()
                        )
                    if far < outer - 1:
                        pl.when(has_above)(lambda piece=piece: upward(far, piece).wait_send())

        for piece in range(chunks):
            across(piece).wait_send()
            for step in range(1, pairs):
                sideways(piece, step).wait_send()

    def retire_out(unit):
        block, piece = going(unit)
        for direction, onward in directions:
            has = (block <= z) if direction > 0 else (block >= z)

            @pl.when(has & onward)
            def _(direction=direction):
                along(block, piece, direction).wait_send()

        for step in range(1, pairs):
            to_chip(block, piece, step).wait_send()
        for step in range(pairs):
            to_partner(block, piece, step).wait_send()
        for step in range(1, inner):
            ask(block, piece, step).wait_send()

    def retire_back(unit):
        block, piece = coming(unit)
        for step in range(1, inner):
            reply(block, piece, step).wait_send()
        across(chunks + unit).wait_send()
        for step in range(1, pairs):
            sideways(chunks + unit, step).wait_send()

    def step_all(unit, carried):
        pl.when(within(unit, 0, units))(lambda: arrive(unit))
        two = unit - late_choose
        pl.when(within(two, 0, units))(lambda: choose(two))
        one = unit - late_spread
        pl.when(one == 0)(retire_early)
        pl.when(within(one, 0, units))(lambda: spread(one))
        pl.when(within(two, 0, chunks))(lambda: expand_shared(two))
        three = unit - late_expand
        pl.when(within(three, 0, units))(lambda: expand(three))
        four = unit - late_produce
        pl.when(within(four, 0, units))(lambda: produce(four))
        five = unit - late_blend
        pl.when(within(five, 0, units))(lambda: blend(five))
        six = unit - late_pass
        pl.when(within(six, 0, units))(lambda: reduce_pass(chunks + six))
        seven = unit - late_deliver
        pl.when(within(seven, 0, units))(lambda: deliver(seven))
        pl.when(within(unit - late_deliver, 0, units))(lambda: retire_out(unit - late_deliver))
        pl.when(within(seven, 0, units))(lambda: retire_back(seven))
        eight = unit - late_relay
        pl.when(within(eight, 0, 2 * chunks) & jnp.logical_not(is_edge))(lambda: relay(eight))
        return carried

    lax.fori_loop(0, units + late_deliver, step_all, 0)

    for piece in range(chunks):
        total = stream[piece] + final[piece]
        for place, copy in enumerate((to_mate(piece), to_other(0, piece))):
            copy.wait_recv()
            total = total + from_owner[place, piece].astype(f32)
        out_ref[:, piece * span : (piece + 1) * span] = total.astype(bf16)

    for piece in range(chunks):
        for number in range(2):
            pl.when(is_edge)(
                lambda number=number, piece=piece: to_inner(number, piece).wait_send()
            )
            pl.when(jnp.logical_not(is_edge))(
                lambda number=number, piece=piece: to_other(number, piece).wait_send()
            )
        to_mate(piece).wait_send()


LAGS = (3, 4, 7, 20, 23, 24, 27, 30)


def layer_rows(
    groups,
    collective_id,
    seats,
    query_narrow,
    key_narrow,
    value_narrow,
    gates_narrow,
    query_broad,
    key_broad,
    value_broad,
    gates_broad,
    project_narrow,
    project_broad,
    residual,
    norm_gain,
    route_ids,
    route_weight,
    expert_gate,
    expert_up,
    expert_down,
    shared_gate,
    shared_up,
    shared_down,
):
    outer, inner, n_tp = groups.outer, groups.inner, groups.n_tp
    dma = pltpu.SemaphoreType.DMA
    width = residual.shape[1]
    chunks = width // math.gcd(width, 1024)
    span = width // chunks
    count, top = route_ids.shape
    tokens = query_narrow.shape[0]
    heads_n, heads_b = gates_narrow.shape[1], gates_broad.shape[1]
    group_rows = n_tp * count
    seat_rows = n_tp * seats
    pairs = n_tp // 2
    units = outer * chunks
    sums = chunks + units
    lanes = -(-inner * seat_rows // 128) * 128
    bf16, f32 = jnp.bfloat16, jnp.float32
    expert_width, shared_width = expert_gate.shape[2], shared_gate.shape[1]
    vmem, anywhere = pl.BlockSpec(memory_space=pltpu.VMEM), pl.BlockSpec(memory_space=pl.ANY)
    return pl.pallas_call(
        functools.partial(layer_kernel, groups, chunks, seats),
        out_shape=jax.ShapeDtypeStruct((count, width), bf16),
        in_specs=[anywhere] * 20,
        out_specs=vmem,
        scratch_shapes=[
            pltpu.VMEM((groups.n_sp, 3, tokens, key_broad.shape[1]), bf16),
            pltpu.VMEM((heads_n, tokens, NARROW_SIZE), bf16),
            pltpu.VMEM((heads_b, tokens, BROAD_SIZE), bf16),
            pltpu.VMEM(gates_narrow.shape[::-1], f32),
            pltpu.VMEM(gates_broad.shape[::-1], f32),
            pltpu.VMEM((top, count), jnp.int32),
            pltpu.VMEM((top, count), f32),
            pltpu.VMEM((1, width), f32),
            *[pltpu.VMEM((number, tokens, tokens), f32) for _ in range(3) for number in (heads_n, heads_b)],
            pltpu.VMEM((heads_n, tokens, NARROW_SIZE), f32),
            pltpu.VMEM((heads_b, tokens, BROAD_SIZE), f32),
            pltpu.VMEM(query_narrow.shape, bf16),
            pltpu.VMEM(query_broad.shape, bf16),
            pltpu.VMEM((chunks, project_narrow.shape[0], span), bf16),
            pltpu.VMEM((chunks, project_broad.shape[0], span), bf16),
            pltpu.VMEM((width, expert_width), bf16),
            pltpu.VMEM((width, expert_width), bf16),
            pltpu.VMEM((expert_width, width), bf16),
            pltpu.VMEM((width, shared_width), bf16),
            pltpu.VMEM((width, shared_width), bf16),
            pltpu.VMEM((shared_width, width), bf16),
            pltpu.VMEM((count, width), bf16),
            pltpu.VMEM((outer, n_tp, 2, top, group_rows), f32),
            pltpu.VMEM((outer, lanes, group_rows), bf16),
            pltpu.VMEM((outer, group_rows, lanes), bf16),
            pltpu.VMEM((chunks, count, span), f32),
            pltpu.VMEM((outer, chunks, n_tp, count, span), bf16),
            pltpu.VMEM((outer, chunks, inner, seat_rows, span), bf16),
            pltpu.VMEM((outer, chunks, inner - 1, seat_rows, span), bf16),
            pltpu.VMEM((inner * seat_rows, expert_width), f32),
            pltpu.VMEM((inner * seat_rows, expert_width), f32),
            pltpu.VMEM((outer, inner * seat_rows, expert_width), bf16),
            pltpu.VMEM((group_rows, shared_width), f32),
            pltpu.VMEM((group_rows, shared_width), f32),
            pltpu.VMEM((group_rows, shared_width), bf16),
            pltpu.VMEM((outer, chunks, inner, seat_rows, span), bf16),
            pltpu.VMEM((outer, chunks, inner - 1, seat_rows, span), bf16),
            pltpu.VMEM((sums, 2, pairs, count, span), bf16),
            pltpu.VMEM((sums, pairs, count, span), bf16),
            pltpu.VMEM((sums, count, span), f32),
            pltpu.VMEM((sums, pairs - 1, count, span), bf16),
            pltpu.VMEM((sums, pairs - 1, count, span), bf16),
            pltpu.VMEM((3, chunks, count, span), bf16),
            pltpu.VMEM((2, chunks, count, span), bf16),
            pltpu.VMEM((2, chunks, count, span), bf16),
            pltpu.VMEM((chunks, count, span), f32),
            dma((chunks + 4, 2)),
            dma((9 + heads_n + heads_b,)),
            dma((outer, 3)),
            dma((outer + 1, 3)),
            dma((outer, inner - 1, 3)),
            dma((outer, inner - 1, 3)),
            dma((outer * n_tp,)),
            dma((outer * n_tp,)),
            dma((outer, chunks, 2)),
            dma((outer, chunks)),
            dma((outer, chunks, pairs - 1)),
            dma((outer, chunks, pairs - 1)),
            dma((outer, chunks, pairs)),
            dma((outer, chunks, pairs)),
            dma((outer, chunks, inner - 1)),
            dma((outer, chunks, inner - 1)),
            dma((outer, chunks, inner - 1)),
            dma((outer, chunks, inner - 1)),
            dma((sums,)),
            dma((sums,)),
            dma((sums, pairs - 1)),
            dma((sums, pairs - 1)),
            dma((3, chunks)),
            dma((2, chunks)),
            dma((2, chunks)),
        ],
        compiler_params=pltpu.CompilerParams(
            collective_id=collective_id, has_side_effects=True, vmem_limit_bytes=54 * 2**20
        ),
        name="layer_rows",
    )(
        query_narrow,
        key_narrow,
        value_narrow,
        gates_narrow.T,
        query_broad,
        key_broad,
        value_broad,
        gates_broad.T,
        route_ids.T,
        route_weight.T,
        norm_gain.reshape(1, width),
        project_narrow,
        project_broad,
        residual,
        expert_gate,
        expert_up,
        expert_down,
        shared_gate,
        shared_up,
        shared_down,
    )


def local(
    groups,
    query_narrow,
    key_narrow,
    value_narrow,
    gates_narrow,
    query_broad,
    key_broad,
    value_broad,
    gates_broad,
    project_narrow,
    project_broad,
    residual,
    norm_gain,
    route_ids,
    route_weight,
    expert_gate,
    expert_up,
    expert_down,
    shared_gate,
    shared_up,
    shared_down,
):
    spots = 2 * route_ids.size // (groups.n_sp * groups.n_tp * expert_gate.shape[0])
    if (
        spots % 8 == 0
        and groups.n_tp == 4
        and groups.inner == 2
        and groups.outer == 4
        and expert_gate.shape[0] == 1
        and 2 * key_narrow.shape[1] == key_broad.shape[1]
    ):
        return layer_rows(
            groups,
            0,
            spots,
            query_narrow,
            key_narrow,
            value_narrow,
            gates_narrow,
            query_broad,
            key_broad,
            value_broad,
            gates_broad,
            project_narrow,
            project_broad,
            residual,
            norm_gain,
            route_ids,
            route_weight,
            expert_gate,
            expert_up,
            expert_down,
            shared_gate,
            shared_up,
            shared_down,
        )
    tokens = query_narrow.shape[0]
    notes = jnp.concatenate(
        [
            route_ids.astype(jnp.float32).T,
            route_weight.astype(jnp.bfloat16).astype(jnp.float32).T,
        ],
        axis=0,
    )
    own_pairs = jnp.concatenate([key_narrow, key_broad, value_narrow, value_broad], axis=1)
    all_pairs, all_notes = gather(groups, 0, own_pairs, notes)
    all_pairs = all_pairs.reshape(-1, own_pairs.shape[1])
    vmem = pl.BlockSpec(memory_space=pltpu.VMEM)
    heads_out = pl.pallas_call(
        attend_kernel,
        out_shape=(
            jax.ShapeDtypeStruct(query_narrow.shape, jnp.bfloat16),
            jax.ShapeDtypeStruct(query_broad.shape, jnp.bfloat16),
        ),
        in_specs=[vmem] * 7,
        out_specs=(vmem, vmem),
        name="attend",
    )(
        query_narrow,
        query_broad,
        gates_narrow,
        gates_broad,
        gates_narrow.T,
        gates_broad.T,
        all_pairs,
    )
    partial_value = jnp.dot(heads_out[0], project_narrow, preferred_element_type=jnp.float32)
    partial_value = partial_value + jnp.dot(
        heads_out[1], project_broad, preferred_element_type=jnp.float32
    )
    n_tp, outer, plane = groups.n_tp, groups.outer, groups.plane
    sub_rows, width = route_ids.shape[0], residual.shape[1]
    (portions,) = swap(
        groups, 1, (partial_value.astype(jnp.bfloat16).reshape(n_tp, sub_rows, width), "tp", 0, 0)
    )
    stream, own_normed = pl.pallas_call(
        norm_kernel,
        out_shape=(
            jax.ShapeDtypeStruct((sub_rows, width), jnp.float32),
            jax.ShapeDtypeStruct((sub_rows, width), jnp.bfloat16),
        ),
        in_specs=[vmem] * 3,
        out_specs=(vmem, vmem),
        name="norm",
    )(portions, residual, norm_gain.reshape(1, width))
    top_count = route_ids.shape[1]
    local_experts = expert_gate.shape[0]
    expert_total = groups.n_sp * n_tp * local_experts
    capacity = 2 * sub_rows * top_count // expert_total
    seat_rows = local_experts * capacity
    fused = seat_rows % 8 == 0 and n_tp % 2 == 0
    plane_experts = plane * local_experts
    first_expert = groups.mine("outer") * plane_experts
    line_ids = all_notes[:, :top_count].astype(jnp.int32)
    line_weights = all_notes[:, top_count:]
    named = (
        line_ids[:, None]
        == first_expert + jnp.arange(plane_experts, dtype=jnp.int32)[None, :, None, None]
    )
    chosen = jnp.any(named, axis=2)
    strength = jnp.sum(jnp.where(named, line_weights[:, None], 0.0), axis=2)
    before = jnp.arange(sub_rows)[:, None] < jnp.arange(sub_rows)[None, :]
    rank = jnp.sum(jnp.where(chosen[:, :, :, None] & before, 1, 0), axis=2)
    seats = chosen[:, :, None, :] & (
        rank[:, :, None, :] == jnp.arange(capacity, dtype=jnp.int32)[None, None, :, None]
    )
    dispatch = seats.astype(jnp.bfloat16).reshape(outer, plane_experts * capacity, sub_rows)
    combiner = (
        jnp.where(seats, strength[:, :, None, :], 0.0)
        .astype(jnp.bfloat16)
        .reshape(outer, plane_experts * capacity, sub_rows)
    )
    if fused:
        normed, inbound = dispatch_rows(groups, 2, own_normed, dispatch, seat_rows)
    else:
        normed, line_normed = swap(
            groups, 2, (own_normed, "tp", None, 0), (own_normed, "outer", None, 0)
        )
        outbound = jnp.einsum("zct,ztd->zcd", dispatch, line_normed, preferred_element_type=jnp.float32)
        outbound = outbound.astype(jnp.bfloat16).reshape(
            outer, plane, local_experts * capacity, width
        )
        (inbound,) = swap(groups, 3, (outbound, "plane", 1, 0))
    normed = normed.reshape(tokens, width)
    grouped = inbound.reshape(plane * outer, local_experts, capacity, width)
    gate_out = jnp.einsum(
        "secd,edh->sech", grouped, expert_gate, preferred_element_type=jnp.float32
    )
    up_out = jnp.einsum("secd,edh->sech", grouped, expert_up, preferred_element_type=jnp.float32)
    hidden = (jax.nn.silu(gate_out) * up_out).astype(jnp.bfloat16)
    result = jnp.einsum(
        "sech,ehd->secd", hidden, expert_down, preferred_element_type=jnp.float32
    ).astype(jnp.bfloat16)
    shared_hidden = (
        jax.nn.silu(jnp.dot(normed, shared_gate, preferred_element_type=jnp.float32))
        * jnp.dot(normed, shared_up, preferred_element_type=jnp.float32)
    ).astype(jnp.bfloat16)
    shared_out = jnp.dot(shared_hidden, shared_down, preferred_element_type=jnp.float32).astype(
        jnp.bfloat16
    )
    shared_out = shared_out.reshape(n_tp, sub_rows, width)
    if fused:
        routed_parts, shared_parts = combine_rows(
            groups, 4, result.reshape(inbound.shape), combiner.transpose(0, 2, 1), shared_out
        )
    else:
        (returned,) = swap(groups, 4, (result.reshape(inbound.shape), "plane", 0, 1))
        returned = returned.reshape(outer, plane_experts * capacity, width)
        line_routed = jnp.einsum(
            "zct,zcd->ztd", combiner, returned, preferred_element_type=jnp.float32
        ).astype(jnp.bfloat16)
        routed_parts, shared_parts = swap(
            groups,
            5,
            (line_routed, "outer", 0, 0),
            (shared_out, "tp", 0, 0),
        )
    tile = math.gcd(width, 1024)
    return pl.pallas_call(
        add_kernel,
        grid=(width // tile,),
        out_shape=jax.ShapeDtypeStruct((sub_rows, width), jnp.bfloat16),
        in_specs=[
            pl.BlockSpec((sub_rows, tile), lambda i: (0, i)),
            pl.BlockSpec((n_tp, sub_rows, tile), lambda i: (0, 0, i)),
            pl.BlockSpec((outer, sub_rows, tile), lambda i: (0, 0, i)),
        ],
        out_specs=pl.BlockSpec((sub_rows, tile), lambda i: (0, i)),
        name="add_parts",
    )(stream, shared_parts, routed_parts)


def solution(mesh):
    placed = (
        P("sp", "tp"),
        P("sp", "tp"),
        P("sp", "tp"),
        P(None, "tp"),
        P("sp", "tp"),
        P("sp", "tp"),
        P("sp", "tp"),
        P(None, "tp"),
        P("tp", None),
        P("tp", None),
        P("sp", None),
        P(),
        P(("sp", "tp"), None),
        P(("sp", "tp"), None),
        P(("sp", "tp"), None, None),
        P(("sp", "tp"), None, None),
        P(("sp", "tp"), None, None),
        P(None, "tp"),
        P(None, "tp"),
        P("tp", None),
    )
    groups = Groups(mesh.shape["sp"], mesh.shape["tp"])
    return jax.shard_map(
        functools.partial(local, groups), mesh=mesh, in_specs=placed, out_specs=P(("sp", "tp"), None), check_vma=False
    )
```
